128 devices in a mesh: kv: 16 (over z, y), tp: 8 (over x, core).
Axes of the slice: x: 4, y: 4, z: 4, core: 2. Of those that a mesh axis runs over, the one named last changes fastest.
Arguments:
- hidden_rows: bfloat16 [16384, 4096], P(('kv', 'tp')), may hold values from -6 to 6
- queries: bfloat16 [16384, 4096], P('kv', 'tp'), may hold values from -6 to 6
- key_rows: bfloat16 [16384, 1024], P('kv', 'tp'), may hold values from -6 to 6
- value_rows: bfloat16 [16384, 1024], P('kv', 'tp'), may hold values from -6 to 6
- branch_gates: float32 [2, 32, 16384], P(None, 'tp', 'kv'), may hold values from 0.05 to 0.95
- log_sums: float32 [2, 32, 16384], P(None, 'tp', 'kv'), may hold values from 1 to 7
- chosen: int32 [8, 128, 16], P('tp', 'kv'), may hold values from 0 to 511, as said below
- out_grad: bfloat16 [16384, 4096], P('kv', 'tp'), may hold values from -6 to 6
Outputs:
- grad_queries: bfloat16 [16384, 4096], P('kv', 'tp')
- grad_keys: bfloat16 [16384, 1024], P('kv', 'tp')
- grad_values: bfloat16 [16384, 1024], P('kv', 'tp')
- grad_weight: float32 [4096, 4096], P('kv', 'tp')
The draws below stay inside these ranges and needn't reach their ends.
Inputs may be any that keep to these rules, and one draw needn't show every extreme that they name: `chosen`: each list names distinct key blocks, among them the blocks that cover the query block's own rows; blocks past a query's position may be named and carry no weight for it. For one key head, the lists of the query blocks of one index of kv name at most 16 key blocks (counted with repetition) that lie at any one other index of kv.
All inputs are finite; a program needn't handle non-finite values.
Results may differ from the reference program's by a relative error of at most 0.011.
Values may be sent and summed in bfloat16 or wider, within the bound.
A program may use at most 128 MiB of HBM per device.

```python
import jax
import jax.numpy as jnp
from jax import lax

MODEL = 4096
HEADS = 32
KV_HEADS = 8
HEAD_DIM = 128
TOK_DEV = 1024
QUERY_BLOCK = 128
KEY_BLOCK = 32
POOL_BLOCK = 32
CHOSEN = 16
SEQ = 16384


def block_shared_rows(key):
    width = KV_HEADS * HEAD_DIM
    pool_count = SEQ // POOL_BLOCK
    key_parts = jax.random.split(key, 2)
    common = 0.8 * jax.random.normal(key_parts[0], (pool_count, 1, width), jnp.float32)
    rough = 0.6 * jax.random.normal(key_parts[1], (pool_count, POOL_BLOCK, width), jnp.float32)
    rows = jnp.clip((common + rough).reshape(SEQ, width), -6.0, 6.0)
    return rows.astype(jnp.bfloat16)


def draw_key_rows(key, part):
    return block_shared_rows(jax.random.fold_in(key, 31))


def draw_value_rows(key, part):
    return block_shared_rows(jax.random.fold_in(key, 37))


def draw_log_sums(key, part):
    key_parts = jax.random.split(jax.random.fold_in(key, 17), 2)
    seen_count = (jnp.arange(SEQ, dtype=jnp.int32) + 1) // POOL_BLOCK
    pool_level = jnp.log((seen_count + 3).astype(jnp.float32))[None, None, :]
    pooled_part = jnp.minimum(pool_level + jax.random.uniform(key_parts[0], (1, HEADS, SEQ), jnp.float32, 0.25, 0.75), 7.0)
    chosen_part = jax.random.uniform(key_parts[1], (1, HEADS, SEQ), jnp.float32, 5.0, 7.0)
    return jnp.concatenate([pooled_part, chosen_part], axis=0).astype(jnp.float32)


def draw_chosen(key, part):
    devices = SEQ // TOK_DEV
    per_device = TOK_DEV // QUERY_BLOCK
    blocks_here = TOK_DEV // KEY_BLOCK
    own_count = QUERY_BLOCK // KEY_BLOCK
    query_blocks = SEQ // QUERY_BLOCK
    free_owners = (CHOSEN - own_count) // 2 - 2
    pair_count = free_owners + 2
    key_parts = jax.random.split(key, 6)
    block_ids = jnp.arange(query_blocks, dtype=jnp.int32)
    device_of = block_ids // per_device
    owner_ids = jnp.arange(devices, dtype=jnp.int32)
    before = (device_of - 1) % devices
    across = (device_of + devices // 2) % devices
    hot_owner = jax.random.randint(key_parts[0], (KV_HEADS, 1, 1), 0, devices)
    owner_score = jax.random.randint(key_parts[1], (KV_HEADS, query_blocks, devices), 0, 1000)
    owner_score = owner_score + jnp.where(owner_ids[None, None, :] == hot_owner, 2000, 0)
    banned = (owner_ids[None, :] == device_of[:, None]) | (owner_ids[None, :] == before[:, None]) | (owner_ids[None, :] == across[:, None])
    owner_score = jnp.where(banned[None], -1, owner_score) * devices + owner_ids[None, None, :]
    _, drawn_owners = lax.top_k(owner_score, free_owners)
    fixed_owners = jnp.broadcast_to(jnp.stack([before, across], axis=-1)[None], (KV_HEADS, query_blocks, 2))
    pair_owners = jnp.concatenate([fixed_owners, drawn_owners.astype(jnp.int32)], axis=-1)
    shape = (KV_HEADS, query_blocks, pair_count)
    first_pick = jnp.minimum(jax.random.randint(key_parts[2], shape, 0, blocks_here), jax.random.randint(key_parts[3], shape, 0, blocks_here))
    second_pick = (first_pick + 1 + jax.random.randint(key_parts[4], shape, 0, blocks_here - 1)) % blocks_here
    others = jnp.concatenate([pair_owners * blocks_here + first_pick, pair_owners * blocks_here + second_pick], axis=-1)
    own_blocks = block_ids[:, None] * own_count + jnp.arange(own_count, dtype=jnp.int32)[None, :]
    own_blocks = jnp.broadcast_to(own_blocks[None], (KV_HEADS, query_blocks, own_count))
    block_lists = jnp.concatenate([own_blocks, others], axis=-1).astype(jnp.int32)
    sort_keys = jax.random.randint(key_parts[5], (KV_HEADS, query_blocks, CHOSEN), 0, 1 << 20) * CHOSEN + jnp.arange(CHOSEN, dtype=jnp.int32)
    reorder = jnp.argsort(sort_keys, axis=-1)
    return jnp.take_along_axis(block_lists, reorder, axis=-1).astype(jnp.int32)


def levels(rng, extent, shards, low, largest):
    def one(dim, blocks):
        steps = jax.random.uniform(jax.random.fold_in(jax.random.fold_in(rng, 6), dim), (blocks,), jnp.float32, low / len(shards), largest / len(shards))
        return jnp.repeat(jnp.exp(steps), extent[dim] // blocks).reshape((-1,) + (1,) * (len(extent) - dim - 1))

    factor_of = one(*shards[0])
    for cut in shards[1:]:
        factor_of = factor_of * one(*cut)
    return factor_of


def scatter_about(key, shape, deviation, reach, cuts=(), held_as=jnp.bfloat16):
    entries = deviation * jax.random.normal(key, shape, jnp.float32)
    if cuts:
        entries = entries * levels(key, shape, cuts, -0.22, 0.18)
    return jnp.clip(entries, -reach, reach).astype(held_as)


def setup_inputs(seed: int = 0) -> dict:
    arg_keys = jax.random.split(jax.random.key(seed), 9)
    return {
        "hidden_rows": scatter_about(arg_keys[0], (SEQ, MODEL), 1.0, 6.0, ((0, 128),)),
        "queries": scatter_about(arg_keys[1], (SEQ, HEADS * HEAD_DIM), 1.0, 6.0, ((0, 16), (1, 8))),
        "key_rows": draw_key_rows(jax.random.fold_in(arg_keys[8], 71), 0),
        "value_rows": draw_value_rows(jax.random.fold_in(arg_keys[8], 71), 0),
        "branch_gates": jnp.clip(0.05 + 0.9 * jax.random.uniform(arg_keys[4], (2, HEADS, SEQ), jnp.float32) ** levels(arg_keys[4], (2, HEADS, SEQ), ((1, 8), (2, 16)), -0.2, 0.2), 0.05, 0.95),
        "log_sums": draw_log_sums(jax.random.fold_in(arg_keys[8], 71), 0),
        "chosen": draw_chosen(jax.random.fold_in(arg_keys[8], 71), 0),
        "out_grad": scatter_about(arg_keys[7], (SEQ, HEADS * HEAD_DIM), 1.0, 6.0, ((0, 16), (1, 8))),
    }


def rounded(value):
    return lax.optimization_barrier(value.astype(jnp.bfloat16)).astype(jnp.float32)


def attend_back(query_rows, key_set, value_set, cotangent, log_sum, visible, score_scale):
    query_wide = query_rows.astype(jnp.float32)
    key_wide = key_set.astype(jnp.float32)
    value_wide = value_set.astype(jnp.float32)
    scores = jnp.einsum('grd,md->grm', query_wide, key_wide) * score_scale
    weights = jnp.where(visible[None], jnp.exp(scores - log_sum[:, :, None]), 0.0)
    weights_low = rounded(weights)
    branch_out = jnp.einsum('grm,md->grd', weights_low, value_wide)
    row_delta = jnp.sum(cotangent * branch_out, axis=-1)
    grad_prob = jnp.einsum('grd,md->grm', cotangent, value_wide)
    dscore = rounded(weights * (grad_prob - row_delta[:, :, None]))
    dquery = jnp.einsum('grm,md->grd', dscore, key_wide) * score_scale
    grad_key = jnp.einsum('grm,grd->md', dscore, query_wide) * score_scale
    grad_value = jnp.einsum('grm,grd->md', weights_low, cotangent)
    return dquery, grad_key, grad_value


def reference(hidden_rows, queries, key_rows, value_rows, branch_gates, log_sums, chosen, out_grad):
    seq_len = queries.shape[0]
    group_size = HEADS // KV_HEADS
    score_scale = HEAD_DIM ** -0.5
    pool_count = seq_len // POOL_BLOCK
    query_blocks = seq_len // QUERY_BLOCK
    positions = jnp.arange(seq_len, dtype=jnp.int32)
    pool_end = jnp.arange(pool_count, dtype=jnp.int32) * POOL_BLOCK + POOL_BLOCK - 1
    pool_visible = pool_end[None, :] <= positions[:, None]
    block_offsets = jnp.arange(KEY_BLOCK, dtype=jnp.int32)
    query_offsets = jnp.arange(QUERY_BLOCK, dtype=jnp.int32)

    def per_head(which_head):
        key_cols = lax.dynamic_slice_in_dim(key_rows, which_head * HEAD_DIM, HEAD_DIM, 1)
        value_cols = lax.dynamic_slice_in_dim(value_rows, which_head * HEAD_DIM, HEAD_DIM, 1)
        first_col = which_head * group_size * HEAD_DIM
        query_cols = lax.dynamic_slice_in_dim(queries, first_col, group_size * HEAD_DIM, 1)
        query_cols = query_cols.reshape(seq_len, group_size, HEAD_DIM).transpose(1, 0, 2)
        grad_cols = lax.dynamic_slice_in_dim(out_grad, first_col, group_size * HEAD_DIM, 1)
        grad_cols = grad_cols.reshape(seq_len, group_size, HEAD_DIM).transpose(1, 0, 2).astype(jnp.float32)
        gate_cols = lax.dynamic_slice_in_dim(branch_gates, which_head * group_size, group_size, 1)
        sum_cols = lax.dynamic_slice_in_dim(log_sums, which_head * group_size, group_size, 1)
        pooled_keys = jnp.mean(key_cols.astype(jnp.float32).reshape(pool_count, POOL_BLOCK, HEAD_DIM), axis=1).astype(jnp.bfloat16)
        pooled_values = jnp.mean(value_cols.astype(jnp.float32).reshape(pool_count, POOL_BLOCK, HEAD_DIM), axis=1).astype(jnp.bfloat16)
        cot_pool = rounded(gate_cols[0][:, :, None] * grad_cols)
        cot_chosen = rounded(gate_cols[1][:, :, None] * grad_cols)
        pool_dquery, pool_dkeys, pool_dvalues = attend_back(query_cols, pooled_keys, pooled_values, cot_pool, sum_cols[0], pool_visible, score_scale)
        head_lists = lax.dynamic_index_in_dim(chosen, which_head, 0, keepdims=False)

        def one_block(totals, block_index):
            key_total, value_total = totals
            picked = lax.dynamic_index_in_dim(head_lists, block_index, 0, keepdims=False)
            key_index = (picked[:, None] * KEY_BLOCK + block_offsets[None, :]).reshape(-1).astype(jnp.int32)
            row_start = (block_index * QUERY_BLOCK).astype(jnp.int32)
            query_part = lax.dynamic_slice_in_dim(query_cols, row_start, QUERY_BLOCK, 1)
            cot_part = lax.dynamic_slice_in_dim(cot_chosen, row_start, QUERY_BLOCK, 1)
            sum_part = lax.dynamic_slice_in_dim(sum_cols[1], row_start, QUERY_BLOCK, 1)
            visible = key_index[None, :] <= (row_start + query_offsets)[:, None]
            dquery, grad_key, grad_value = attend_back(query_part, key_cols[key_index], value_cols[key_index], cot_part, sum_part, visible, score_scale)
            return (key_total.at[key_index].add(grad_key), value_total.at[key_index].add(grad_value)), dquery

        empty_rows = jnp.zeros((seq_len, HEAD_DIM), jnp.float32)
        (pick_dkeys, pick_dvalues), pick_dquery = lax.scan(one_block, (empty_rows, empty_rows), jnp.arange(query_blocks, dtype=jnp.int32))
        pick_dquery = pick_dquery.transpose(1, 0, 2, 3).reshape(group_size, seq_len, HEAD_DIM)
        head_query = (pool_dquery + pick_dquery).astype(jnp.bfloat16).transpose(1, 0, 2).reshape(seq_len, group_size * HEAD_DIM)
        head_key = (pick_dkeys + jnp.repeat(pool_dkeys, POOL_BLOCK, axis=0) / POOL_BLOCK).astype(jnp.bfloat16)
        head_value = (pick_dvalues + jnp.repeat(pool_dvalues, POOL_BLOCK, axis=0) / POOL_BLOCK).astype(jnp.bfloat16)
        return head_query, head_key, head_value

    head_queries, head_keys, head_values = lax.map(per_head, jnp.arange(KV_HEADS, dtype=jnp.int32))
    grad_queries = head_queries.transpose(1, 0, 2).reshape(seq_len, HEADS * HEAD_DIM)
    grad_keys = head_keys.transpose(1, 0, 2).reshape(seq_len, KV_HEADS * HEAD_DIM)
    grad_values = head_values.transpose(1, 0, 2).reshape(seq_len, KV_HEADS * HEAD_DIM)
    grad_weight = jnp.dot(hidden_rows.T, grad_queries, preferred_element_type=jnp.float32)
    return grad_queries, grad_keys, grad_values, grad_weight
```

```python
import jax
import jax.numpy as jnp
from jax import lax
from jax.experimental import pallas as pl
from jax.experimental.pallas import tpu as pltpu
from jax.sharding import PartitionSpec as P

HEADS = 32
KV_HEADS = 8
HEAD_DIM = 128
QUERY_BLOCK = 128
KEY_BLOCK = 32
POOL_BLOCK = 32
CHOSEN = 16
GROUP = HEADS // KV_HEADS
SIDE = 4
OWNERS = SIDE * SIDE
TOKENS = 1024
BLOCKS = TOKENS // QUERY_BLOCK
POOLED = TOKENS // POOL_BLOCK
SEQ = TOKENS * OWNERS
MODEL = 4096
SCALE = HEAD_DIM ** (-0.5)
LOG2E = 1.4426950408889634
MESH = pl.DeviceIdType.MESH
F32 = jnp.float32
BF16 = jnp.bfloat16

NT = (((1,), (1,)), ((), ()))
NN = (((1,), (0,)), ((), ()))


def dot(a, b, dims):
    return lax.dot_general(a, b, dims, preferred_element_type=F32)


class Sender:
    def __init__(self, send_sems, recv_sems):
        self.send_sems, self.recv_sems, self.at, self.sent = send_sems, recv_sems, 0, []

    def __call__(self, src, dst, dev):
        copy = pltpu.make_async_remote_copy(
            src_ref=src,
            dst_ref=dst,
            send_sem=self.send_sems.at[self.at],
            recv_sem=self.recv_sems.at[self.at],
            device_id=dev,
            device_id_type=MESH,
        )
        self.at += 1
        copy.start()
        self.sent.append(copy)
        return copy

    def finish(self):
        for copy in self.sent:
            copy.wait_send()


def place():
    kv, tp = lax.axis_index("kv"), lax.axis_index("tp")
    return kv, tp, kv // SIDE, kv % SIDE, tp // 2, tp % 2


def shifted(c, o):
    return (c + (o + SIDE)) % SIDE


def meet(devices):
    barrier = pltpu.get_barrier_semaphore()
    for dev in devices:
        pl.semaphore_signal(barrier, inc=1, device_id=dev, device_id_type=MESH)
    pl.semaphore_wait(barrier, len(devices))


def tile_operands(q_ref, g_ref, gate_ref, ls_ref, branch, t):
    rows = pl.ds(pl.multiple_of(t * QUERY_BLOCK, QUERY_BLOCK), QUERY_BLOCK)
    gates = jnp.concatenate([gate_ref[0, :, rows], gate_ref[1, :, rows]], axis=0).T
    qs, cs, ls = [], [], []
    for h in range(GROUP):
        cols = slice(h * HEAD_DIM, (h + 1) * HEAD_DIM)
        qs.append(q_ref[rows, cols])
        at = branch * GROUP + h
        cs.append((gates[:, at : at + 1] * g_ref[rows, cols].astype(F32)).astype(BF16))
        ls.append(ls_ref[branch, h : h + 1, rows])
    return (
        jnp.concatenate(qs, axis=0),
        jnp.concatenate(cs, axis=0),
        jnp.concatenate(ls, axis=1) * LOG2E,
    )


def attend_back(qs, cs, log_sum, keys, values, visible):
    scores = dot(keys, qs, NT) * (SCALE * LOG2E)
    p = jnp.where(visible, jnp.exp2(scores - log_sum), 0.0)
    pr = p.astype(BF16)
    dp = dot(values, cs, NT)
    delta = jnp.sum(pr.astype(F32) * dp, axis=0, keepdims=True)
    ds = (p * (dp - delta)).astype(BF16)
    return dot(keys.T, ds, NN), dot(ds, qs, NN), dot(pr, cs, NN)


def gather_kernel(
    k_ref, v_ref, h_ref, q_ref, g_ref, gate_ref, ls_ref,
    k_all, v_all, h_all, dq_ref, dpk_ref, dpv_ref,
    pool_all, pk_ref, pv_ref, pool_here,
    pool_send, pool_recv, send_sems, recv_sems, local_sems,
):
    kv, tp, cz, cy, cx, core = place()
    half = TOKENS // 2

    def device(oz, oy):
        return (shifted(cz, oz) * SIDE + shifted(cy, oy), tp)

    def along(axis, o):
        return device(o, 0) if axis == 0 else device(0, o)

    def owner(axis, o1, o2):
        a, b = (o1, o2) if axis == 0 else (o2, o1)
        return shifted(cz, a) * SIDE + shifted(cy, b)

    def xdev(o, c):
        return (kv, shifted(cx, o) * 2 + c)

    local = [
        pltpu.make_async_copy(k_ref, k_all.at[kv], local_sems.at[0]),
        pltpu.make_async_copy(v_ref, v_all.at[kv], local_sems.at[1]),
        pltpu.make_async_copy(h_ref, h_all.at[tp], local_sems.at[2]),
    ]
    for copy in local:
        copy.start()

    blk = lax.broadcasted_iota(jnp.int32, (POOLED, TOKENS), 0)
    row = lax.broadcasted_iota(jnp.int32, (POOLED, TOKENS), 1)
    mean = jnp.where(row // POOL_BLOCK == blk, 1.0 / POOL_BLOCK, 0.0).astype(BF16)
    pool_here[0] = dot(mean, k_ref[...], NN).astype(BF16)
    pool_here[1] = dot(mean, v_ref[...], NN).astype(BF16)

    others = [(oz, oy) for oz in range(SIDE) for oy in range(SIDE) if (oz, oy) != (0, 0)]
    meet([device(oz, oy) for oz, oy in others] + [xdev(1, core), xdev(-1, core), xdev(0, 1 - core)])

    pool_sender = Sender(pool_send, pool_recv)
    for oz, oy in others:
        pool_sender(pool_here, pool_all.at[kv], device(oz, oy))
    pool_all[kv] = pool_here[...]

    send = Sender(send_sems, recv_sems)
    first, wide = {}, {}
    arrays = ((0, k_ref, k_all), (1, v_ref, v_all))
    for axis, here, full in arrays:
        first[axis] = [send(here, full.at[kv], along(axis, s)) for s in (1, -1)]
    x_first = [send(h_ref, h_all.at[tp], xdev(s, core)) for s in (1, -1)]
    x_over = [send(h_ref, h_all.at[tp], xdev(0, 1 - core))]
    for axis, here, full in arrays:
        wide[axis] = [(0, [send(here, full.at[kv], along(1 - axis, s)) for s in (1, -1)])]

    for copy in pool_sender.sent:
        copy.wait_recv()
    pk_ref[...] = pool_all[:, 0].reshape(OWNERS * POOLED, HEAD_DIM)
    pv_ref[...] = pool_all[:, 1].reshape(OWNERS * POOLED, HEAD_DIM)
    dpk_ref[...] = jnp.zeros_like(dpk_ref)
    dpv_ref[...] = jnp.zeros_like(dpv_ref)

    n_pool = OWNERS * POOLED
    wide_q = GROUP * QUERY_BLOCK
    pool_end = lax.broadcasted_iota(jnp.int32, (n_pool, wide_q), 0) * POOL_BLOCK + POOL_BLOCK - 1
    lane = lax.broadcasted_iota(jnp.int32, (n_pool, wide_q), 1) % QUERY_BLOCK
    ahead = pool_end - lane

    def tile(t, carry):
        qs, cs, log_sum = tile_operands(q_ref, g_ref, gate_ref, ls_ref, 0, t)
        visible = ahead <= kv * TOKENS + t * QUERY_BLOCK
        dq, dk, dv = attend_back(qs, cs, log_sum, pk_ref[...], pv_ref[...], visible)
        dq_ref[t] = dq
        dpk_ref[...] += dk
        dpv_ref[...] += dv
        return carry

    lax.fori_loop(0, 4, tile, 0)

    second = {}
    for axis, here, full in arrays:
        plus, minus = first[axis]
        plus.wait_recv()
        part = full.at[owner(axis, -1, 0), pl.ds(0, half)]
        fwd = send(part, part, along(axis, 1))
        whole = full.at[owner(axis, -1, 0)]
        wide[axis].append((-1, [send(whole, whole, along(1 - axis, s)) for s in (1, -1)]))
        minus.wait_recv()
        part = full.at[owner(axis, 1, 0), pl.ds(half, half)]
        bwd = send(part, part, along(axis, -1))
        whole = full.at[owner(axis, 1, 0)]
        wide[axis].append((1, [send(whole, whole, along(1 - axis, s)) for s in (1, -1)]))
        second[axis] = (fwd, bwd)

    lax.fori_loop(4, BLOCKS, tile, 0)
    dpk_ref[...] = dpk_ref[...] * SCALE

    last = []

    def across(axis, full, o, pair):
        plus, minus = pair
        plus.wait_recv()
        part = full.at[owner(axis, o, -1), pl.ds(0, half)]
        last.append(send(part, part, along(1 - axis, 1)))
        minus.wait_recv()
        part = full.at[owner(axis, o, 1), pl.ds(half, half)]
        last.append(send(part, part, along(1 - axis, -1)))

    for axis, here, full in arrays:
        across(axis, full, *wide[axis][0])
    for axis, here, full in arrays:
        for copy in second[axis]:
            copy.wait_recv()
        whole = full.at[owner(axis, 2, 0)]
        wide[axis].append((2, [send(whole, whole, along(1 - axis, s)) for s in (1, -1)]))
    rows = h_ref.shape[0] // 2
    plus, minus = x_first
    plus.wait_recv()
    whole = h_all.at[shifted(cx, -1) * 2 + core]
    part = whole.at[pl.ds(0, rows)]
    x_second = [send(part, part, xdev(1, core))]
    x_over.append(send(whole, whole, xdev(0, 1 - core)))
    minus.wait_recv()
    whole = h_all.at[shifted(cx, 1) * 2 + core]
    part = whole.at[pl.ds(rows, rows)]
    x_second.append(send(part, part, xdev(-1, core)))
    x_over.append(send(whole, whole, xdev(0, 1 - core)))
    for i in (1, 2):
        for axis, here, full in arrays:
            across(axis, full, *wide[axis][i])
    for copy in x_second:
        copy.wait_recv()
    whole = h_all.at[shifted(cx, 2) * 2 + core]
    x_over.append(send(whole, whole, xdev(0, 1 - core)))
    for axis, here, full in arrays:
        across(axis, full, *wide[axis][3])
    for copy in last:
        copy.wait_recv()
    for copy in x_over:
        copy.wait_recv()
    pool_sender.finish()
    send.finish()
    for copy in local:
        copy.wait()


GATHER_COPIES = 2 * (2 + 2 + 8 + 8) + 2 + 2 + 4


def run_gather(k, v, h, q, g, gates, sums):
    any_spec = pl.BlockSpec(memory_space=pl.ANY)
    vmem = pl.BlockSpec(memory_space=pltpu.VMEM)
    n_pool = OWNERS * POOLED
    return pl.pallas_call(
        gather_kernel,
        name="gather",
        out_shape=(
            jax.ShapeDtypeStruct((OWNERS, TOKENS, HEAD_DIM), BF16),
            jax.ShapeDtypeStruct((OWNERS, TOKENS, HEAD_DIM), BF16),
            jax.ShapeDtypeStruct((8, TOKENS // 8, MODEL), BF16),
            jax.ShapeDtypeStruct((BLOCKS, HEAD_DIM, GROUP * QUERY_BLOCK), F32),
            jax.ShapeDtypeStruct((n_pool, HEAD_DIM), F32),
            jax.ShapeDtypeStruct((n_pool, HEAD_DIM), F32),
        ),
        in_specs=[vmem] * 7,
        out_specs=(any_spec, any_spec, any_spec, vmem, vmem, vmem),
        scratch_shapes=[
            pltpu.VMEM((OWNERS, 2, POOLED, HEAD_DIM), BF16),
            pltpu.VMEM((n_pool, HEAD_DIM), BF16),
            pltpu.VMEM((n_pool, HEAD_DIM), BF16),
            pltpu.VMEM((2, POOLED, HEAD_DIM), BF16),
            pltpu.SemaphoreType.DMA((OWNERS - 1,)),
            pltpu.SemaphoreType.DMA((OWNERS - 1,)),
            pltpu.SemaphoreType.DMA((GATHER_COPIES,)),
            pltpu.SemaphoreType.DMA((GATHER_COPIES,)),
            pltpu.SemaphoreType.DMA((3,)),
        ],
        compiler_params=pltpu.CompilerParams(collective_id=0, has_side_effects=True),
    )(k, v, h, q, g, gates, sums)


def chosen_kernel(
    chosen_ref, k_ref, v_ref, q_ref, g_ref, gate_ref, ls_ref, dqp_ref, dpk_ref, dpv_ref,
    gq_ref, gqt_ref, dk_ref, dv_ref,
    acc_k, acc_v, kb, vb,
):
    kv = lax.axis_index("kv")
    n_pool = OWNERS * POOLED

    def start(i, carry):
        at = pl.multiple_of(i * 8, 8)
        for acc, pooled in ((acc_k, dpk_ref), (acc_v, dpv_ref)):
            part = pooled[pl.ds(at, 8), :] * (1.0 / POOL_BLOCK)
            rows = jnp.broadcast_to(part[:, None, :], (8, POOL_BLOCK, HEAD_DIM))
            acc[pl.ds(pl.multiple_of(at * POOL_BLOCK, 8 * POOL_BLOCK), 8 * POOL_BLOCK), :] = (
                rows.reshape(8 * POOL_BLOCK, HEAD_DIM)
            )
        return carry

    lax.fori_loop(0, n_pool // 8, start, 0)

    wide_q = GROUP * QUERY_BLOCK
    ahead = (
        lax.broadcasted_iota(jnp.int32, (KEY_BLOCK, wide_q), 0)
        - lax.broadcasted_iota(jnp.int32, (KEY_BLOCK, wide_q), 1) % QUERY_BLOCK
    )

    def block(b, carry):
        qs, cs, log_sum = tile_operands(q_ref, g_ref, gate_ref, ls_ref, 1, b)
        start_row = kv * TOKENS + b * QUERY_BLOCK
        seen, at = [], []
        for c in range(CHOSEN):
            first = pl.multiple_of(chosen_ref[b, c] * KEY_BLOCK, KEY_BLOCK)
            at.append(first)
            kb[pl.ds(c * KEY_BLOCK, KEY_BLOCK), :] = k_ref[pl.ds(first, KEY_BLOCK), :]
            vb[pl.ds(c * KEY_BLOCK, KEY_BLOCK), :] = v_ref[pl.ds(first, KEY_BLOCK), :]
            seen.append(ahead <= start_row - first)
        visible = jnp.concatenate(seen, axis=0)
        dq, dk, dv = attend_back(qs, cs, log_sum, kb[...], vb[...], visible)
        dk = dk * SCALE
        total = (dqp_ref[b] + dq) * SCALE
        rows = pl.ds(pl.multiple_of(b * QUERY_BLOCK, QUERY_BLOCK), QUERY_BLOCK)
        for h in range(GROUP):
            cols = slice(h * HEAD_DIM, (h + 1) * HEAD_DIM)
            part = total[:, cols]
            gqt_ref[cols, rows] = part.astype(BF16)
            gq_ref[rows, cols] = part.T.astype(BF16)
        for c in range(CHOSEN):
            here = pl.ds(at[c], KEY_BLOCK)
            piece = slice(c * KEY_BLOCK, (c + 1) * KEY_BLOCK)
            acc_k[here, :] += dk[piece]
            acc_v[here, :] += dv[piece]
        return carry

    lax.fori_loop(0, BLOCKS, block, 0)

    def finish(i, carry):
        rows = pl.ds(pl.multiple_of(i * 512, 512), 512)
        dk_ref[rows, :] = acc_k[rows, :].astype(BF16)
        dv_ref[rows, :] = acc_v[rows, :].astype(BF16)
        return carry

    lax.fori_loop(0, SEQ // 512, finish, 0)


def run_chosen(chosen, k_all, v_all, q, g, gates, sums, dqp, dpk, dpv):
    vmem = pl.BlockSpec(memory_space=pltpu.VMEM)
    smem = pl.BlockSpec(memory_space=pltpu.SMEM)
    return pl.pallas_call(
        chosen_kernel,
        name="chosen",
        out_shape=(
            jax.ShapeDtypeStruct((TOKENS, GROUP * HEAD_DIM), BF16),
            jax.ShapeDtypeStruct((GROUP * HEAD_DIM, TOKENS), BF16),
            jax.ShapeDtypeStruct((SEQ, HEAD_DIM), BF16),
            jax.ShapeDtypeStruct((SEQ, HEAD_DIM), BF16),
        ),
        in_specs=[smem] + [vmem] * 9,
        out_specs=(vmem,) * 4,
        scratch_shapes=[
            pltpu.VMEM((SEQ, HEAD_DIM), F32),
            pltpu.VMEM((SEQ, HEAD_DIM), F32),
            pltpu.VMEM((CHOSEN * KEY_BLOCK, HEAD_DIM), BF16),
            pltpu.VMEM((CHOSEN * KEY_BLOCK, HEAD_DIM), BF16),
        ],
    )(chosen, k_all, v_all, q, g, gates, sums, dqp, dpk, dpv)


class Reduce:
    def __init__(self, send, axis, src, bufs, coords, along):
        (self.relay, self.direct, self.comb, self.out, self.total,
         self.relay2, self.direct2, self.comb2, self.out2) = bufs
        self.send, self.axis, self.src = send, axis, src
        self.c1, self.c2 = (coords[0], coords[1]) if axis == 0 else (coords[1], coords[0])
        self.to1 = lambda o: along(axis, o)
        self.to2 = lambda o: along(1 - axis, o)
        self.half = src.shape[2] // 2
        self.lo, self.hi = pl.ds(0, self.half), pl.ds(self.half, self.half)

    def bundle(self, o, rows):
        c = shifted(self.c1, o)
        return self.src.at[c, :, rows] if self.axis == 0 else self.src.at[:, c, rows]

    def piece(self, o, i, rows):
        c = shifted(self.c1, o)
        if self.axis == 0:
            return self.src[c, i, rows, :]
        return self.src[i, c, rows, :]

    def part(self, o, rows):
        return self.total.at[shifted(self.c2, o), rows]

    def begin(self):
        s = self.send
        self.r = [
            s(self.bundle(2, self.lo), self.relay.at[0], self.to1(1)),
            s(self.bundle(2, self.hi), self.relay.at[1], self.to1(-1)),
        ]
        self.d = [
            s(self.bundle(1, self.hi), self.direct.at[0], self.to1(1)),
            s(self.bundle(-1, self.lo), self.direct.at[1], self.to1(-1)),
        ]

    def combine(self):
        self.c = []
        for n, (o, rows) in enumerate(((1, self.lo), (-1, self.hi))):
            self.r[n].wait_recv()

            def add(i, carry, n=n, o=o, rows=rows):
                self.out[n, i] = (
                    self.piece(o, i, rows).astype(F32) + self.relay[n, i].astype(F32)
                ).astype(BF16)
                return carry

            lax.fori_loop(0, SIDE, add, 0)
            self.c.append(self.send(self.out.at[n], self.comb.at[n], self.to1(o)))

    def turn(self):
        for copy in self.d + self.c:
            copy.wait_recv()

        def add(i, carry):
            self.total[i, self.lo, :] = (
                self.piece(0, i, self.lo).astype(F32)
                + self.comb[0, i].astype(F32)
                + self.direct[1, i].astype(F32)
            ).astype(BF16)
            self.total[i, self.hi, :] = (
                self.piece(0, i, self.hi).astype(F32)
                + self.comb[1, i].astype(F32)
                + self.direct[0, i].astype(F32)
            ).astype(BF16)
            return carry

        lax.fori_loop(0, SIDE, add, 0)
        s = self.send
        self.r = [
            s(self.part(2, self.lo), self.relay2.at[0], self.to2(1)),
            s(self.part(2, self.hi), self.relay2.at[1], self.to2(-1)),
        ]
        self.d = [
            s(self.part(1, self.hi), self.direct2.at[0], self.to2(1)),
            s(self.part(-1, self.lo), self.direct2.at[1], self.to2(-1)),
        ]

    def combine2(self):
        self.c = []
        for n, (o, rows) in enumerate(((1, self.lo), (-1, self.hi))):
            self.r[n].wait_recv()
            self.out2[n] = (
                self.total[shifted(self.c2, o), rows, :].astype(F32) + self.relay2[n].astype(F32)
            ).astype(BF16)
            self.c.append(self.send(self.out2.at[n], self.comb2.at[n], self.to2(o)))

    def end(self):
        for copy in self.d + self.c:
            copy.wait_recv()
        own = self.c2
        low = (
            self.total[own, self.lo, :].astype(F32)
            + self.comb2[0].astype(F32)
            + self.direct2[1].astype(F32)
        )
        high = (
            self.total[own, self.hi, :].astype(F32)
            + self.comb2[1].astype(F32)
            + self.direct2[0].astype(F32)
        )
        return low, high


def reduce_buffers(rows, lanes):
    half = rows // 2
    wide = pltpu.VMEM((2, SIDE, half, lanes), BF16)
    slim = pltpu.VMEM((2, half, lanes), BF16)
    return [wide] * 4 + [pltpu.VMEM((SIDE, rows, lanes), BF16)] + [slim] * 4


REDUCE_BUFS = 9
GW_ROWS = GROUP * HEAD_DIM // 2
GW_COLS = MODEL // OWNERS


def scatter_kernel(dk_ref, dv_ref, h_ref, gqt_ref, gk_out, gv_out, gw_out, gw0, gw1, *rest):
    bufs = [rest[i * REDUCE_BUFS : (i + 1) * REDUCE_BUFS] for i in range(4)]
    send_sems, recv_sems = rest[4 * REDUCE_BUFS :]
    kv, tp, cz, cy, cx, core = place()

    def along(axis, o):
        if axis == 0:
            return (shifted(cz, o) * SIDE + cy, tp)
        return (cz * SIDE + shifted(cy, o), tp)

    meet([along(axis, o) for axis in (0, 1) for o in (1, -1)])
    send = Sender(send_sems, recv_sems)
    rk, rv, w0, w1 = [
        Reduce(send, axis, src, buf, (cz, cy), along)
        for axis, src, buf in zip((0, 1, 0, 1), (dk_ref, dv_ref, gw0, gw1), bufs)
    ]
    rk.begin()
    rv.begin()

    def product(j, carry):
        cols = pl.ds(pl.multiple_of(j * GW_COLS, GW_COLS), GW_COLS)
        part = dot(gqt_ref[...], h_ref[:, cols], NN).astype(BF16)
        gw0[j // SIDE, j % SIDE] = part[:GW_ROWS]
        gw1[j // SIDE, j % SIDE] = part[GW_ROWS:]
        return carry

    lax.fori_loop(0, OWNERS, product, 0)
    rk.combine()
    rv.combine()
    w0.begin()
    w1.begin()
    rk.turn()
    rv.turn()
    w0.combine()
    w1.combine()
    rk.combine2()
    rv.combine2()
    w0.turn()
    w1.turn()
    half = TOKENS // 2
    for r, out in ((rk, gk_out), (rv, gv_out)):
        low, high = r.end()
        out[:half, :] = low.astype(BF16)
        out[half:, :] = high.astype(BF16)
    w0.combine2()
    w1.combine2()
    half = GW_ROWS // 2
    for n, r in enumerate((w0, w1)):
        low, high = r.end()
        gw_out[:, n * GW_ROWS : n * GW_ROWS + half] = low.T
        gw_out[:, n * GW_ROWS + half : (n + 1) * GW_ROWS] = high.T
    send.finish()


SCATTER_COPIES = 4 * 12


def run_scatter(dk, dv, h_all, gqt):
    vmem = pl.BlockSpec(memory_space=pltpu.VMEM)
    return pl.pallas_call(
        scatter_kernel,
        name="scatter",
        out_shape=(
            jax.ShapeDtypeStruct((TOKENS, HEAD_DIM), BF16),
            jax.ShapeDtypeStruct((TOKENS, HEAD_DIM), BF16),
            jax.ShapeDtypeStruct((GW_COLS, GROUP * HEAD_DIM), F32),
        ),
        in_specs=[vmem] * 4,
        out_specs=(vmem,) * 3,
        scratch_shapes=[
            pltpu.VMEM((SIDE, SIDE, GW_ROWS, GW_COLS), BF16),
            pltpu.VMEM((SIDE, SIDE, GW_ROWS, GW_COLS), BF16),
            *reduce_buffers(TOKENS, HEAD_DIM),
            *reduce_buffers(TOKENS, HEAD_DIM),
            *reduce_buffers(GW_ROWS, GW_COLS),
            *reduce_buffers(GW_ROWS, GW_COLS),
            pltpu.SemaphoreType.DMA((SCATTER_COPIES,)),
            pltpu.SemaphoreType.DMA((SCATTER_COPIES,)),
        ],
        compiler_params=pltpu.CompilerParams(collective_id=1, has_side_effects=True),
    )(dk, dv, h_all, gqt)


def body(hidden_rows, queries, key_rows, value_rows, branch_gates, log_sums, chosen, out_grad):
    k_all, v_all, h_all, dqp, dpk, dpv = run_gather(
        key_rows, value_rows, hidden_rows, queries, out_grad, branch_gates, log_sums
    )
    gq, gqt, dk, dv = run_chosen(
        chosen.reshape(BLOCKS, CHOSEN),
        k_all.reshape(SEQ, HEAD_DIM),
        v_all.reshape(SEQ, HEAD_DIM),
        queries, out_grad, branch_gates, log_sums, dqp, dpk, dpv,
    )
    plane = (SIDE, SIDE, TOKENS, HEAD_DIM)
    gk, gv, gw = run_scatter(
        dk.reshape(plane), dv.reshape(plane), h_all.reshape(TOKENS, MODEL), gqt
    )
    return gq, gk, gv, gw


def solution(mesh):
    placed = (
        P(("kv", "tp"), None),
        P("kv", "tp"),
        P("kv", "tp"),
        P("kv", "tp"),
        P(None, "tp", "kv"),
        P(None, "tp", "kv"),
        P("tp", "kv", None),
        P("kv", "tp"),
    )
    return jax.shard_map(
        body,
        mesh=mesh,
        in_specs=placed,
        out_specs=(P("kv", "tp"), P("kv", "tp"), P("kv", "tp"), P("kv", "tp")),
        check_vma=False,
    )
```

```python
import jax
import jax.numpy as jnp
from jax import lax
from jax.experimental import pallas as pl
from jax.experimental.pallas import tpu as pltpu
from jax.sharding import PartitionSpec as P

HEADS = 32
KV_HEADS = 8
HEAD_DIM = 128
QUERY_BLOCK = 128
KEY_BLOCK = 32
POOL_BLOCK = 32
CHOSEN = 16
GROUP = HEADS // KV_HEADS
SIDE = 4
OWNERS = SIDE * SIDE
TOKENS = 1024
BLOCKS = TOKENS // QUERY_BLOCK
POOLED = TOKENS // POOL_BLOCK
SEQ = TOKENS * OWNERS
MODEL = 4096
SCALE = HEAD_DIM ** (-0.5)
LOG2E = 1.4426950408889634
MIB = 1 << 20
MESH = pl.DeviceIdType.MESH
F32 = jnp.float32
BF16 = jnp.bfloat16

NT = (((1,), (1,)), ((), ()))
NN = (((1,), (0,)), ((), ()))


def dot(a, b, dims):
    return lax.dot_general(a, b, dims, preferred_element_type=F32)


class Sender:
    def __init__(self, send_sems, recv_sems):
        self.send_sems, self.recv_sems, self.at, self.sent = send_sems, recv_sems, 0, []

    def __call__(self, src, dst, dev):
        copy = pltpu.make_async_remote_copy(
            src_ref=src,
            dst_ref=dst,
            send_sem=self.send_sems.at[self.at],
            recv_sem=self.recv_sems.at[self.at],
            device_id=dev,
            device_id_type=MESH,
        )
        self.at += 1
        copy.start()
        self.sent.append(copy)
        return copy

    def finish(self):
        for copy in self.sent:
            copy.wait_send()


def place():
    kv, tp = lax.axis_index("kv"), lax.axis_index("tp")
    return kv, tp, kv // SIDE, kv % SIDE, tp // 2, tp % 2


def shifted(c, o):
    return (c + (o + SIDE)) % SIDE


def meet(devices):
    barrier = pltpu.get_barrier_semaphore()
    for dev in devices:
        pl.semaphore_signal(barrier, inc=1, device_id=dev, device_id_type=MESH)
    pl.semaphore_wait(barrier, len(devices))


def tile_operands(q_ref, g_ref, gate_ref, ls_ref, branch, t):
    rows = pl.ds(pl.multiple_of(t * QUERY_BLOCK, QUERY_BLOCK), QUERY_BLOCK)
    gates = jnp.concatenate([gate_ref[0, :, rows], gate_ref[1, :, rows]], axis=0).T
    qs, cs, ls = [], [], []
    for h in range(GROUP):
        cols = slice(h * HEAD_DIM, (h + 1) * HEAD_DIM)
        qs.append(q_ref[rows, cols])
        at = branch * GROUP + h
        cs.append((gates[:, at : at + 1] * g_ref[rows, cols].astype(F32)).astype(BF16))
        ls.append(ls_ref[branch, h : h + 1, rows])
    return (
        jnp.concatenate(qs, axis=0),
        jnp.concatenate(cs, axis=0),
        jnp.concatenate(ls, axis=1) * LOG2E,
    )


def attend_back(qs, cs, log_sum, keys, values, visible):
    scores = dot(keys, qs, NT) * (SCALE * LOG2E)
    p = jnp.where(visible, jnp.exp2(scores - log_sum), 0.0)
    pr = p.astype(BF16)
    dp = dot(values, cs, NT)
    delta = jnp.sum(pr.astype(F32) * dp, axis=0, keepdims=True)
    ds = (p * (dp - delta)).astype(BF16)
    return dot(keys.T, ds, NN), dot(ds, qs, NN), dot(pr, cs, NN)


def gather_kernel(
    k_ref, v_ref, h_ref, q_ref, g_ref, gate_ref, ls_ref,
    k_all, v_all, h_all, dq_ref, dpk_ref, dpv_ref,
    pool_all, pk_ref, pv_ref, pool_here,
    pool_send, pool_recv, send_sems, recv_sems, local_sems,
):
    kv, tp, cz, cy, cx, core = place()
    half = TOKENS // 2

    def device(oz, oy):
        return (shifted(cz, oz) * SIDE + shifted(cy, oy), tp)

    def along(axis, o):
        return device(o, 0) if axis == 0 else device(0, o)

    def owner(axis, o1, o2):
        a, b = (o1, o2) if axis == 0 else (o2, o1)
        return shifted(cz, a) * SIDE + shifted(cy, b)

    def xdev(o, c):
        return (kv, shifted(cx, o) * 2 + c)

    local = [
        pltpu.make_async_copy(k_ref, k_all.at[kv], local_sems.at[0]),
        pltpu.make_async_copy(v_ref, v_all.at[kv], local_sems.at[1]),
        pltpu.make_async_copy(h_ref, h_all.at[tp], local_sems.at[2]),
    ]
    for copy in local:
        copy.start()

    blk = lax.broadcasted_iota(jnp.int32, (POOLED, TOKENS), 0)
    row = lax.broadcasted_iota(jnp.int32, (POOLED, TOKENS), 1)
    mean = jnp.where(row // POOL_BLOCK == blk, 1.0 / POOL_BLOCK, 0.0).astype(BF16)
    pool_here[0] = dot(mean, k_ref[...], NN).astype(BF16)
    pool_here[1] = dot(mean, v_ref[...], NN).astype(BF16)

    others = [(oz, oy) for oz in range(SIDE) for oy in range(SIDE) if (oz, oy) != (0, 0)]
    meet([device(oz, oy) for oz, oy in others] + [xdev(1, core), xdev(-1, core), xdev(0, 1 - core)])

    pool_sender = Sender(pool_send, pool_recv)
    for oz, oy in others:
        pool_sender(pool_here, pool_all.at[kv], device(oz, oy))
    pool_all[kv] = pool_here[...]

    send = Sender(send_sems, recv_sems)
    first, wide = {}, {}
    arrays = ((0, k_ref, k_all), (1, v_ref, v_all))
    for axis, here, full in arrays:
        first[axis] = [send(here, full.at[kv], along(axis, s)) for s in (1, -1)]
    x_first = [send(h_ref, h_all.at[tp], xdev(s, core)) for s in (1, -1)]
    x_over = [send(h_ref, h_all.at[tp], xdev(0, 1 - core))]
    for axis, here, full in arrays:
        wide[axis] = [(0, [send(here, full.at[kv], along(1 - axis, s)) for s in (1, -1)])]

    for copy in pool_sender.sent:
        copy.wait_recv()
    pk_ref[...] = pool_all[:, 0].reshape(OWNERS * POOLED, HEAD_DIM)
    pv_ref[...] = pool_all[:, 1].reshape(OWNERS * POOLED, HEAD_DIM)
    dpk_ref[...] = jnp.zeros_like(dpk_ref)
    dpv_ref[...] = jnp.zeros_like(dpv_ref)

    n_pool = OWNERS * POOLED
    wide_q = GROUP * QUERY_BLOCK
    pool_end = lax.broadcasted_iota(jnp.int32, (n_pool, wide_q), 0) * POOL_BLOCK + POOL_BLOCK - 1
    lane = lax.broadcasted_iota(jnp.int32, (n_pool, wide_q), 1) % QUERY_BLOCK
    ahead = pool_end - lane

    def tile(t, carry):
        qs, cs, log_sum = tile_operands(q_ref, g_ref, gate_ref, ls_ref, 0, t)
        visible = ahead <= kv * TOKENS + t * QUERY_BLOCK
        dq, dk, dv = attend_back(qs, cs, log_sum, pk_ref[...], pv_ref[...], visible)
        dq_ref[t] = dq
        dpk_ref[...] += dk
        dpv_ref[...] += dv
        return carry

    lax.fori_loop(0, 4, tile, 0)

    second = {}
    for axis, here, full in arrays:
        plus, minus = first[axis]
        plus.wait_recv()
        part = full.at[owner(axis, -1, 0), pl.ds(0, half)]
        fwd = send(part, part, along(axis, 1))
        whole = full.at[owner(axis, -1, 0)]
        wide[axis].append((-1, [send(whole, whole, along(1 - axis, s)) for s in (1, -1)]))
        minus.wait_recv()
        part = full.at[owner(axis, 1, 0), pl.ds(half, half)]
        bwd = send(part, part, along(axis, -1))
        whole = full.at[owner(axis, 1, 0)]
        wide[axis].append((1, [send(whole, whole, along(1 - axis, s)) for s in (1, -1)]))
        second[axis] = (fwd, bwd)

    lax.fori_loop(4, BLOCKS, tile, 0)
    dpk_ref[...] = dpk_ref[...] * SCALE

    last = []

    def across(axis, full, o, pair):
        plus, minus = pair
        plus.wait_recv()
        part = full.at[owner(axis, o, -1), pl.ds(0, half)]
        last.append(send(part, part, along(1 - axis, 1)))
        minus.wait_recv()
        part = full.at[owner(axis, o, 1), pl.ds(half, half)]
        last.append(send(part, part, along(1 - axis, -1)))

    for axis, here, full in arrays:
        across(axis, full, *wide[axis][0])
    for axis, here, full in arrays:
        for copy in second[axis]:
            copy.wait_recv()
        whole = full.at[owner(axis, 2, 0)]
        wide[axis].append((2, [send(whole, whole, along(1 - axis, s)) for s in (1, -1)]))
    rows = h_ref.shape[0] // 2
    plus, minus = x_first
    plus.wait_recv()
    whole = h_all.at[shifted(cx, -1) * 2 + core]
    part = whole.at[pl.ds(0, rows)]
    x_second = [send(part, part, xdev(1, core))]
    x_over.append(send(whole, whole, xdev(0, 1 - core)))
    minus.wait_recv()
    whole = h_all.at[shifted(cx, 1) * 2 + core]
    part = whole.at[pl.ds(rows, rows)]
    x_second.append(send(part, part, xdev(-1, core)))
    x_over.append(send(whole, whole, xdev(0, 1 - core)))
    for i in (1, 2):
        for axis, here, full in arrays:
            across(axis, full, *wide[axis][i])
    for copy in x_second:
        copy.wait_recv()
    whole = h_all.at[shifted(cx, 2) * 2 + core]
    x_over.append(send(whole, whole, xdev(0, 1 - core)))
    for axis, here, full in arrays:
        across(axis, full, *wide[axis][3])
    for copy in last:
        copy.wait_recv()
    for copy in x_over:
        copy.wait_recv()
    pool_sender.finish()
    send.finish()
    for copy in local:
        copy.wait()


GATHER_COPIES = 2 * (2 + 2 + 8 + 8) + 2 + 2 + 4


def run_gather(k, v, h, q, g, gates, sums):
    any_spec = pl.BlockSpec(memory_space=pl.ANY)
    vmem = pl.BlockSpec(memory_space=pltpu.VMEM)
    n_pool = OWNERS * POOLED
    return pl.pallas_call(
        gather_kernel,
        name="gather",
        out_shape=(
            jax.ShapeDtypeStruct((OWNERS, TOKENS, HEAD_DIM), BF16),
            jax.ShapeDtypeStruct((OWNERS, TOKENS, HEAD_DIM), BF16),
            jax.ShapeDtypeStruct((8, TOKENS // 8, MODEL), BF16),
            jax.ShapeDtypeStruct((BLOCKS, HEAD_DIM, GROUP * QUERY_BLOCK), F32),
            jax.ShapeDtypeStruct((n_pool, HEAD_DIM), F32),
            jax.ShapeDtypeStruct((n_pool, HEAD_DIM), F32),
        ),
        in_specs=[vmem] * 7,
        out_specs=(any_spec, any_spec, any_spec, vmem, vmem, vmem),
        scratch_shapes=[
            pltpu.VMEM((OWNERS, 2, POOLED, HEAD_DIM), BF16),
            pltpu.VMEM((n_pool, HEAD_DIM), BF16),
            pltpu.VMEM((n_pool, HEAD_DIM), BF16),
            pltpu.VMEM((2, POOLED, HEAD_DIM), BF16),
            pltpu.SemaphoreType.DMA((OWNERS - 1,)),
            pltpu.SemaphoreType.DMA((OWNERS - 1,)),
            pltpu.SemaphoreType.DMA((GATHER_COPIES,)),
            pltpu.SemaphoreType.DMA((GATHER_COPIES,)),
            pltpu.SemaphoreType.DMA((3,)),
        ],
        compiler_params=pltpu.CompilerParams(
            collective_id=0, has_side_effects=True, vmem_limit_bytes=12 * MIB
        ),
    )(k, v, h, q, g, gates, sums)


def chosen_kernel(
    chosen_ref, k_ref, v_ref, q_ref, g_ref, gate_ref, ls_ref, dqp_ref, dpk_ref, dpv_ref,
    gq_ref, gqt_ref, dk_ref, dv_ref,
    acc_k, acc_v, kb, vb,
):
    kv = lax.axis_index("kv")
    n_pool = OWNERS * POOLED

    def start(i, carry):
        at = pl.multiple_of(i * 8, 8)
        for acc, pooled in ((acc_k, dpk_ref), (acc_v, dpv_ref)):
            part = pooled[pl.ds(at, 8), :] * (1.0 / POOL_BLOCK)
            rows = jnp.broadcast_to(part[:, None, :], (8, POOL_BLOCK, HEAD_DIM))
            acc[pl.ds(pl.multiple_of(at * POOL_BLOCK, 8 * POOL_BLOCK), 8 * POOL_BLOCK), :] = (
                rows.reshape(8 * POOL_BLOCK, HEAD_DIM)
            )
        return carry

    lax.fori_loop(0, n_pool // 8, start, 0)

    wide_q = GROUP * QUERY_BLOCK
    ahead = (
        lax.broadcasted_iota(jnp.int32, (KEY_BLOCK, wide_q), 0)
        - lax.broadcasted_iota(jnp.int32, (KEY_BLOCK, wide_q), 1) % QUERY_BLOCK
    )

    def block(b, carry):
        qs, cs, log_sum = tile_operands(q_ref, g_ref, gate_ref, ls_ref, 1, b)
        start_row = kv * TOKENS + b * QUERY_BLOCK
        seen, at = [], []
        for c in range(CHOSEN):
            first = pl.multiple_of(chosen_ref[b, c] * KEY_BLOCK, KEY_BLOCK)
            at.append(first)
            kb[pl.ds(c * KEY_BLOCK, KEY_BLOCK), :] = k_ref[pl.ds(first, KEY_BLOCK), :]
            vb[pl.ds(c * KEY_BLOCK, KEY_BLOCK), :] = v_ref[pl.ds(first, KEY_BLOCK), :]
            seen.append(ahead <= start_row - first)
        visible = jnp.concatenate(seen, axis=0)
        dq, dk, dv = attend_back(qs, cs, log_sum, kb[...], vb[...], visible)
        dk = dk * SCALE
        total = (dqp_ref[b] + dq) * SCALE
        rows = pl.ds(pl.multiple_of(b * QUERY_BLOCK, QUERY_BLOCK), QUERY_BLOCK)
        for h in range(GROUP):
            cols = slice(h * HEAD_DIM, (h + 1) * HEAD_DIM)
            part = total[:, cols]
            gqt_ref[cols, rows] = part.astype(BF16)
            gq_ref[rows, cols] = part.T.astype(BF16)
        for c in range(CHOSEN):
            here = pl.ds(at[c], KEY_BLOCK)
            piece = slice(c * KEY_BLOCK, (c + 1) * KEY_BLOCK)
            acc_k[here, :] += dk[piece]
            acc_v[here, :] += dv[piece]
        return carry

    lax.fori_loop(0, BLOCKS, block, 0)

    def finish(i, carry):
        rows = pl.ds(pl.multiple_of(i * 512, 512), 512)
        dk_ref[rows, :] = acc_k[rows, :].astype(BF16)
        dv_ref[rows, :] = acc_v[rows, :].astype(BF16)
        return carry

    lax.fori_loop(0, SEQ // 512, finish, 0)


def run_chosen(chosen, k_all, v_all, q, g, gates, sums, dqp, dpk, dpv):
    vmem = pl.BlockSpec(memory_space=pltpu.VMEM)
    smem = pl.BlockSpec(memory_space=pltpu.SMEM)
    return pl.pallas_call(
        chosen_kernel,
        name="chosen",
        out_shape=(
            jax.ShapeDtypeStruct((TOKENS, GROUP * HEAD_DIM), BF16),
            jax.ShapeDtypeStruct((GROUP * HEAD_DIM, TOKENS), BF16),
            jax.ShapeDtypeStruct((SEQ, HEAD_DIM), BF16),
            jax.ShapeDtypeStruct((SEQ, HEAD_DIM), BF16),
        ),
        in_specs=[smem] + [vmem] * 9,
        out_specs=(vmem,) * 4,
        scratch_shapes=[
            pltpu.VMEM((SEQ, HEAD_DIM), F32),
            pltpu.VMEM((SEQ, HEAD_DIM), F32),
            pltpu.VMEM((CHOSEN * KEY_BLOCK, HEAD_DIM), BF16),
            pltpu.VMEM((CHOSEN * KEY_BLOCK, HEAD_DIM), BF16),
        ],
        compiler_params=pltpu.CompilerParams(vmem_limit_bytes=24 * MIB),
    )(chosen, k_all, v_all, q, g, gates, sums, dqp, dpk, dpv)


class Reduce:
    def __init__(self, send, axis, src, bufs, coords, along):
        (self.relay, self.direct, self.comb, self.out, self.total,
         self.relay2, self.direct2, self.comb2, self.out2) = bufs
        self.send, self.axis, self.src = send, axis, src
        self.c1, self.c2 = (coords[0], coords[1]) if axis == 0 else (coords[1], coords[0])
        self.to1 = lambda o: along(axis, o)
        self.to2 = lambda o: along(1 - axis, o)
        self.half = src.shape[2] // 2
        self.lo, self.hi = pl.ds(0, self.half), pl.ds(self.half, self.half)

    def bundle(self, o, rows):
        c = shifted(self.c1, o)
        return self.src.at[c, :, rows] if self.axis == 0 else self.src.at[:, c, rows]

    def piece(self, o, i, rows):
        c = shifted(self.c1, o)
        if self.axis == 0:
            return self.src[c, i, rows, :]
        return self.src[i, c, rows, :]

    def part(self, o, rows):
        return self.total.at[shifted(self.c2, o), rows]

    def begin(self):
        s = self.send
        self.r = [
            s(self.bundle(2, self.lo), self.relay.at[0], self.to1(1)),
            s(self.bundle(2, self.hi), self.relay.at[1], self.to1(-1)),
        ]
        self.d = [
            s(self.bundle(1, self.hi), self.direct.at[0], self.to1(1)),
            s(self.bundle(-1, self.lo), self.direct.at[1], self.to1(-1)),
        ]

    def combine(self):
        self.c = []
        for n, (o, rows) in enumerate(((1, self.lo), (-1, self.hi))):
            self.r[n].wait_recv()

            def add(i, carry, n=n, o=o, rows=rows):
                self.out[n, i] = (
                    self.piece(o, i, rows).astype(F32) + self.relay[n, i].astype(F32)
                ).astype(BF16)
                return carry

            lax.fori_loop(0, SIDE, add, 0)
            self.c.append(self.send(self.out.at[n], self.comb.at[n], self.to1(o)))

    def turn(self):
        for copy in self.d + self.c:
            copy.wait_recv()

        def add(i, carry):
            self.total[i, self.lo, :] = (
                self.piece(0, i, self.lo).astype(F32)
                + self.comb[0, i].astype(F32)
                + self.direct[1, i].astype(F32)
            ).astype(BF16)
            self.total[i, self.hi, :] = (
                self.piece(0, i, self.hi).astype(F32)
                + self.comb[1, i].astype(F32)
                + self.direct[0, i].astype(F32)
            ).astype(BF16)
            return carry

        lax.fori_loop(0, SIDE, add, 0)
        s = self.send
        self.r = [
            s(self.part(2, self.lo), self.relay2.at[0], self.to2(1)),
            s(self.part(2, self.hi), self.relay2.at[1], self.to2(-1)),
        ]
        self.d = [
            s(self.part(1, self.hi), self.direct2.at[0], self.to2(1)),
            s(self.part(-1, self.lo), self.direct2.at[1], self.to2(-1)),
        ]

    def combine2(self):
        self.c = []
        for n, (o, rows) in enumerate(((1, self.lo), (-1, self.hi))):
            self.r[n].wait_recv()
            self.out2[n] = (
                self.total[shifted(self.c2, o), rows, :].astype(F32) + self.relay2[n].astype(F32)
            ).astype(BF16)
            self.c.append(self.send(self.out2.at[n], self.comb2.at[n], self.to2(o)))

    def end(self):
        for copy in self.d + self.c:
            copy.wait_recv()
        own = self.c2
        low = (
            self.total[own, self.lo, :].astype(F32)
            + self.comb2[0].astype(F32)
            + self.direct2[1].astype(F32)
        )
        high = (
            self.total[own, self.hi, :].astype(F32)
            + self.comb2[1].astype(F32)
            + self.direct2[0].astype(F32)
        )
        return low, high


def reduce_buffers(rows, lanes):
    half = rows // 2
    wide = pltpu.VMEM((2, SIDE, half, lanes), BF16)
    slim = pltpu.VMEM((2, half, lanes), BF16)
    return [wide] * 4 + [pltpu.VMEM((SIDE, rows, lanes), BF16)] + [slim] * 4


REDUCE_BUFS = 9
GW_ROWS = GROUP * HEAD_DIM // 2
GW_COLS = MODEL // OWNERS


def scatter_kernel(dk_ref, dv_ref, h_ref, gqt_ref, gk_out, gv_out, gw_out, gw0, gw1, *rest):
    bufs = [rest[i * REDUCE_BUFS : (i + 1) * REDUCE_BUFS] for i in range(4)]
    send_sems, recv_sems = rest[4 * REDUCE_BUFS :]
    kv, tp, cz, cy, cx, core = place()

    def along(axis, o):
        if axis == 0:
            return (shifted(cz, o) * SIDE + cy, tp)
        return (cz * SIDE + shifted(cy, o), tp)

    meet([along(axis, o) for axis in (0, 1) for o in (1, -1)])
    send = Sender(send_sems, recv_sems)
    rk, rv, w0, w1 = [
        Reduce(send, axis, src, buf, (cz, cy), along)
        for axis, src, buf in zip((0, 1, 0, 1), (dk_ref, dv_ref, gw0, gw1), bufs)
    ]
    rk.begin()
    rv.begin()

    def product(j, carry):
        cols = pl.ds(pl.multiple_of(j * GW_COLS, GW_COLS), GW_COLS)
        part = dot(gqt_ref[...], h_ref[:, cols], NN).astype(BF16)
        gw0[j // SIDE, j % SIDE] = part[:GW_ROWS]
        gw1[j // SIDE, j % SIDE] = part[GW_ROWS:]
        return carry

    lax.fori_loop(0, OWNERS, product, 0)
    rk.combine()
    rv.combine()
    w0.begin()
    w1.begin()
    rk.turn()
    rv.turn()
    w0.combine()
    w1.combine()
    rk.combine2()
    rv.combine2()
    w0.turn()
    w1.turn()
    half = TOKENS // 2
    for r, out in ((rk, gk_out), (rv, gv_out)):
        low, high = r.end()
        out[:half, :] = low.astype(BF16)
        out[half:, :] = high.astype(BF16)
    w0.combine2()
    w1.combine2()
    half = GW_ROWS // 2
    for n, r in enumerate((w0, w1)):
        low, high = r.end()
        gw_out[:, n * GW_ROWS : n * GW_ROWS + half] = low.T
        gw_out[:, n * GW_ROWS + half : (n + 1) * GW_ROWS] = high.T
    send.finish()


SCATTER_COPIES = 4 * 12


def run_scatter(dk, dv, h_all, gqt):
    vmem = pl.BlockSpec(memory_space=pltpu.VMEM)
    return pl.pallas_call(
        scatter_kernel,
        name="scatter",
        out_shape=(
            jax.ShapeDtypeStruct((TOKENS, HEAD_DIM), BF16),
            jax.ShapeDtypeStruct((TOKENS, HEAD_DIM), BF16),
            jax.ShapeDtypeStruct((GW_COLS, GROUP * HEAD_DIM), F32),
        ),
        in_specs=[vmem] * 4,
        out_specs=(vmem,) * 3,
        scratch_shapes=[
            pltpu.VMEM((SIDE, SIDE, GW_ROWS, GW_COLS), BF16),
            pltpu.VMEM((SIDE, SIDE, GW_ROWS, GW_COLS), BF16),
            *reduce_buffers(TOKENS, HEAD_DIM),
            *reduce_buffers(TOKENS, HEAD_DIM),
            *reduce_buffers(GW_ROWS, GW_COLS),
            *reduce_buffers(GW_ROWS, GW_COLS),
            pltpu.SemaphoreType.DMA((SCATTER_COPIES,)),
            pltpu.SemaphoreType.DMA((SCATTER_COPIES,)),
        ],
        compiler_params=pltpu.CompilerParams(
            collective_id=1, has_side_effects=True, vmem_limit_bytes=24 * MIB
        ),
    )(dk, dv, h_all, gqt)


def finish_kernel(gk_ref, gv_ref, gw_ref, gk_out, gv_out, gw_out):
    gk_out[...] = gk_ref[...]
    gv_out[...] = gv_ref[...]
    gw_out[...] = gw_ref[...]


def run_finish(gk, gv, gw):
    vmem = pl.BlockSpec(memory_space=pltpu.VMEM)
    return pl.pallas_call(
        finish_kernel,
        name="finish",
        out_shape=tuple(jax.ShapeDtypeStruct(a.shape, a.dtype) for a in (gk, gv, gw)),
        in_specs=[vmem] * 3,
        out_specs=(vmem,) * 3,
        compiler_params=pltpu.CompilerParams(vmem_limit_bytes=8 * MIB),
    )(gk, gv, gw)


def body(hidden_rows, queries, key_rows, value_rows, branch_gates, log_sums, chosen, out_grad):
    k_all, v_all, h_all, dqp, dpk, dpv = run_gather(
        key_rows, value_rows, hidden_rows, queries, out_grad, branch_gates, log_sums
    )
    gq, gqt, dk, dv = run_chosen(
        chosen.reshape(BLOCKS, CHOSEN),
        k_all.reshape(SEQ, HEAD_DIM),
        v_all.reshape(SEQ, HEAD_DIM),
        queries, out_grad, branch_gates, log_sums, dqp, dpk, dpv,
    )
    plane = (SIDE, SIDE, TOKENS, HEAD_DIM)
    gk, gv, gw = run_scatter(
        dk.reshape(plane), dv.reshape(plane), h_all.reshape(TOKENS, MODEL), gqt
    )
    gk, gv, gw = run_finish(gk, gv, gw)
    return gq, gk, gv, gw


def solution(mesh):
    placed = (
        P(("kv", "tp"), None),
        P("kv", "tp"),
        P("kv", "tp"),
        P("kv", "tp"),
        P(None, "tp", "kv"),
        P(None, "tp", "kv"),
        P("tp", "kv", None),
        P("kv", "tp"),
    )
    return jax.shard_map(
        body,
        mesh=mesh,
        in_specs=placed,
        out_specs=(P("kv", "tp"), P("kv", "tp"), P("kv", "tp"), P("kv", "tp")),
        check_vma=False,
    )
```

```python
import jax
import jax.numpy as jnp
from jax import lax
from jax.experimental import pallas as pl
from jax.experimental.pallas import tpu as pltpu
from jax.sharding import PartitionSpec as P

HEADS = 32
KV_HEADS = 8
HEAD_DIM = 128
QUERY_BLOCK = 128
KEY_BLOCK = 32
POOL_BLOCK = 32
CHOSEN = 16
GROUP = HEADS // KV_HEADS
SIDE = 4
OWNERS = SIDE * SIDE
TOKENS = 1024
BLOCKS = TOKENS // QUERY_BLOCK
POOLED = TOKENS // POOL_BLOCK
SEQ = TOKENS * OWNERS
MODEL = 4096
SCALE = HEAD_DIM ** (-0.5)
LOG2E = 1.4426950408889634
MIB = 1 << 20
MESH = pl.DeviceIdType.MESH
F32 = jnp.float32
BF16 = jnp.bfloat16

NT = (((1,), (1,)), ((), ()))
NN = (((1,), (0,)), ((), ()))


def dot(a, b, dims):
    return lax.dot_general(a, b, dims, preferred_element_type=F32)


class Sender:
    def __init__(self, send_sems, recv_sems):
        self.send_sems, self.recv_sems, self.at, self.sent = send_sems, recv_sems, 0, []

    def __call__(self, src, dst, dev):
        copy = pltpu.make_async_remote_copy(
            src_ref=src,
            dst_ref=dst,
            send_sem=self.send_sems.at[self.at],
            recv_sem=self.recv_sems.at[self.at],
            device_id=dev,
            device_id_type=MESH,
        )
        self.at += 1
        copy.start()
        self.sent.append(copy)
        return copy

    def finish(self):
        for copy in self.sent:
            copy.wait_send()


def place():
    kv, tp = lax.axis_index("kv"), lax.axis_index("tp")
    return kv, tp, kv // SIDE, kv % SIDE, tp // 2, tp % 2


def shifted(c, o):
    return (c + (o + SIDE)) % SIDE


def greet(devices):
    for dev in devices:
        pl.semaphore_signal(
            pltpu.get_barrier_semaphore(), inc=1, device_id=dev, device_id_type=MESH
        )


def meet(count):
    pl.semaphore_wait(pltpu.get_barrier_semaphore(), count)


def tile_operands(q_ref, g_ref, gate_ref, ls_ref, t):
    rows = pl.ds(pl.multiple_of(t * QUERY_BLOCK, QUERY_BLOCK), QUERY_BLOCK)
    gates = jnp.concatenate([gate_ref[0, :, rows], gate_ref[1, :, rows]], axis=0).T
    qs, cs, ls = [], ([], []), ([], [])
    for h in range(GROUP):
        cols = slice(h * HEAD_DIM, (h + 1) * HEAD_DIM)
        qs.append(q_ref[rows, cols])
        grad = g_ref[rows, cols].astype(F32)
        for branch in (0, 1):
            at = branch * GROUP + h
            cs[branch].append((gates[:, at : at + 1] * grad).astype(BF16))
            ls[branch].append(ls_ref[branch, h : h + 1, rows])
    return (
        jnp.concatenate(qs, axis=0),
        [jnp.concatenate(c, axis=0) for c in cs],
        [jnp.concatenate(x, axis=1) * LOG2E for x in ls],
    )


def attend_back(qs, cs, log_sum, keys, values, visible):
    scores = dot(keys, qs, NT) * (SCALE * LOG2E)
    p = jnp.where(visible, jnp.exp2(scores - log_sum), 0.0)
    pr = p.astype(BF16)
    dp = dot(values, cs, NT)
    delta = jnp.sum(pr.astype(F32) * dp, axis=0, keepdims=True)
    ds = (p * (dp - delta)).astype(BF16)
    return dot(keys.T, ds, NN), dot(ds, qs, NN), dot(pr, cs, NN)


def gather_kernel(
    k_ref, v_ref, h_ref, q_hbm, g_hbm, gate_hbm, ls_hbm,
    k_all, v_all, h_all, dq_ref, dpk_ref, dpv_ref, qs_all, cs_all, ls_rows,
    q_ref, g_ref, gate_ref, ls_ref, pool_all, pk_ref, pv_ref, pool_here,
    pool_send, pool_recv, send_sems, recv_sems, local_sems,
):
    kv, tp, cz, cy, cx, core = place()
    half = TOKENS // 2

    def device(oz, oy):
        return (shifted(cz, oz) * SIDE + shifted(cy, oy), tp)

    def along(axis, o):
        return device(o, 0) if axis == 0 else device(0, o)

    def owner(axis, o1, o2):
        a, b = (o1, o2) if axis == 0 else (o2, o1)
        return shifted(cz, a) * SIDE + shifted(cy, b)

    def xdev(o, c):
        return (kv, shifted(cx, o) * 2 + c)

    others = [(oz, oy) for oz in range(SIDE) for oy in range(SIDE) if (oz, oy) != (0, 0)]
    peers = [device(oz, oy) for oz, oy in others] + [
        xdev(1, core), xdev(-1, core), xdev(0, 1 - core)
    ]
    greet(peers)
    local = [
        pltpu.make_async_copy(src, dst, local_sems.at[i])
        for i, (src, dst) in enumerate(
            (
                (k_ref, k_all.at[kv]),
                (v_ref, v_all.at[kv]),
                (h_ref, h_all.at[tp]),
                (gate_hbm, gate_ref),
                (ls_hbm, ls_ref),
                (q_hbm, q_ref),
                (g_hbm, g_ref),
            )
        )
    ]
    for copy in local:
        copy.start()

    blk = lax.broadcasted_iota(jnp.int32, (POOLED, TOKENS), 0)
    row = lax.broadcasted_iota(jnp.int32, (POOLED, TOKENS), 1)
    mean = jnp.where(row // POOL_BLOCK == blk, 1.0 / POOL_BLOCK, 0.0).astype(BF16)
    local[0].wait()
    pool_here[0] = dot(mean, k_all[kv], NN).astype(BF16)
    local[1].wait()
    pool_here[1] = dot(mean, v_all[kv], NN).astype(BF16)
    meet(len(peers))

    pool_sender = Sender(pool_send, pool_recv)
    for oz, oy in others:
        pool_sender(pool_here, pool_all.at[kv], device(oz, oy))
    pool_all[kv] = pool_here[...]

    send = Sender(send_sems, recv_sems)
    first, wide = {}, {}
    arrays = ((0, k_all), (1, v_all))
    for axis, full in arrays:
        here = full.at[kv]
        first[axis] = [send(here, here, along(axis, s)) for s in (1, -1)]
    local[2].wait()
    here = h_all.at[tp]
    x_first = [send(here, here, xdev(s, core)) for s in (1, -1)]
    x_over = [send(here, here, xdev(0, 1 - core))]
    for axis, full in arrays:
        here = full.at[kv]
        wide[axis] = [(0, [send(here, here, along(1 - axis, s)) for s in (1, -1)])]

    for copy in local[3:]:
        copy.wait()
    for copy in pool_sender.sent:
        copy.wait_recv()
    pk_ref[...] = pool_all[:, 0].reshape(OWNERS * POOLED, HEAD_DIM)
    pv_ref[...] = pool_all[:, 1].reshape(OWNERS * POOLED, HEAD_DIM)
    dpk_ref[...] = jnp.zeros_like(dpk_ref)
    dpv_ref[...] = jnp.zeros_like(dpv_ref)

    n_pool = OWNERS * POOLED
    wide_q = GROUP * QUERY_BLOCK
    pool_end = lax.broadcasted_iota(jnp.int32, (n_pool, wide_q), 0) * POOL_BLOCK + POOL_BLOCK - 1
    lane = lax.broadcasted_iota(jnp.int32, (n_pool, wide_q), 1) % QUERY_BLOCK
    ahead = pool_end - lane

    def tile(t, carry):
        qs, cs, ls = tile_operands(q_ref, g_ref, gate_ref, ls_ref, t)
        qs_all[t] = qs
        cs_all[t] = cs[1]
        ls_rows[t] = ls[1]
        visible = ahead <= kv * TOKENS + t * QUERY_BLOCK
        dq, dk, dv = attend_back(qs, cs[0], ls[0], pk_ref[...], pv_ref[...], visible)
        dq_ref[t] = dq
        dpk_ref[...] += dk
        dpv_ref[...] += dv
        return carry

    lax.fori_loop(0, 4, tile, 0)

    second = {}
    for axis, full in arrays:
        plus, minus = first[axis]
        plus.wait_recv()
        part = full.at[owner(axis, -1, 0), pl.ds(0, half)]
        fwd = send(part, part, along(axis, 1))
        whole = full.at[owner(axis, -1, 0)]
        wide[axis].append((-1, [send(whole, whole, along(1 - axis, s)) for s in (1, -1)]))
        minus.wait_recv()
        part = full.at[owner(axis, 1, 0), pl.ds(half, half)]
        bwd = send(part, part, along(axis, -1))
        whole = full.at[owner(axis, 1, 0)]
        wide[axis].append((1, [send(whole, whole, along(1 - axis, s)) for s in (1, -1)]))
        second[axis] = (fwd, bwd)

    lax.fori_loop(4, BLOCKS, tile, 0)
    dpk_ref[...] = dpk_ref[...] * (SCALE / POOL_BLOCK)
    dpv_ref[...] = dpv_ref[...] * (1.0 / POOL_BLOCK)

    last = []

    def across(axis, full, o, pair):
        plus, minus = pair
        plus.wait_recv()
        part = full.at[owner(axis, o, -1), pl.ds(0, half)]
        last.append(send(part, part, along(1 - axis, 1)))
        minus.wait_recv()
        part = full.at[owner(axis, o, 1), pl.ds(half, half)]
        last.append(send(part, part, along(1 - axis, -1)))

    for axis, full in arrays:
        across(axis, full, *wide[axis][0])
    for axis, full in arrays:
        for copy in second[axis]:
            copy.wait_recv()
        whole = full.at[owner(axis, 2, 0)]
        wide[axis].append((2, [send(whole, whole, along(1 - axis, s)) for s in (1, -1)]))
    rows = TOKENS // 16
    plus, minus = x_first
    plus.wait_recv()
    whole = h_all.at[shifted(cx, -1) * 2 + core]
    part = whole.at[pl.ds(0, rows)]
    x_second = [send(part, part, xdev(1, core))]
    x_over.append(send(whole, whole, xdev(0, 1 - core)))
    minus.wait_recv()
    whole = h_all.at[shifted(cx, 1) * 2 + core]
    part = whole.at[pl.ds(rows, rows)]
    x_second.append(send(part, part, xdev(-1, core)))
    x_over.append(send(whole, whole, xdev(0, 1 - core)))
    for i in (1, 2):
        for axis, full in arrays:
            across(axis, full, *wide[axis][i])
    for copy in x_second:
        copy.wait_recv()
    whole = h_all.at[shifted(cx, 2) * 2 + core]
    x_over.append(send(whole, whole, xdev(0, 1 - core)))
    for axis, full in arrays:
        across(axis, full, *wide[axis][3])
    for copy in last:
        copy.wait_recv()
    for copy in x_over:
        copy.wait_recv()
    pool_sender.finish()
    send.finish()


GATHER_COPIES = 2 * (2 + 2 + 8 + 8) + 2 + 2 + 4


def run_gather(k, v, h, q, g, gates, sums):
    hbm = pl.BlockSpec(memory_space=pltpu.HBM)
    vmem = pl.BlockSpec(memory_space=pltpu.VMEM)
    n_pool = OWNERS * POOLED
    wide_q = GROUP * QUERY_BLOCK
    return pl.pallas_call(
        gather_kernel,
        name="gather",
        out_shape=(
            jax.ShapeDtypeStruct((OWNERS, TOKENS, HEAD_DIM), BF16),
            jax.ShapeDtypeStruct((OWNERS, TOKENS, HEAD_DIM), BF16),
            jax.ShapeDtypeStruct((8, TOKENS // 8, MODEL), BF16),
            jax.ShapeDtypeStruct((BLOCKS, HEAD_DIM, wide_q), F32),
            jax.ShapeDtypeStruct((n_pool, HEAD_DIM), F32),
            jax.ShapeDtypeStruct((n_pool, HEAD_DIM), F32),
            jax.ShapeDtypeStruct((BLOCKS, wide_q, HEAD_DIM), BF16),
            jax.ShapeDtypeStruct((BLOCKS, wide_q, HEAD_DIM), BF16),
            jax.ShapeDtypeStruct((BLOCKS, 1, wide_q), F32),
        ),
        in_specs=[hbm] * 7,
        out_specs=(vmem,) * 9,
        scratch_shapes=[
            pltpu.VMEM(q.shape, BF16),
            pltpu.VMEM(g.shape, BF16),
            pltpu.VMEM(gates.shape, F32),
            pltpu.VMEM(sums.shape, F32),
            pltpu.VMEM((OWNERS, 2, POOLED, HEAD_DIM), BF16),
            pltpu.VMEM((n_pool, HEAD_DIM), BF16),
            pltpu.VMEM((n_pool, HEAD_DIM), BF16),
            pltpu.VMEM((2, POOLED, HEAD_DIM), BF16),
            pltpu.SemaphoreType.DMA((OWNERS - 1,)),
            pltpu.SemaphoreType.DMA((OWNERS - 1,)),
            pltpu.SemaphoreType.DMA((GATHER_COPIES,)),
            pltpu.SemaphoreType.DMA((GATHER_COPIES,)),
            pltpu.SemaphoreType.DMA((7,)),
        ],
        compiler_params=pltpu.CompilerParams(
            collective_id=0, has_side_effects=True, vmem_limit_bytes=12 * MIB
        ),
        cost_estimate=pl.CostEstimate(
            flops=40_000_000_000, bytes_accessed=8 * MIB, transcendentals=0
        ),
    )(*(pltpu.with_memory_space_constraint(a, pltpu.HBM) for a in (k, v, h, q, g, gates, sums)))


class Reduce:
    def __init__(self, send, axis, src, bufs, coords, along):
        self.relay, self.direct, self.comb, self.relay2, self.direct2, self.comb2 = bufs
        self.send, self.axis, self.src = send, axis, src
        self.c1, self.c2 = (coords[0], coords[1]) if axis == 0 else (coords[1], coords[0])
        self.to1 = lambda o: along(axis, o)
        self.to2 = lambda o: along(1 - axis, o)
        self.half = src.shape[2] // 2
        self.rows = (pl.ds(0, self.half), pl.ds(self.half, self.half))

    def bundle(self, o, n):
        c = shifted(self.c1, o)
        rows = self.rows[n]
        return self.src.at[c, :, rows] if self.axis == 0 else self.src.at[:, c, rows]

    def piece(self, o, i, n):
        c = shifted(self.c1, o)
        if self.axis == 0:
            return self.src[c, i, self.rows[n], :].astype(F32)
        return self.src[i, c, self.rows[n], :].astype(F32)

    def part(self, o, n):
        return self.comb.at[n, shifted(self.c2, o)]

    def begin(self):
        s = self.send
        self.r = [
            s(self.bundle(2, 0), self.relay.at[0], self.to1(1)),
            s(self.bundle(2, 1), self.relay.at[1], self.to1(-1)),
        ]
        self.d = [
            s(self.bundle(1, 1), self.direct.at[0], self.to1(1)),
            s(self.bundle(-1, 0), self.direct.at[1], self.to1(-1)),
        ]

    def combine(self):
        self.c = []
        for n, o in enumerate((1, -1)):
            self.r[n].wait_recv()

            def add(i, carry, n=n, o=o):
                self.relay[n, i] = (self.piece(o, i, n) + self.relay[n, i].astype(F32)).astype(BF16)
                return carry

            lax.fori_loop(0, SIDE, add, 0)
            self.c.append(self.send(self.relay.at[n], self.comb.at[n], self.to1(o)))

    def turn(self):
        for copy in self.d + self.c:
            copy.wait_recv()

        def add(i, carry):
            for n in (0, 1):
                self.comb[n, i] = (
                    self.piece(0, i, n)
                    + self.comb[n, i].astype(F32)
                    + self.direct[1 - n, i].astype(F32)
                ).astype(BF16)
            return carry

        lax.fori_loop(0, SIDE, add, 0)
        s = self.send
        self.r = [
            s(self.part(2, 0), self.relay2.at[0], self.to2(1)),
            s(self.part(2, 1), self.relay2.at[1], self.to2(-1)),
        ]
        self.d = [
            s(self.part(1, 1), self.direct2.at[0], self.to2(1)),
            s(self.part(-1, 0), self.direct2.at[1], self.to2(-1)),
        ]

    def combine2(self):
        self.c = []
        for n, o in enumerate((1, -1)):
            self.r[n].wait_recv()
            self.relay2[n] = (
                self.comb[n, shifted(self.c2, o)].astype(F32) + self.relay2[n].astype(F32)
            ).astype(BF16)
            self.c.append(self.send(self.relay2.at[n], self.comb2.at[n], self.to2(o)))

    def end(self):
        for copy in self.d + self.c:
            copy.wait_recv()
        return [
            self.comb[n, self.c2].astype(F32)
            + self.comb2[n].astype(F32)
            + self.direct2[1 - n].astype(F32)
            for n in (0, 1)
        ]


def reduce_buffers(rows, lanes):
    half = rows // 2
    wide = pltpu.VMEM((2, SIDE, half, lanes), BF16)
    slim = pltpu.VMEM((2, half, lanes), BF16)
    return [wide] * 3 + [slim] * 3


REDUCE_BUFS = 6
GW_COLS = MODEL // OWNERS
PAIR = GROUP // 2 * HEAD_DIM
PAIR_Q = GROUP // 2 * QUERY_BLOCK
SETS = CHOSEN * KEY_BLOCK


def scatter_kernel(
    chosen_ref, k_ref, v_ref, h_ref, dqp_ref, dpk_ref, dpv_ref, qs_all, cs_all, ls_rows,
    gq_ref, gk_out, gv_out, gw_out,
    kb, vb, dk_set, dv_set, gqt, dk_all, dv_all, gw0, gw1, gw2, gw3, order, *rest
):
    bufs = [rest[i * REDUCE_BUFS : (i + 1) * REDUCE_BUFS] for i in range(6)]
    send_sems, recv_sems = rest[6 * REDUCE_BUFS :]
    kv, tp, cz, cy, cx, core = place()

    def along(axis, o):
        if axis == 0:
            return (shifted(cz, o) * SIDE + cy, tp)
        return (cz * SIDE + shifted(cy, o), tp)

    peers = [along(axis, o) for axis in (0, 1) for o in (1, -1)]
    greet(peers)
    send = Sender(send_sems, recv_sems)
    gws = (gw0, gw1, gw2, gw3)
    rk, rv, w0, w1, w2, w3 = [
        Reduce(send, axis, src, buf, (cz, cy), along)
        for axis, src, buf in zip((0, 1, 0, 1, 0, 1), (dk_all, dv_all) + gws, bufs)
    ]

    ahead = (
        lax.broadcasted_iota(jnp.int32, (KEY_BLOCK, PAIR_Q), 0)
        - lax.broadcasted_iota(jnp.int32, (KEY_BLOCK, PAIR_Q), 1) % QUERY_BLOCK
    )

    def attend(pair):
        across = slice(pair * PAIR_Q, (pair + 1) * PAIR_Q)

        def block(b, carry):
            start_row = kv * TOKENS + b * QUERY_BLOCK
            seen = []
            for c in range(CHOSEN):
                at = chosen_ref[b, c]
                kb[c * KEY_BLOCK : (c + 1) * KEY_BLOCK, :] = k_ref[at]
                vb[c * KEY_BLOCK : (c + 1) * KEY_BLOCK, :] = v_ref[at]
                seen.append(ahead <= start_row - at * KEY_BLOCK)
            dq, dk, dv = attend_back(
                qs_all[b, across, :],
                cs_all[b, across, :],
                ls_rows[b, :, across],
                kb[...],
                vb[...],
                jnp.concatenate(seen, axis=0),
            )
            total = (dqp_ref[b, :, across] + dq) * SCALE
            rows = pl.ds(pl.multiple_of(b * QUERY_BLOCK, QUERY_BLOCK), QUERY_BLOCK)
            for h in range(GROUP // 2):
                part = total[:, h * QUERY_BLOCK : (h + 1) * QUERY_BLOCK]
                at = pair * PAIR + h * HEAD_DIM
                gqt[at : at + HEAD_DIM, rows] = part.astype(BF16)
                gq_ref[rows, at : at + HEAD_DIM] = part.T.astype(BF16)
            here = pl.ds(pl.multiple_of(b * SETS, SETS), SETS)
            if pair == 0:
                dk_set[here, :] = dk
                dv_set[here, :] = dv
            else:
                dk_set[here, :] += dk
                dv_set[here, :] += dv
            return carry

        return block

    def product(pair):
        def one(j, carry):
            cols = pl.ds(pl.multiple_of(j * GW_COLS, GW_COLS), GW_COLS)
            part = dot(gqt[pair * PAIR : (pair + 1) * PAIR, :], h_ref[:, cols], NN).astype(BF16)
            gws[2 * pair][j // SIDE, j % SIDE] = part[:HEAD_DIM]
            gws[2 * pair + 1][j // SIDE, j % SIDE] = part[HEAD_DIM:]
            return carry

        lax.fori_loop(0, OWNERS, one, 0)

    lax.fori_loop(0, BLOCKS, attend(0), 0)
    product(0)
    meet(len(peers))
    w0.begin()
    w1.begin()
    lax.fori_loop(0, BLOCKS // 2, attend(1), 0)
    w0.combine()
    w1.combine()
    lax.fori_loop(BLOCKS // 2, BLOCKS, attend(1), 0)

    lane = lax.broadcasted_iota(jnp.int32, (1, BLOCKS * CHOSEN), 1)
    listed = jnp.zeros((1, BLOCKS * CHOSEN), jnp.int32)
    for b in range(BLOCKS):
        for c in range(CHOSEN):
            listed = jnp.where(lane == b * CHOSEN + c, chosen_ref[b, c], listed)
    n_pool = OWNERS * POOLED
    hits = lax.broadcasted_iota(jnp.int32, (n_pool, BLOCKS * CHOSEN), 0) == listed
    hits = jnp.where(hits, 1.0, 0.0).astype(BF16)
    plane = (SIDE, SIDE, POOLED, HEAD_DIM)

    def spread(r, carry):
        every = pl.ds(r, BLOCKS * CHOSEN, stride=KEY_BLOCK)
        part = jnp.concatenate([dk_set[every, :], dv_set[every, :]], axis=1).astype(BF16)
        got = dot(hits, part, NN)
        rows = pl.ds(pl.multiple_of(r * POOLED, POOLED), POOLED)
        dk = got[:, :HEAD_DIM] * SCALE + dpk_ref[...]
        dv = got[:, HEAD_DIM:] + dpv_ref[...]
        dk_all[:, :, rows, :] = dk.astype(BF16).reshape(plane)
        dv_all[:, :, rows, :] = dv.astype(BF16).reshape(plane)
        return carry

    lax.fori_loop(0, KEY_BLOCK, spread, 0)
    rk.begin()
    rv.begin()
    w0.turn()
    w1.turn()
    product(1)
    rk.combine()
    rv.combine()
    w2.begin()
    w3.begin()
    w0.combine2()
    w1.combine2()
    rk.turn()
    rv.turn()
    w2.combine()
    w3.combine()
    rk.combine2()
    rv.combine2()
    w2.turn()
    w3.turn()

    def weight(n, w):
        for i, part in enumerate(w.end()):
            at = n * HEAD_DIM + i * HEAD_DIM // 2
            gw_out[:, at : at + HEAD_DIM // 2] = part.T

    weight(0, w0)
    weight(1, w1)
    for r, out in ((rk, gk_out), (rv, gv_out)):
        for n, part in enumerate(r.end()):
            for i in range(KEY_BLOCK // 2):
                at = n * (KEY_BLOCK // 2) + i
                order[pl.ds(at, POOLED, stride=KEY_BLOCK), :] = part[i * POOLED : (i + 1) * POOLED]
        out[...] = order[...].astype(BF16)
    w2.combine2()
    w3.combine2()
    weight(2, w2)
    weight(3, w3)
    send.finish()


SCATTER_COPIES = 6 * 12
SCATTER_MIB = 31


def run_scatter(chosen, k_all, v_all, h_all, dqp, dpk, dpv, qs, cs, ls):
    vmem = pl.BlockSpec(memory_space=pltpu.VMEM)
    smem = pl.BlockSpec(memory_space=pltpu.SMEM)
    dense = pltpu.VMEM((SIDE, SIDE, TOKENS, HEAD_DIM), BF16)
    grad = pltpu.VMEM((SIDE, SIDE, HEAD_DIM, GW_COLS), BF16)
    return pl.pallas_call(
        scatter_kernel,
        name="scatter",
        out_shape=(
            jax.ShapeDtypeStruct((TOKENS, GROUP * HEAD_DIM), BF16),
            jax.ShapeDtypeStruct((TOKENS, HEAD_DIM), BF16),
            jax.ShapeDtypeStruct((TOKENS, HEAD_DIM), BF16),
            jax.ShapeDtypeStruct((GW_COLS, GROUP * HEAD_DIM), F32),
        ),
        in_specs=[smem] + [vmem] * 9,
        out_specs=(vmem,) * 4,
        scratch_shapes=[
            pltpu.VMEM((SETS, HEAD_DIM), BF16),
            pltpu.VMEM((SETS, HEAD_DIM), BF16),
            pltpu.VMEM((BLOCKS * SETS, HEAD_DIM), F32),
            pltpu.VMEM((BLOCKS * SETS, HEAD_DIM), F32),
            pltpu.VMEM((GROUP * HEAD_DIM, TOKENS), BF16),
            dense,
            dense,
            grad,
            grad,
            grad,
            grad,
            pltpu.VMEM((TOKENS, HEAD_DIM), F32),
            *reduce_buffers(TOKENS, HEAD_DIM),
            *reduce_buffers(TOKENS, HEAD_DIM),
            *(reduce_buffers(HEAD_DIM, GW_COLS) * 4),
            pltpu.SemaphoreType.DMA((SCATTER_COPIES,)),
            pltpu.SemaphoreType.DMA((SCATTER_COPIES,)),
        ],
        compiler_params=pltpu.CompilerParams(
            collective_id=1, has_side_effects=True, vmem_limit_bytes=SCATTER_MIB * MIB
        ),
    )(chosen, k_all, v_all, h_all, dqp, dpk, dpv, qs, cs, ls)


def finish_kernel(*refs):
    for src, out in zip(refs[:4], refs[4:]):
        out[...] = src[...]


def run_finish(*outs):
    vmem = pl.BlockSpec(memory_space=pltpu.VMEM)
    return pl.pallas_call(
        finish_kernel,
        name="finish",
        out_shape=tuple(jax.ShapeDtypeStruct(a.shape, a.dtype) for a in outs),
        in_specs=[vmem] * 4,
        out_specs=(vmem,) * 4,
        compiler_params=pltpu.CompilerParams(vmem_limit_bytes=8 * MIB),
    )(*outs)


def body(hidden_rows, queries, key_rows, value_rows, branch_gates, log_sums, chosen, out_grad):
    k_all, v_all, h_all, *pooled = run_gather(
        key_rows, value_rows, hidden_rows, queries, out_grad, branch_gates, log_sums
    )
    outs = run_scatter(
        chosen.reshape(BLOCKS, CHOSEN),
        k_all.reshape(SEQ // KEY_BLOCK, KEY_BLOCK, HEAD_DIM),
        v_all.reshape(SEQ // KEY_BLOCK, KEY_BLOCK, HEAD_DIM),
        h_all.reshape(TOKENS, MODEL),
        *pooled,
    )
    return run_finish(*outs)


def solution(mesh):
    placed = (
        P(("kv", "tp"), None),
        P("kv", "tp"),
        P("kv", "tp"),
        P("kv", "tp"),
        P(None, "tp", "kv"),
        P(None, "tp", "kv"),
        P("tp", "kv", None),
        P("kv", "tp"),
    )
    return jax.shard_map(
        body,
        mesh=mesh,
        in_specs=placed,
        out_specs=(P("kv", "tp"), P("kv", "tp"), P("kv", "tp"), P("kv", "tp")),
        check_vma=False,
    )
```

```python
import jax
import jax.numpy as jnp
from jax import lax
from jax.experimental import pallas as pl
from jax.experimental.pallas import tpu as pltpu
from jax.sharding import PartitionSpec as P

HEADS = 32
KV_HEADS = 8
HEAD_DIM = 128
QUERY_BLOCK = 128
KEY_BLOCK = 32
POOL_BLOCK = 32
CHOSEN = 16
GROUP = HEADS // KV_HEADS
SIDE = 4
OWNERS = SIDE * SIDE
TOKENS = 1024
BLOCKS = TOKENS // QUERY_BLOCK
POOLED = TOKENS // POOL_BLOCK
SEQ = TOKENS * OWNERS
MODEL = 4096
SCALE = HEAD_DIM ** (-0.5)
LOG2E = 1.4426950408889634
MIB = 1 << 20
MESH = pl.DeviceIdType.MESH
F32 = jnp.float32
BF16 = jnp.bfloat16

NT = (((1,), (1,)), ((), ()))
NN = (((1,), (0,)), ((), ()))


def dot(a, b, dims):
    return lax.dot_general(a, b, dims, preferred_element_type=F32)


class Sender:
    def __init__(self, send_sems, recv_sems):
        self.send_sems, self.recv_sems, self.at, self.sent = send_sems, recv_sems, 0, []

    def __call__(self, src, dst, dev):
        copy = pltpu.make_async_remote_copy(
            src_ref=src,
            dst_ref=dst,
            send_sem=self.send_sems.at[self.at],
            recv_sem=self.recv_sems.at[self.at],
            device_id=dev,
            device_id_type=MESH,
        )
        self.at += 1
        copy.start()
        self.sent.append(copy)
        return copy

    def finish(self):
        for copy in self.sent:
            copy.wait_send()


def place():
    kv, tp = lax.axis_index("kv"), lax.axis_index("tp")
    return kv, tp, kv // SIDE, kv % SIDE, tp // 2, tp % 2


def shifted(c, o):
    return (c + (o + SIDE)) % SIDE


def greet(devices):
    for dev in devices:
        pl.semaphore_signal(
            pltpu.get_barrier_semaphore(), inc=1, device_id=dev, device_id_type=MESH
        )


def meet(count):
    pl.semaphore_wait(pltpu.get_barrier_semaphore(), count)


def tile_operands(q_ref, g_ref, gate_ref, ls_ref, t):
    rows = pl.ds(pl.multiple_of(t * QUERY_BLOCK, QUERY_BLOCK), QUERY_BLOCK)
    gates = jnp.concatenate([gate_ref[0, :, rows], gate_ref[1, :, rows]], axis=0).T
    qs, cs, ls = [], ([], []), ([], [])
    for h in range(GROUP):
        cols = slice(h * HEAD_DIM, (h + 1) * HEAD_DIM)
        qs.append(q_ref[rows, cols])
        grad = g_ref[rows, cols].astype(F32)
        for branch in (0, 1):
            at = branch * GROUP + h
            cs[branch].append((gates[:, at : at + 1] * grad).astype(BF16))
            ls[branch].append(ls_ref[branch, h : h + 1, rows])
    return (
        jnp.concatenate(qs, axis=0),
        [jnp.concatenate(c, axis=0) for c in cs],
        [jnp.concatenate(x, axis=1) * LOG2E for x in ls],
    )


def attend_back(qs, cs, log_sum, keys, values, visible):
    scores = dot(keys, qs, NT) * (SCALE * LOG2E)
    p = jnp.where(visible, jnp.exp2(scores - log_sum), 0.0)
    pr = p.astype(BF16)
    dp = dot(values, cs, NT)
    delta = jnp.sum(pr.astype(F32) * dp, axis=0, keepdims=True)
    ds = (p * (dp - delta)).astype(BF16)
    return dot(keys.T, ds, NN), dot(ds, qs, NN), dot(pr, cs, NN)


def gather_kernel(
    k_ref, v_ref, h_ref, q_hbm, g_hbm, gate_hbm, ls_hbm,
    k_all, v_all, h_all, dq_ref, dpk_ref, dpv_ref, qs_all, cs_all, ls_rows,
    q_ref, g_ref, gate_ref, ls_ref, pool_all, pk_ref, pv_ref, pool_here,
    pool_send, pool_recv, send_sems, recv_sems, local_sems,
):
    kv, tp, cz, cy, cx, core = place()
    half = TOKENS // 2

    def device(oz, oy):
        return (shifted(cz, oz) * SIDE + shifted(cy, oy), tp)

    def along(axis, o):
        return device(o, 0) if axis == 0 else device(0, o)

    def owner(axis, o1, o2):
        a, b = (o1, o2) if axis == 0 else (o2, o1)
        return shifted(cz, a) * SIDE + shifted(cy, b)

    def xdev(o, c):
        return (kv, shifted(cx, o) * 2 + c)

    others = [(oz, oy) for oz in range(SIDE) for oy in range(SIDE) if (oz, oy) != (0, 0)]
    peers = [device(oz, oy) for oz, oy in others] + [
        xdev(1, core), xdev(-1, core), xdev(0, 1 - core)
    ]
    greet(peers)
    local = [
        pltpu.make_async_copy(src, dst, local_sems.at[i])
        for i, (src, dst) in enumerate(
            (
                (k_ref, k_all.at[kv]),
                (v_ref, v_all.at[kv]),
                (h_ref, h_all.at[tp]),
                (gate_hbm, gate_ref),
                (ls_hbm, ls_ref),
                (q_hbm, q_ref),
                (g_hbm, g_ref),
            )
        )
    ]
    for copy in local:
        copy.start()

    blk = lax.broadcasted_iota(jnp.int32, (POOLED, TOKENS), 0)
    row = lax.broadcasted_iota(jnp.int32, (POOLED, TOKENS), 1)
    mean = jnp.where(row // POOL_BLOCK == blk, 1.0 / POOL_BLOCK, 0.0).astype(BF16)
    local[0].wait()
    pool_here[0] = dot(mean, k_all[kv], NN).astype(BF16)
    local[1].wait()
    pool_here[1] = dot(mean, v_all[kv], NN).astype(BF16)
    meet(len(peers))

    pool_sender = Sender(pool_send, pool_recv)
    for oz, oy in others:
        pool_sender(pool_here, pool_all.at[kv], device(oz, oy))
    pool_all[kv] = pool_here[...]

    send = Sender(send_sems, recv_sems)
    first, wide = {}, {}
    arrays = ((0, k_all), (1, v_all))
    for axis, full in arrays:
        here = full.at[kv]
        first[axis] = [send(here, here, along(axis, s)) for s in (1, -1)]
    local[2].wait()
    here = h_all.at[tp]
    x_first = [send(here, here, xdev(s, core)) for s in (1, -1)]
    x_over = [send(here, here, xdev(0, 1 - core))]
    for axis, full in arrays:
        here = full.at[kv]
        wide[axis] = [(0, [send(here, here, along(1 - axis, s)) for s in (1, -1)])]

    for copy in local[3:]:
        copy.wait()
    for copy in pool_sender.sent:
        copy.wait_recv()
    pk_ref[...] = pool_all[:, 0].reshape(OWNERS * POOLED, HEAD_DIM)
    pv_ref[...] = pool_all[:, 1].reshape(OWNERS * POOLED, HEAD_DIM)
    dpk_ref[...] = jnp.zeros_like(dpk_ref)
    dpv_ref[...] = jnp.zeros_like(dpv_ref)

    n_pool = OWNERS * POOLED
    wide_q = GROUP * QUERY_BLOCK
    pool_end = lax.broadcasted_iota(jnp.int32, (n_pool, wide_q), 0) * POOL_BLOCK + POOL_BLOCK - 1
    lane = lax.broadcasted_iota(jnp.int32, (n_pool, wide_q), 1) % QUERY_BLOCK
    ahead = pool_end - lane

    def tile(t, carry):
        qs, cs, ls = tile_operands(q_ref, g_ref, gate_ref, ls_ref, t)
        qs_all[t] = qs
        cs_all[t] = cs[1]
        ls_rows[t] = ls[1]
        visible = ahead <= kv * TOKENS + t * QUERY_BLOCK
        dq, dk, dv = attend_back(qs, cs[0], ls[0], pk_ref[...], pv_ref[...], visible)
        dq_ref[t] = dq
        dpk_ref[...] += dk
        dpv_ref[...] += dv
        return carry

    lax.fori_loop(0, 4, tile, 0)

    second = {}
    for axis, full in arrays:
        plus, minus = first[axis]
        plus.wait_recv()
        part = full.at[owner(axis, -1, 0), pl.ds(0, half)]
        fwd = send(part, part, along(axis, 1))
        whole = full.at[owner(axis, -1, 0)]
        wide[axis].append((-1, [send(whole, whole, along(1 - axis, s)) for s in (1, -1)]))
        minus.wait_recv()
        part = full.at[owner(axis, 1, 0), pl.ds(half, half)]
        bwd = send(part, part, along(axis, -1))
        whole = full.at[owner(axis, 1, 0)]
        wide[axis].append((1, [send(whole, whole, along(1 - axis, s)) for s in (1, -1)]))
        second[axis] = (fwd, bwd)

    lax.fori_loop(4, BLOCKS, tile, 0)
    dpk_ref[...] = dpk_ref[...] * (SCALE / POOL_BLOCK)
    dpv_ref[...] = dpv_ref[...] * (1.0 / POOL_BLOCK)

    last = []

    def across(axis, full, o, pair):
        plus, minus = pair
        plus.wait_recv()
        part = full.at[owner(axis, o, -1), pl.ds(0, half)]
        last.append(send(part, part, along(1 - axis, 1)))
        minus.wait_recv()
        part = full.at[owner(axis, o, 1), pl.ds(half, half)]
        last.append(send(part, part, along(1 - axis, -1)))

    for axis, full in arrays:
        across(axis, full, *wide[axis][0])
    for axis, full in arrays:
        for copy in second[axis]:
            copy.wait_recv()
        whole = full.at[owner(axis, 2, 0)]
        wide[axis].append((2, [send(whole, whole, along(1 - axis, s)) for s in (1, -1)]))
    rows = TOKENS // 16
    plus, minus = x_first
    plus.wait_recv()
    whole = h_all.at[shifted(cx, -1) * 2 + core]
    part = whole.at[pl.ds(0, rows)]
    x_second = [send(part, part, xdev(1, core))]
    x_over.append(send(whole, whole, xdev(0, 1 - core)))
    minus.wait_recv()
    whole = h_all.at[shifted(cx, 1) * 2 + core]
    part = whole.at[pl.ds(rows, rows)]
    x_second.append(send(part, part, xdev(-1, core)))
    x_over.append(send(whole, whole, xdev(0, 1 - core)))
    for i in (1, 2):
        for axis, full in arrays:
            across(axis, full, *wide[axis][i])
    for copy in x_second:
        copy.wait_recv()
    whole = h_all.at[shifted(cx, 2) * 2 + core]
    x_over.append(send(whole, whole, xdev(0, 1 - core)))
    for axis, full in arrays:
        across(axis, full, *wide[axis][3])
    for copy in last:
        copy.wait_recv()
    for copy in x_over:
        copy.wait_recv()
    pool_sender.finish()
    send.finish()


GATHER_COPIES = 2 * (2 + 2 + 8 + 8) + 2 + 2 + 4


def run_gather(k, v, h, q, g, gates, sums):
    hbm = pl.BlockSpec(memory_space=pltpu.HBM)
    vmem = pl.BlockSpec(memory_space=pltpu.VMEM)
    n_pool = OWNERS * POOLED
    wide_q = GROUP * QUERY_BLOCK
    return pl.pallas_call(
        gather_kernel,
        name="gather",
        out_shape=(
            jax.ShapeDtypeStruct((OWNERS, TOKENS, HEAD_DIM), BF16),
            jax.ShapeDtypeStruct((OWNERS, TOKENS, HEAD_DIM), BF16),
            jax.ShapeDtypeStruct((8, TOKENS // 8, MODEL), BF16),
            jax.ShapeDtypeStruct((BLOCKS, HEAD_DIM, wide_q), F32),
            jax.ShapeDtypeStruct((n_pool, HEAD_DIM), F32),
            jax.ShapeDtypeStruct((n_pool, HEAD_DIM), F32),
            jax.ShapeDtypeStruct((BLOCKS, wide_q, HEAD_DIM), BF16),
            jax.ShapeDtypeStruct((BLOCKS, wide_q, HEAD_DIM), BF16),
            jax.ShapeDtypeStruct((BLOCKS, 1, wide_q), F32),
        ),
        in_specs=[hbm] * 7,
        out_specs=(vmem,) * 9,
        scratch_shapes=[
            pltpu.VMEM(q.shape, BF16),
            pltpu.VMEM(g.shape, BF16),
            pltpu.VMEM(gates.shape, F32),
            pltpu.VMEM(sums.shape, F32),
            pltpu.VMEM((OWNERS, 2, POOLED, HEAD_DIM), BF16),
            pltpu.VMEM((n_pool, HEAD_DIM), BF16),
            pltpu.VMEM((n_pool, HEAD_DIM), BF16),
            pltpu.VMEM((2, POOLED, HEAD_DIM), BF16),
            pltpu.SemaphoreType.DMA((OWNERS - 1,)),
            pltpu.SemaphoreType.DMA((OWNERS - 1,)),
            pltpu.SemaphoreType.DMA((GATHER_COPIES,)),
            pltpu.SemaphoreType.DMA((GATHER_COPIES,)),
            pltpu.SemaphoreType.DMA((7,)),
        ],
        compiler_params=pltpu.CompilerParams(
            collective_id=0, has_side_effects=True, vmem_limit_bytes=12 * MIB
        ),
        cost_estimate=pl.CostEstimate(
            flops=40_000_000_000, bytes_accessed=8 * MIB, transcendentals=0
        ),
    )(*(pltpu.with_memory_space_constraint(a, pltpu.HBM) for a in (k, v, h, q, g, gates, sums)))


class Reduce:
    def __init__(self, send, axis, src, bufs, coords, along):
        self.relay, self.direct, self.comb, self.relay2, self.direct2, self.comb2 = bufs
        self.send, self.axis, self.src = send, axis, src
        self.c1, self.c2 = (coords[0], coords[1]) if axis == 0 else (coords[1], coords[0])
        self.to1 = lambda o: along(axis, o)
        self.to2 = lambda o: along(1 - axis, o)
        self.half = src.shape[2] // 2
        self.rows = (pl.ds(0, self.half), pl.ds(self.half, self.half))

    def bundle(self, o, n):
        c = shifted(self.c1, o)
        rows = self.rows[n]
        return self.src.at[c, :, rows] if self.axis == 0 else self.src.at[:, c, rows]

    def piece(self, o, i, n):
        c = shifted(self.c1, o)
        if self.axis == 0:
            return self.src[c, i, self.rows[n], :].astype(F32)
        return self.src[i, c, self.rows[n], :].astype(F32)

    def part(self, o, n):
        return self.comb.at[n, shifted(self.c2, o)]

    def begin(self):
        s = self.send
        self.r = [
            s(self.bundle(2, 0), self.relay.at[0], self.to1(1)),
            s(self.bundle(2, 1), self.relay.at[1], self.to1(-1)),
        ]
        self.d = [
            s(self.bundle(1, 1), self.direct.at[0], self.to1(1)),
            s(self.bundle(-1, 0), self.direct.at[1], self.to1(-1)),
        ]

    def combine(self):
        self.c = []
        for n, o in enumerate((1, -1)):
            self.r[n].wait_recv()

            def add(i, carry, n=n, o=o):
                self.relay[n, i] = (self.piece(o, i, n) + self.relay[n, i].astype(F32)).astype(BF16)
                return carry

            lax.fori_loop(0, SIDE, add, 0)
            self.c.append(self.send(self.relay.at[n], self.comb.at[n], self.to1(o)))

    def turn(self):
        for copy in self.d + self.c:
            copy.wait_recv()

        def add(i, carry):
            for n in (0, 1):
                self.comb[n, i] = (
                    self.piece(0, i, n)
                    + self.comb[n, i].astype(F32)
                    + self.direct[1 - n, i].astype(F32)
                ).astype(BF16)
            return carry

        lax.fori_loop(0, SIDE, add, 0)
        s = self.send
        self.r = [
            s(self.part(2, 0), self.relay2.at[0], self.to2(1)),
            s(self.part(2, 1), self.relay2.at[1], self.to2(-1)),
        ]
        self.d = [
            s(self.part(1, 1), self.direct2.at[0], self.to2(1)),
            s(self.part(-1, 0), self.direct2.at[1], self.to2(-1)),
        ]

    def combine2(self):
        self.c = []
        for n, o in enumerate((1, -1)):
            self.r[n].wait_recv()
            self.relay2[n] = (
                self.comb[n, shifted(self.c2, o)].astype(F32) + self.relay2[n].astype(F32)
            ).astype(BF16)
            self.c.append(self.send(self.relay2.at[n], self.comb2.at[n], self.to2(o)))

    def end(self):
        for copy in self.d + self.c:
            copy.wait_recv()
        return [
            self.comb[n, self.c2].astype(F32)
            + self.comb2[n].astype(F32)
            + self.direct2[1 - n].astype(F32)
            for n in (0, 1)
        ]


def reduce_buffers(rows, lanes):
    half = rows // 2
    wide = pltpu.VMEM((2, SIDE, half, lanes), BF16)
    slim = pltpu.VMEM((2, half, lanes), BF16)
    return [wide] * 3 + [slim] * 3


REDUCE_BUFS = 6
GW_COLS = MODEL // OWNERS
PAIR = GROUP // 2 * HEAD_DIM
PAIR_Q = GROUP // 2 * QUERY_BLOCK
UNROLL = 4
HALF_BLOCK = KEY_BLOCK // 2
SETS = CHOSEN * KEY_BLOCK


def scatter_kernel(
    chosen_ref, k_ref, v_ref, h_ref, dqp_ref, dpk_ref, dpv_ref, qs_all, cs_all, ls_rows,
    gq_ref, gk_out, gv_out, gw_out,
    kb, vb, dk_set, dv_set, gqt, dk0, dv0, dk1, dv1, gw0, gw1, gw2, gw3, *rest
):
    bufs = [rest[i * REDUCE_BUFS : (i + 1) * REDUCE_BUFS] for i in range(8)]
    send_sems, recv_sems = rest[8 * REDUCE_BUFS :]
    kv, tp, cz, cy, cx, core = place()

    def along(axis, o):
        if axis == 0:
            return (shifted(cz, o) * SIDE + cy, tp)
        return (cz * SIDE + shifted(cy, o), tp)

    peers = [along(axis, o) for axis in (0, 1) for o in (1, -1)]
    greet(peers)
    send = Sender(send_sems, recv_sems)
    gws = (gw0, gw1, gw2, gw3)
    kv_parts = (dk0, dv0, dk1, dv1)
    k0, v0, k1, v1, w0, w1, w2, w3 = [
        Reduce(send, axis, src, buf, (cz, cy), along)
        for axis, src, buf in zip((0, 1) * 4, kv_parts + gws, bufs)
    ]

    ahead = (
        lax.broadcasted_iota(jnp.int32, (KEY_BLOCK, PAIR_Q), 0)
        - lax.broadcasted_iota(jnp.int32, (KEY_BLOCK, PAIR_Q), 1) % QUERY_BLOCK
    )

    def attend(pair):
        across = slice(pair * PAIR_Q, (pair + 1) * PAIR_Q)

        def block(b, carry):
            start_row = kv * TOKENS + b * QUERY_BLOCK
            seen = []
            for c in range(CHOSEN):
                at = chosen_ref[b, c]
                kb[c * KEY_BLOCK : (c + 1) * KEY_BLOCK, :] = k_ref[at]
                vb[c * KEY_BLOCK : (c + 1) * KEY_BLOCK, :] = v_ref[at]
                seen.append(ahead <= start_row - at * KEY_BLOCK)
            dq, dk, dv = attend_back(
                qs_all[b, across, :],
                cs_all[b, across, :],
                ls_rows[b, :, across],
                kb[...],
                vb[...],
                jnp.concatenate(seen, axis=0),
            )
            total = (dqp_ref[b, :, across] + dq) * SCALE
            rows = pl.ds(pl.multiple_of(b * QUERY_BLOCK, QUERY_BLOCK), QUERY_BLOCK)
            for h in range(GROUP // 2):
                part = total[:, h * QUERY_BLOCK : (h + 1) * QUERY_BLOCK]
                at = pair * PAIR + h * HEAD_DIM
                gqt[at : at + HEAD_DIM, rows] = part.astype(BF16)
                gq_ref[rows, at : at + HEAD_DIM] = part.T.astype(BF16)
            here = pl.ds(pl.multiple_of(b * SETS, SETS), SETS)
            if pair == 0:
                dk_set[here, :] = dk
                dv_set[here, :] = dv
            else:
                dk_set[here, :] += dk
                dv_set[here, :] += dv
            return carry

        return block

    def product(pair):
        def one(j, carry):
            wide = SIDE * GW_COLS
            cols = pl.ds(pl.multiple_of(j * wide, wide), wide)
            part = dot(gqt[pair * PAIR : (pair + 1) * PAIR, :], h_ref[:, cols], NN).astype(BF16)
            for i in range(SIDE):
                piece = part[:, i * GW_COLS : (i + 1) * GW_COLS]
                gws[2 * pair][j, i] = piece[:HEAD_DIM]
                gws[2 * pair + 1][j, i] = piece[HEAD_DIM:]
            return carry

        lax.fori_loop(0, SIDE, one, 0)

    lax.fori_loop(0, BLOCKS, attend(0), 0)
    product(0)
    meet(len(peers))
    w0.begin()
    w1.begin()
    lax.fori_loop(0, BLOCKS // 2, attend(1), 0)
    w0.combine()
    w1.combine()
    lax.fori_loop(BLOCKS // 2, BLOCKS, attend(1), 0)

    product(1)
    w2.begin()
    w3.begin()
    w0.turn()
    w1.turn()

    lane = lax.broadcasted_iota(jnp.int32, (1, BLOCKS * CHOSEN), 1)
    listed = jnp.zeros((1, BLOCKS * CHOSEN), jnp.int32)
    for b in range(BLOCKS):
        for c in range(CHOSEN):
            listed = jnp.where(lane == b * CHOSEN + c, chosen_ref[b, c], listed)
    n_pool = OWNERS * POOLED
    hits = lax.broadcasted_iota(jnp.int32, (n_pool, BLOCKS * CHOSEN), 0) == listed
    hits = jnp.where(hits, 1.0, 0.0).astype(BF16)
    plane = (SIDE, SIDE, POOLED, HEAD_DIM)

    def spread(part):
        dk_out, dv_out = kv_parts[2 * part : 2 * part + 2]

        def one(i, carry):
            every = pl.ds(part * HALF_BLOCK + i, BLOCKS * CHOSEN, stride=KEY_BLOCK)
            got = jnp.concatenate([dk_set[every, :], dv_set[every, :]], axis=1).astype(BF16)
            got = dot(hits, got, NN)
            rows = pl.ds(pl.multiple_of(i * POOLED, POOLED), POOLED)
            dk = got[:, :HEAD_DIM] * SCALE + dpk_ref[...]
            dv = got[:, HEAD_DIM:] + dpv_ref[...]
            dk_out[:, :, rows, :] = dk.astype(BF16).reshape(plane)
            dv_out[:, :, rows, :] = dv.astype(BF16).reshape(plane)
            return carry

        lax.fori_loop(0, HALF_BLOCK, one, 0, unroll=UNROLL)

    spread(0)
    k0.begin()
    v0.begin()
    w2.combine()
    w3.combine()
    w0.combine2()
    w1.combine2()
    spread(1)
    k1.begin()
    v1.begin()
    w2.turn()
    w3.turn()

    def weight(n, w):
        for i, part in enumerate(w.end()):
            at = n * HEAD_DIM + i * HEAD_DIM // 2
            gw_out[:, at : at + HEAD_DIM // 2] = part.T

    def ordered(into, part, r):
        for n, rows in enumerate(r.end()):
            for i in range(HALF_BLOCK // 2):
                at = part * HALF_BLOCK + n * (HALF_BLOCK // 2) + i
                into[pl.ds(at, POOLED, stride=KEY_BLOCK), :] = rows[i * POOLED : (i + 1) * POOLED]

    weight(0, w0)
    weight(1, w1)
    k0.combine()
    v0.combine()
    w2.combine2()
    w3.combine2()
    k1.combine()
    v1.combine()
    weight(2, w2)
    weight(3, w3)
    k0.turn()
    v0.turn()
    k1.turn()
    v1.turn()
    k0.combine2()
    v0.combine2()
    k1.combine2()
    v1.combine2()
    ordered(dk_set, 0, k0)
    ordered(dv_set, 0, v0)
    ordered(dk_set, 1, k1)
    ordered(dv_set, 1, v1)
    gk_out[...] = dk_set[:TOKENS, :].astype(BF16)
    gv_out[...] = dv_set[:TOKENS, :].astype(BF16)
    send.finish()


SCATTER_COPIES = 8 * 12
SCATTER_MIB = 30.7


def run_scatter(chosen, k_all, v_all, h_all, dqp, dpk, dpv, qs, cs, ls):
    vmem = pl.BlockSpec(memory_space=pltpu.VMEM)
    smem = pl.BlockSpec(memory_space=pltpu.SMEM)
    dense = pltpu.VMEM((SIDE, SIDE, TOKENS // 2, HEAD_DIM), BF16)
    grad = pltpu.VMEM((SIDE, SIDE, HEAD_DIM, GW_COLS), BF16)
    return pl.pallas_call(
        scatter_kernel,
        name="scatter",
        out_shape=(
            jax.ShapeDtypeStruct((TOKENS, GROUP * HEAD_DIM), BF16),
            jax.ShapeDtypeStruct((TOKENS, HEAD_DIM), BF16),
            jax.ShapeDtypeStruct((TOKENS, HEAD_DIM), BF16),
            jax.ShapeDtypeStruct((GW_COLS, GROUP * HEAD_DIM), F32),
        ),
        in_specs=[smem] + [vmem] * 9,
        out_specs=(vmem,) * 4,
        scratch_shapes=[
            pltpu.VMEM((SETS, HEAD_DIM), BF16),
            pltpu.VMEM((SETS, HEAD_DIM), BF16),
            pltpu.VMEM((BLOCKS * SETS, HEAD_DIM), F32),
            pltpu.VMEM((BLOCKS * SETS, HEAD_DIM), F32),
            pltpu.VMEM((GROUP * HEAD_DIM, TOKENS), BF16),
            dense,
            dense,
            dense,
            dense,
            grad,
            grad,
            grad,
            grad,
            *(reduce_buffers(TOKENS // 2, HEAD_DIM) * 4),
            *(reduce_buffers(HEAD_DIM, GW_COLS) * 4),
            pltpu.SemaphoreType.DMA((SCATTER_COPIES,)),
            pltpu.SemaphoreType.DMA((SCATTER_COPIES,)),
        ],
        compiler_params=pltpu.CompilerParams(
            collective_id=1, has_side_effects=True, vmem_limit_bytes=int(SCATTER_MIB * MIB)
        ),
    )(chosen, k_all, v_all, h_all, dqp, dpk, dpv, qs, cs, ls)


def finish_kernel(*refs):
    for src, out in zip(refs[:4], refs[4:]):
        out[...] = src[...]


def run_finish(*outs):
    vmem = pl.BlockSpec(memory_space=pltpu.VMEM)
    return pl.pallas_call(
        finish_kernel,
        name="finish",
        out_shape=tuple(jax.ShapeDtypeStruct(a.shape, a.dtype) for a in outs),
        in_specs=[vmem] * 4,
        out_specs=(vmem,) * 4,
        compiler_params=pltpu.CompilerParams(vmem_limit_bytes=8 * MIB),
    )(*outs)


def body(hidden_rows, queries, key_rows, value_rows, branch_gates, log_sums, chosen, out_grad):
    k_all, v_all, h_all, *pooled = run_gather(
        key_rows, value_rows, hidden_rows, queries, out_grad, branch_gates, log_sums
    )
    outs = run_scatter(
        chosen.reshape(BLOCKS, CHOSEN),
        k_all.reshape(SEQ // KEY_BLOCK, KEY_BLOCK, HEAD_DIM),
        v_all.reshape(SEQ // KEY_BLOCK, KEY_BLOCK, HEAD_DIM),
        h_all.reshape(TOKENS, MODEL),
        *pooled,
    )
    return run_finish(*outs)


def solution(mesh):
    placed = (
        P(("kv", "tp"), None),
        P("kv", "tp"),
        P("kv", "tp"),
        P("kv", "tp"),
        P(None, "tp", "kv"),
        P(None, "tp", "kv"),
        P("tp", "kv", None),
        P("kv", "tp"),
    )
    return jax.shard_map(
        body,
        mesh=mesh,
        in_specs=placed,
        out_specs=(P("kv", "tp"), P("kv", "tp"), P("kv", "tp"), P("kv", "tp")),
        check_vma=False,
    )
```

```python
import jax
import jax.numpy as jnp
from jax import lax
from jax.experimental import pallas as pl
from jax.experimental.pallas import tpu as pltpu
from jax.sharding import PartitionSpec as P

HEADS = 32
KV_HEADS = 8
HEAD_DIM = 128
QUERY_BLOCK = 128
KEY_BLOCK = 32
POOL_BLOCK = 32
CHOSEN = 16
GROUP = HEADS // KV_HEADS
SIDE = 4
OWNERS = SIDE * SIDE
TOKENS = 1024
BLOCKS = TOKENS // QUERY_BLOCK
POOLED = TOKENS // POOL_BLOCK
SEQ = TOKENS * OWNERS
LISTED = BLOCKS * CHOSEN
SLOTS = OWNERS * CHOSEN
MODEL = 4096
SCALE = HEAD_DIM ** (-0.5)
LOG2E = 1.4426950408889634
MIB = 1 << 20
MESH = pl.DeviceIdType.MESH
F32 = jnp.float32
BF16 = jnp.bfloat16

NT = (((1,), (1,)), ((), ()))
NN = (((1,), (0,)), ((), ()))


def dot(a, b, dims):
    return lax.dot_general(a, b, dims, preferred_element_type=F32)


class Sender:
    def __init__(self, send_sems, recv_sems):
        self.send_sems, self.recv_sems, self.at, self.sent = send_sems, recv_sems, 0, []

    def __call__(self, src, dst, dev):
        copy = pltpu.make_async_remote_copy(
            src_ref=src,
            dst_ref=dst,
            send_sem=self.send_sems.at[self.at],
            recv_sem=self.recv_sems.at[self.at],
            device_id=dev,
            device_id_type=MESH,
        )
        self.at += 1
        copy.start()
        self.sent.append(copy)
        return copy

    def finish(self):
        for copy in self.sent:
            copy.wait_send()


def place():
    kv, tp = lax.axis_index("kv"), lax.axis_index("tp")
    return kv, tp, kv // SIDE, kv % SIDE, tp // 2, tp % 2


def shifted(c, o):
    return (c + (o + SIDE)) % SIDE


def greet(devices):
    for dev in devices:
        pl.semaphore_signal(
            pltpu.get_barrier_semaphore(), inc=1, device_id=dev, device_id_type=MESH
        )


def meet(count):
    pl.semaphore_wait(pltpu.get_barrier_semaphore(), count)


def tile_operands(q_ref, g_ref, gate_ref, ls_ref, t):
    rows = pl.ds(pl.multiple_of(t * QUERY_BLOCK, QUERY_BLOCK), QUERY_BLOCK)
    gates = jnp.concatenate([gate_ref[0, :, rows], gate_ref[1, :, rows]], axis=0).T
    qs, cs, ls = [], ([], []), ([], [])
    for h in range(GROUP):
        cols = slice(h * HEAD_DIM, (h + 1) * HEAD_DIM)
        qs.append(q_ref[rows, cols])
        grad = g_ref[rows, cols].astype(F32)
        for branch in (0, 1):
            at = branch * GROUP + h
            cs[branch].append((gates[:, at : at + 1] * grad).astype(BF16))
            ls[branch].append(ls_ref[branch, h : h + 1, rows])
    return (
        jnp.concatenate(qs, axis=0),
        [jnp.concatenate(c, axis=0) for c in cs],
        [jnp.concatenate(x, axis=1) * LOG2E for x in ls],
    )


def attend_back(qs, cs, log_sum, keys, values, visible):
    scores = dot(keys, qs, NT) * (SCALE * LOG2E)
    p = jnp.where(visible, jnp.exp2(scores - log_sum), 0.0)
    pr = p.astype(BF16)
    dp = dot(values, cs, NT)
    delta = jnp.sum(pr.astype(F32) * dp, axis=0, keepdims=True)
    ds = (p * (dp - delta)).astype(BF16)
    return dot(keys.T, ds, NN), dot(ds, qs, NN), dot(pr, cs, NN)


def gather_kernel(
    k_ref, v_ref, h_ref, q_hbm, g_hbm, gate_hbm, ls_hbm, chosen_hbm,
    k_all, v_all, h_all, dq_ref, dpk_ref, dpv_ref, qs_all, cs_all, ls_rows, pick_ref, place_ref,
    chosen_ref, q_ref, g_ref, gate_ref, ls_ref, pool_all, pk_ref, pv_ref, pool_here,
    pool_send, pool_recv, send_sems, recv_sems, local_sems,
):
    kv, tp, cz, cy, cx, core = place()
    half = TOKENS // 2

    def device(oz, oy):
        return (shifted(cz, oz) * SIDE + shifted(cy, oy), tp)

    def along(axis, o):
        return device(o, 0) if axis == 0 else device(0, o)

    def owner(axis, o1, o2):
        a, b = (o1, o2) if axis == 0 else (o2, o1)
        return shifted(cz, a) * SIDE + shifted(cy, b)

    def xdev(o, c):
        return (kv, shifted(cx, o) * 2 + c)

    others = [(oz, oy) for oz in range(SIDE) for oy in range(SIDE) if (oz, oy) != (0, 0)]
    peers = [device(oz, oy) for oz, oy in others] + [
        xdev(1, core), xdev(-1, core), xdev(0, 1 - core)
    ]
    greet(peers)
    local = [
        pltpu.make_async_copy(src, dst, local_sems.at[i])
        for i, (src, dst) in enumerate(
            (
                (k_ref, k_all.at[kv]),
                (v_ref, v_all.at[kv]),
                (h_ref, h_all.at[tp]),
                (chosen_hbm, chosen_ref),
                (gate_hbm, gate_ref),
                (ls_hbm, ls_ref),
                (q_hbm, q_ref),
                (g_hbm, g_ref),
            )
        )
    ]
    for copy in local:
        copy.start()

    blk = lax.broadcasted_iota(jnp.int32, (POOLED, TOKENS), 0)
    row = lax.broadcasted_iota(jnp.int32, (POOLED, TOKENS), 1)
    mean = jnp.where(row // POOL_BLOCK == blk, 1.0 / POOL_BLOCK, 0.0).astype(BF16)
    local[0].wait()
    pool_here[0] = dot(mean, k_all[kv], NN).astype(BF16)
    local[1].wait()
    pool_here[1] = dot(mean, v_all[kv], NN).astype(BF16)

    local[3].wait()
    lane = lax.broadcasted_iota(jnp.int32, (1, LISTED), 1)
    listed = jnp.zeros((1, LISTED), jnp.int32)
    for b in range(BLOCKS):
        for c in range(CHOSEN):
            listed = jnp.where(lane == b * CHOSEN + c, chosen_ref[b, c], listed)
    row = lax.broadcasted_iota(jnp.int32, (POOLED, LISTED), 0)
    both = jnp.where(row == 0, listed // POOLED, jnp.where(row == 1, listed % POOLED, 0))
    pool_here[2] = both.astype(F32).astype(BF16)
    meet(len(peers))

    pool_sender = Sender(pool_send, pool_recv)
    for oz, oy in others:
        pool_sender(pool_here, pool_all.at[kv], device(oz, oy))
    pool_all[kv] = pool_here[...]

    send = Sender(send_sems, recv_sems)
    first, wide = {}, {}
    arrays = ((0, k_all), (1, v_all))
    for axis, full in arrays:
        here = full.at[kv]
        first[axis] = [send(here, here, along(axis, s)) for s in (1, -1)]
    local[2].wait()
    here = h_all.at[tp]
    x_first = [send(here, here, xdev(s, core)) for s in (1, -1)]
    x_over = [send(here, here, xdev(0, 1 - core))]
    for axis, full in arrays:
        here = full.at[kv]
        wide[axis] = [(0, [send(here, here, along(1 - axis, s)) for s in (1, -1)])]

    for copy in local[4:]:
        copy.wait()
    for copy in pool_sender.sent:
        copy.wait_recv()
    pk_ref[...] = pool_all[:, 0].reshape(OWNERS * POOLED, HEAD_DIM)
    pv_ref[...] = pool_all[:, 1].reshape(OWNERS * POOLED, HEAD_DIM)
    dpk_ref[...] = jnp.zeros_like(dpk_ref)
    dpv_ref[...] = jnp.zeros_like(dpv_ref)

    def listing(i):
        both = pool_all[i, 2].astype(F32)
        owners, numbers, column = both[0:1, :], both[1:2, :], both.T[:, 0:1]
        one = lax.broadcasted_iota(jnp.int32, (LISTED, LISTED), 0)
        two = lax.broadcasted_iota(jnp.int32, (LISTED, LISTED), 1)
        same = jnp.where(column == owners, 1.0, 0.0)
        rank = jnp.sum(jnp.where(one < two, same, 0.0), axis=0, keepdims=True)
        return owners, numbers, rank

    def grid(rows, f):
        return f(lax.broadcasted_iota(jnp.int32, (rows, LISTED), 0)).astype(F32)

    def ones(seen):
        return jnp.where(seen, 1.0, 0.0)

    owners, numbers, rank = listing(kv)
    kv_f = kv.astype(F32)
    at, nth = grid(SLOTS, lambda i: i // CHOSEN), grid(SLOTS, lambda i: i % CHOSEN)
    own = jnp.where(owners == kv_f, -1.0, owners)
    pick_ref[:SLOTS] = (ones(own == at) * ones(rank == nth)).astype(BF16)
    at = grid(POOLED, lambda i: i)
    pick_ref[SLOTS:] = (ones(owners == kv_f) * ones(numbers == at)).astype(BF16)

    for axis in (0, 1):
        def owner_id(i, axis=axis):
            return cz * SIDE + i if axis == 0 else i * SIDE + cy

        for pair in (0, 1):
            total = None
            for n in (0, 1):
                who = owner(axis, (0, -1, 1, 2)[2 * pair + n], 0)
                owners, numbers, rank = listing(who)
                at = grid(LISTED, lambda i: owner_id(i // POOLED))
                nth = grid(LISTED, lambda i: i % POOLED)
                blocks = ones(owners == at) * ones(numbers == nth)
                at = grid(LISTED, lambda i: owner_id((i % 64) // CHOSEN))
                nth = grid(LISTED, lambda i, n=n: jnp.where(i // 64 == n, i % CHOSEN, -1))
                own = jnp.where(owners == who.astype(F32), -1.0, owners)
                slots = ones(own == at) * ones(rank == nth)
                part = dot(blocks.astype(BF16), slots.astype(BF16), NT)
                total = part if total is None else total + part
            place_ref[axis, :, pair * LISTED : (pair + 1) * LISTED] = total.astype(BF16)

    n_pool = OWNERS * POOLED
    wide_q = GROUP * QUERY_BLOCK
    pool_end = lax.broadcasted_iota(jnp.int32, (n_pool, wide_q), 0) * POOL_BLOCK + POOL_BLOCK - 1
    lane = lax.broadcasted_iota(jnp.int32, (n_pool, wide_q), 1) % QUERY_BLOCK
    ahead = pool_end - lane

    def tile(t, carry):
        qs, cs, ls = tile_operands(q_ref, g_ref, gate_ref, ls_ref, t)
        qs_all[t] = qs
        cs_all[t] = cs[1]
        ls_rows[t] = ls[1]
        visible = ahead <= kv * TOKENS + t * QUERY_BLOCK
        dq, dk, dv = attend_back(qs, cs[0], ls[0], pk_ref[...], pv_ref[...], visible)
        dq_ref[t] = dq
        dpk_ref[...] += dk
        dpv_ref[...] += dv
        return carry

    lax.fori_loop(0, 4, tile, 0)

    second = {}
    for axis, full in arrays:
        plus, minus = first[axis]
        plus.wait_recv()
        part = full.at[owner(axis, -1, 0), pl.ds(0, half)]
        fwd = send(part, part, along(axis, 1))
        whole = full.at[owner(axis, -1, 0)]
        wide[axis].append((-1, [send(whole, whole, along(1 - axis, s)) for s in (1, -1)]))
        minus.wait_recv()
        part = full.at[owner(axis, 1, 0), pl.ds(half, half)]
        bwd = send(part, part, along(axis, -1))
        whole = full.at[owner(axis, 1, 0)]
        wide[axis].append((1, [send(whole, whole, along(1 - axis, s)) for s in (1, -1)]))
        second[axis] = (fwd, bwd)

    lax.fori_loop(4, BLOCKS, tile, 0)
    dpk_ref[...] = dpk_ref[...] * (SCALE / POOL_BLOCK)
    dpv_ref[...] = dpv_ref[...] * (1.0 / POOL_BLOCK)

    last = []

    def across(axis, full, o, pair):
        plus, minus = pair
        plus.wait_recv()
        part = full.at[owner(axis, o, -1), pl.ds(0, half)]
        last.append(send(part, part, along(1 - axis, 1)))
        minus.wait_recv()
        part = full.at[owner(axis, o, 1), pl.ds(half, half)]
        last.append(send(part, part, along(1 - axis, -1)))

    for axis, full in arrays:
        across(axis, full, *wide[axis][0])
    for axis, full in arrays:
        for copy in second[axis]:
            copy.wait_recv()
        whole = full.at[owner(axis, 2, 0)]
        wide[axis].append((2, [send(whole, whole, along(1 - axis, s)) for s in (1, -1)]))
    rows = TOKENS // 16
    plus, minus = x_first
    plus.wait_recv()
    whole = h_all.at[shifted(cx, -1) * 2 + core]
    part = whole.at[pl.ds(0, rows)]
    x_second = [send(part, part, xdev(1, core))]
    x_over.append(send(whole, whole, xdev(0, 1 - core)))
    minus.wait_recv()
    whole = h_all.at[shifted(cx, 1) * 2 + core]
    part = whole.at[pl.ds(rows, rows)]
    x_second.append(send(part, part, xdev(-1, core)))
    x_over.append(send(whole, whole, xdev(0, 1 - core)))
    for i in (1, 2):
        for axis, full in arrays:
            across(axis, full, *wide[axis][i])
    for copy in x_second:
        copy.wait_recv()
    whole = h_all.at[shifted(cx, 2) * 2 + core]
    x_over.append(send(whole, whole, xdev(0, 1 - core)))
    for axis, full in arrays:
        across(axis, full, *wide[axis][3])
    for copy in last:
        copy.wait_recv()
    for copy in x_over:
        copy.wait_recv()
    pool_sender.finish()
    send.finish()


GATHER_COPIES = 2 * (2 + 2 + 8 + 8) + 2 + 2 + 4


def run_gather(k, v, h, q, g, gates, sums, chosen):
    hbm = pl.BlockSpec(memory_space=pltpu.HBM)
    vmem = pl.BlockSpec(memory_space=pltpu.VMEM)
    n_pool = OWNERS * POOLED
    wide_q = GROUP * QUERY_BLOCK
    return pl.pallas_call(
        gather_kernel,
        name="gather",
        out_shape=(
            jax.ShapeDtypeStruct((OWNERS, TOKENS, HEAD_DIM), BF16),
            jax.ShapeDtypeStruct((OWNERS, TOKENS, HEAD_DIM), BF16),
            jax.ShapeDtypeStruct((8, TOKENS // 8, MODEL), BF16),
            jax.ShapeDtypeStruct((BLOCKS, HEAD_DIM, wide_q), F32),
            jax.ShapeDtypeStruct((n_pool, HEAD_DIM), F32),
            jax.ShapeDtypeStruct((n_pool, HEAD_DIM), F32),
            jax.ShapeDtypeStruct((BLOCKS, wide_q, HEAD_DIM), BF16),
            jax.ShapeDtypeStruct((BLOCKS, wide_q, HEAD_DIM), BF16),
            jax.ShapeDtypeStruct((BLOCKS, 1, wide_q), F32),
            jax.ShapeDtypeStruct((SLOTS + POOLED, LISTED), BF16),
            jax.ShapeDtypeStruct((2, LISTED, SLOTS), BF16),
        ),
        in_specs=[hbm] * 8,
        out_specs=(vmem,) * 11,
        scratch_shapes=[
            pltpu.SMEM((BLOCKS, CHOSEN), jnp.int32),
            pltpu.VMEM(q.shape, BF16),
            pltpu.VMEM(g.shape, BF16),
            pltpu.VMEM(gates.shape, F32),
            pltpu.VMEM(sums.shape, F32),
            pltpu.VMEM((OWNERS, 3, POOLED, HEAD_DIM), BF16),
            pltpu.VMEM((n_pool, HEAD_DIM), BF16),
            pltpu.VMEM((n_pool, HEAD_DIM), BF16),
            pltpu.VMEM((3, POOLED, HEAD_DIM), BF16),
            pltpu.SemaphoreType.DMA((OWNERS - 1,)),
            pltpu.SemaphoreType.DMA((OWNERS - 1,)),
            pltpu.SemaphoreType.DMA((GATHER_COPIES,)),
            pltpu.SemaphoreType.DMA((GATHER_COPIES,)),
            pltpu.SemaphoreType.DMA((8,)),
        ],
        compiler_params=pltpu.CompilerParams(
            collective_id=0, has_side_effects=True, vmem_limit_bytes=12 * MIB
        ),
        cost_estimate=pl.CostEstimate(
            flops=40_000_000_000, bytes_accessed=8 * MIB, transcendentals=0
        ),
    )(*(pltpu.with_memory_space_constraint(a, pltpu.HBM) for a in (k, v, h, q, g, gates, sums, chosen)))


class Reduce:
    def __init__(self, send, axis, src, bufs, coords, along):
        self.relay, self.direct, self.comb, self.relay2, self.direct2, self.comb2 = bufs
        self.send, self.axis, self.src = send, axis, src
        self.c1, self.c2 = (coords[0], coords[1]) if axis == 0 else (coords[1], coords[0])
        self.to1 = lambda o: along(axis, o)
        self.to2 = lambda o: along(1 - axis, o)
        self.half = src.shape[2] // 2
        self.rows = (pl.ds(0, self.half), pl.ds(self.half, self.half))

    def bundle(self, o, n):
        c = shifted(self.c1, o)
        rows = self.rows[n]
        return self.src.at[c, :, rows] if self.axis == 0 else self.src.at[:, c, rows]

    def piece(self, o, i, n):
        c = shifted(self.c1, o)
        if self.axis == 0:
            return self.src[c, i, self.rows[n], :].astype(F32)
        return self.src[i, c, self.rows[n], :].astype(F32)

    def part(self, o, n):
        return self.comb.at[n, shifted(self.c2, o)]

    def begin(self):
        s = self.send
        self.r = [
            s(self.bundle(2, 0), self.relay.at[0], self.to1(1)),
            s(self.bundle(2, 1), self.relay.at[1], self.to1(-1)),
        ]
        self.d = [
            s(self.bundle(1, 1), self.direct.at[0], self.to1(1)),
            s(self.bundle(-1, 0), self.direct.at[1], self.to1(-1)),
        ]

    def combine(self):
        self.c = []
        for n, o in enumerate((1, -1)):
            self.r[n].wait_recv()

            def add(i, carry, n=n, o=o):
                self.relay[n, i] = (self.piece(o, i, n) + self.relay[n, i].astype(F32)).astype(BF16)
                return carry

            lax.fori_loop(0, SIDE, add, 0)
            self.c.append(self.send(self.relay.at[n], self.comb.at[n], self.to1(o)))

    def turn(self):
        for copy in self.d + self.c:
            copy.wait_recv()

        def add(i, carry):
            for n in (0, 1):
                self.comb[n, i] = (
                    self.piece(0, i, n)
                    + self.comb[n, i].astype(F32)
                    + self.direct[1 - n, i].astype(F32)
                ).astype(BF16)
            return carry

        lax.fori_loop(0, SIDE, add, 0)
        self.start_second()

    def start_second(self):
        s = self.send
        self.r = [
            s(self.part(2, 0), self.relay2.at[0], self.to2(1)),
            s(self.part(2, 1), self.relay2.at[1], self.to2(-1)),
        ]
        self.d = [
            s(self.part(1, 1), self.direct2.at[0], self.to2(1)),
            s(self.part(-1, 0), self.direct2.at[1], self.to2(-1)),
        ]

    def combine2(self):
        self.c = []
        for n, o in enumerate((1, -1)):
            self.r[n].wait_recv()
            self.relay2[n] = (
                self.comb[n, shifted(self.c2, o)].astype(F32) + self.relay2[n].astype(F32)
            ).astype(BF16)
            self.c.append(self.send(self.relay2.at[n], self.comb2.at[n], self.to2(o)))

    def end(self):
        for copy in self.d + self.c:
            copy.wait_recv()
        return [
            self.comb[n, self.c2].astype(F32)
            + self.comb2[n].astype(F32)
            + self.direct2[1 - n].astype(F32)
            for n in (0, 1)
        ]


class ListedReduce(Reduce):
    def __init__(self, send, axis, src, bufs, coords, along, place_ref, own):
        self.passed, self.far, self.near, *after = bufs
        super().__init__(send, axis, src, (None, None, *after), coords, along)
        self.place_ref, self.own = place_ref, own
        self.steps = HALF_BLOCK * CHOSEN
        self.pooled = self

    def begin(self):
        s = self.send
        every = pl.ds(0, self.src.shape[2])
        self.rows = self.rows + (every,)
        self.r = [
            s(self.bundle(2, 0), self.passed.at[0], self.to1(1)),
            s(self.bundle(2, 1), self.passed.at[1], self.to1(-1)),
        ]
        self.d = [
            s(self.bundle(1, 2), self.near.at[0], self.to1(1)),
            s(self.bundle(-1, 2), self.near.at[1], self.to1(-1)),
        ]

    def combine(self):
        self.c = []
        for n, o in enumerate((1, -1)):
            self.r[n].wait_recv()
            self.c.append(self.send(self.passed.at[n], self.far.at[:, self.rows[n]], self.to1(o)))

    def sources(self, rows):
        mine = self.src[self.c1, :, rows, :] if self.axis == 0 else self.src[:, self.c1, rows, :]
        return [mine, self.near[0, :, rows, :], self.near[1, :, rows, :], self.far[:, rows, :]]

    def turn(self):
        for copy in self.d + self.c:
            copy.wait_recv()
        pooled = sum(x.astype(F32) for x in self.pooled.sources(pl.ds(self.steps, POOLED)))
        pooled = pooled.reshape(SIDE * POOLED, HEAD_DIM)
        pooled = jnp.concatenate([pooled, pooled], axis=1)
        for n in (0, 1):

            def put(i, carry, n=n):
                pieces = []
                for j in (0, 1):
                    first = pl.multiple_of((n * HALF_BLOCK // 2 + 2 * i + j) * CHOSEN, CHOSEN)
                    got = [x.reshape(SIDE * CHOSEN, HEAD_DIM) for x in self.sources(pl.ds(first, CHOSEN))]
                    pieces.append(jnp.concatenate(got, axis=0))
                total = dot(self.place_ref[self.axis], jnp.concatenate(pieces, axis=1), NN)
                total = total + pooled
                for j in (0, 1):
                    rows = pl.ds(pl.multiple_of((2 * i + j) * POOLED, POOLED), POOLED)
                    part = total[:, j * HEAD_DIM : (j + 1) * HEAD_DIM].astype(BF16)
                    self.comb[n, :, rows, :] = part.reshape(SIDE, POOLED, HEAD_DIM)
                return carry

            lax.fori_loop(0, HALF_BLOCK // 4, put, 0, unroll=2)
        self.start_second()

    def end(self):
        at = self.own[1]
        size = HALF_BLOCK // 2 * POOLED
        return [
            part + self.own[0][at + n * size : at + (n + 1) * size, :]
            for n, part in enumerate(super().end())
        ]


def listed_buffers(rows):
    half, size = rows // 2, HALF_BLOCK // 2 * POOLED
    slim = pltpu.VMEM((2, size, HEAD_DIM), BF16)
    return [
        pltpu.VMEM((2, SIDE, half, HEAD_DIM), BF16),
        pltpu.VMEM((SIDE, rows, HEAD_DIM), BF16),
        pltpu.VMEM((2, SIDE, rows, HEAD_DIM), BF16),
        pltpu.VMEM((2, SIDE, size, HEAD_DIM), BF16),
        slim, slim, slim,
    ]


def reduce_buffers(rows, lanes):
    half = rows // 2
    wide = pltpu.VMEM((2, SIDE, half, lanes), BF16)
    slim = pltpu.VMEM((2, half, lanes), BF16)
    return [wide] * 3 + [slim] * 3


REDUCE_BUFS = 6
LISTED_BUFS = 7
GW_COLS = MODEL // OWNERS
PAIR = GROUP // 2 * HEAD_DIM
PAIR_Q = GROUP // 2 * QUERY_BLOCK
UNROLL = 4
HALF_BLOCK = KEY_BLOCK // 2
SETS = CHOSEN * KEY_BLOCK


def scatter_kernel(
    chosen_ref, k_ref, v_ref, h_ref, dqp_ref, dpk_ref, dpv_ref, qs_all, cs_all, ls_rows, pick_ref, place_ref,
    gq_ref, gk_out, gv_out, gw_out,
    kb, vb, dk_set, dv_set, gqt, dk0, dv0, dk1, dv1, own_k, own_v, gw0, gw1, gw2, gw3, *rest
):
    cut = 4 * LISTED_BUFS
    bufs = [rest[i * LISTED_BUFS : (i + 1) * LISTED_BUFS] for i in range(4)]
    gw_bufs = [rest[cut + i * REDUCE_BUFS : cut + (i + 1) * REDUCE_BUFS] for i in range(4)]
    send_sems, recv_sems = rest[cut + 4 * REDUCE_BUFS :]
    kv, tp, cz, cy, cx, core = place()

    def along(axis, o):
        if axis == 0:
            return (shifted(cz, o) * SIDE + cy, tp)
        return (cz * SIDE + shifted(cy, o), tp)

    peers = [along(axis, o) for axis in (0, 1) for o in (1, -1)]
    greet(peers)
    send = Sender(send_sems, recv_sems)
    gws = (gw0, gw1, gw2, gw3)
    kv_parts = (dk0, dv0, dk1, dv1)
    half_rows = HALF_BLOCK * POOLED
    owns = ((own_k, 0), (own_v, 0), (own_k, half_rows), (own_v, half_rows))
    k0, v0, k1, v1 = [
        ListedReduce(send, axis, src, buf, (cz, cy), along, place_ref, own)
        for axis, src, buf, own in zip((0, 1) * 2, kv_parts, bufs, owns)
    ]
    k1.pooled, v1.pooled = k0, v0
    w0, w1, w2, w3 = [
        Reduce(send, axis, src, buf, (cz, cy), along)
        for axis, src, buf in zip((0, 1) * 2, gws, gw_bufs)
    ]

    ahead = (
        lax.broadcasted_iota(jnp.int32, (KEY_BLOCK, PAIR_Q), 0)
        - lax.broadcasted_iota(jnp.int32, (KEY_BLOCK, PAIR_Q), 1) % QUERY_BLOCK
    )

    def attend(pair):
        across = slice(pair * PAIR_Q, (pair + 1) * PAIR_Q)

        def block(b, carry):
            start_row = kv * TOKENS + b * QUERY_BLOCK
            seen = []
            for c in range(CHOSEN):
                at = chosen_ref[b, c]
                kb[c * KEY_BLOCK : (c + 1) * KEY_BLOCK, :] = k_ref[at]
                vb[c * KEY_BLOCK : (c + 1) * KEY_BLOCK, :] = v_ref[at]
                seen.append(ahead <= start_row - at * KEY_BLOCK)
            dq, dk, dv = attend_back(
                qs_all[b, across, :],
                cs_all[b, across, :],
                ls_rows[b, :, across],
                kb[...],
                vb[...],
                jnp.concatenate(seen, axis=0),
            )
            total = (dqp_ref[b, :, across] + dq) * SCALE
            rows = pl.ds(pl.multiple_of(b * QUERY_BLOCK, QUERY_BLOCK), QUERY_BLOCK)
            for h in range(GROUP // 2):
                part = total[:, h * QUERY_BLOCK : (h + 1) * QUERY_BLOCK]
                at = pair * PAIR + h * HEAD_DIM
                gqt[at : at + HEAD_DIM, rows] = part.astype(BF16)
                gq_ref[rows, at : at + HEAD_DIM] = part.T.astype(BF16)
            here = pl.ds(pl.multiple_of(b * SETS, SETS), SETS)
            if pair == 0:
                dk_set[here, :] = dk * SCALE
                dv_set[here, :] = dv
            else:
                dk_set[here, :] += dk * SCALE
                dv_set[here, :] += dv
            return carry

        return block

    def product(pair):
        def one(j, carry):
            wide = SIDE * GW_COLS
            cols = pl.ds(pl.multiple_of(j * wide, wide), wide)
            part = dot(gqt[pair * PAIR : (pair + 1) * PAIR, :], h_ref[:, cols], NN).astype(BF16)
            for i in range(SIDE):
                piece = part[:, i * GW_COLS : (i + 1) * GW_COLS]
                gws[2 * pair][j, i] = piece[:HEAD_DIM]
                gws[2 * pair + 1][j, i] = piece[HEAD_DIM:]
            return carry

        lax.fori_loop(0, SIDE, one, 0)

    lax.fori_loop(0, BLOCKS, attend(0), 0)
    product(0)
    meet(len(peers))
    w0.begin()
    w1.begin()
    lax.fori_loop(0, BLOCKS // 2, attend(1), 0)
    w0.combine()
    w1.combine()
    lax.fori_loop(BLOCKS // 2, BLOCKS, attend(1), 0)

    product(1)
    w2.begin()
    w3.begin()
    w0.turn()
    w1.turn()

    slots = (SIDE, SIDE, CHOSEN, HEAD_DIM)

    def spread(part):
        dk_out, dv_out = kv_parts[2 * part : 2 * part + 2]

        def one(i, carry):
            every = pl.ds(part * HALF_BLOCK + i, LISTED, stride=KEY_BLOCK)
            got = jnp.concatenate([dk_set[every, :], dv_set[every, :]], axis=1).astype(BF16)
            got = dot(pick_ref[...], got, NN)
            rows = pl.ds(pl.multiple_of(i * CHOSEN, CHOSEN), CHOSEN)
            dk_out[:, :, rows, :] = got[:SLOTS, :HEAD_DIM].astype(BF16).reshape(slots)
            dv_out[:, :, rows, :] = got[:SLOTS, HEAD_DIM:].astype(BF16).reshape(slots)
            rows = pl.ds(pl.multiple_of((part * HALF_BLOCK + i) * POOLED, POOLED), POOLED)
            own_k[rows, :] = got[SLOTS:, :HEAD_DIM]
            own_v[rows, :] = got[SLOTS:, HEAD_DIM:]
            return carry

        lax.fori_loop(0, HALF_BLOCK, one, 0, unroll=UNROLL)

    tail = slice(HALF_BLOCK * CHOSEN, HALF_BLOCK * CHOSEN + POOLED)
    pooled = (SIDE, SIDE, POOLED, HEAD_DIM)
    dk0[:, :, tail, :] = dpk_ref[...].astype(BF16).reshape(pooled)
    dv0[:, :, tail, :] = dpv_ref[...].astype(BF16).reshape(pooled)
    spread(0)
    k0.begin()
    v0.begin()
    w2.combine()
    w3.combine()
    w0.combine2()
    w1.combine2()
    spread(1)
    k1.begin()
    v1.begin()
    w2.turn()
    w3.turn()

    def weight(n, w):
        for i, part in enumerate(w.end()):
            at = n * HEAD_DIM + i * HEAD_DIM // 2
            gw_out[:, at : at + HEAD_DIM // 2] = part.T

    def ordered(into, part, r):
        for n, rows in enumerate(r.end()):
            for i in range(HALF_BLOCK // 2):
                at = part * HALF_BLOCK + n * (HALF_BLOCK // 2) + i
                into[pl.ds(at, POOLED, stride=KEY_BLOCK), :] = rows[i * POOLED : (i + 1) * POOLED]

    weight(0, w0)
    weight(1, w1)
    k0.combine()
    v0.combine()
    w2.combine2()
    w3.combine2()
    k1.combine()
    v1.combine()
    weight(2, w2)
    weight(3, w3)
    k0.turn()
    v0.turn()
    k1.turn()
    v1.turn()
    k0.combine2()
    v0.combine2()
    k1.combine2()
    v1.combine2()
    ordered(dk_set, 0, k0)
    ordered(dv_set, 0, v0)
    ordered(dk_set, 1, k1)
    ordered(dv_set, 1, v1)
    gk_out[...] = dk_set[:TOKENS, :].astype(BF16)
    gv_out[...] = dv_set[:TOKENS, :].astype(BF16)
    send.finish()


SCATTER_COPIES = 8 * 12
SCATTER_MIB = 28


def run_scatter(chosen, k_all, v_all, h_all, dqp, dpk, dpv, qs, cs, ls, pick, places):
    vmem = pl.BlockSpec(memory_space=pltpu.VMEM)
    smem = pl.BlockSpec(memory_space=pltpu.SMEM)
    first = HALF_BLOCK * CHOSEN + POOLED
    second = HALF_BLOCK * CHOSEN
    outgoing = [pltpu.VMEM((SIDE, SIDE, n, HEAD_DIM), BF16) for n in (first, first, second, second)]
    grad = pltpu.VMEM((SIDE, SIDE, HEAD_DIM, GW_COLS), BF16)
    return pl.pallas_call(
        scatter_kernel,
        name="scatter",
        out_shape=(
            jax.ShapeDtypeStruct((TOKENS, GROUP * HEAD_DIM), BF16),
            jax.ShapeDtypeStruct((TOKENS, HEAD_DIM), BF16),
            jax.ShapeDtypeStruct((TOKENS, HEAD_DIM), BF16),
            jax.ShapeDtypeStruct((GW_COLS, GROUP * HEAD_DIM), F32),
        ),
        in_specs=[smem] + [vmem] * 11,
        out_specs=(vmem,) * 4,
        scratch_shapes=[
            pltpu.VMEM((SETS, HEAD_DIM), BF16),
            pltpu.VMEM((SETS, HEAD_DIM), BF16),
            pltpu.VMEM((BLOCKS * SETS, HEAD_DIM), F32),
            pltpu.VMEM((BLOCKS * SETS, HEAD_DIM), F32),
            pltpu.VMEM((GROUP * HEAD_DIM, TOKENS), BF16),
            *outgoing,
            pltpu.VMEM((TOKENS, HEAD_DIM), F32),
            pltpu.VMEM((TOKENS, HEAD_DIM), F32),
            grad,
            grad,
            grad,
            grad,
            *(listed_buffers(first) * 2),
            *(listed_buffers(second) * 2),
            *(reduce_buffers(HEAD_DIM, GW_COLS) * 4),
            pltpu.SemaphoreType.DMA((SCATTER_COPIES,)),
            pltpu.SemaphoreType.DMA((SCATTER_COPIES,)),
        ],
        compiler_params=pltpu.CompilerParams(
            collective_id=1, has_side_effects=True, vmem_limit_bytes=SCATTER_MIB * MIB
        ),
    )(chosen, k_all, v_all, h_all, dqp, dpk, dpv, qs, cs, ls, pick, places)


def finish_kernel(*refs):
    for src, out in zip(refs[:4], refs[4:]):
        out[...] = src[...]


def run_finish(*outs):
    vmem = pl.BlockSpec(memory_space=pltpu.VMEM)
    return pl.pallas_call(
        finish_kernel,
        name="finish",
        out_shape=tuple(jax.ShapeDtypeStruct(a.shape, a.dtype) for a in outs),
        in_specs=[vmem] * 4,
        out_specs=(vmem,) * 4,
        compiler_params=pltpu.CompilerParams(vmem_limit_bytes=8 * MIB),
    )(*outs)


def body(hidden_rows, queries, key_rows, value_rows, branch_gates, log_sums, chosen, out_grad):
    lists = chosen.reshape(BLOCKS, CHOSEN)
    k_all, v_all, h_all, *more = run_gather(
        key_rows, value_rows, hidden_rows, queries, out_grad, branch_gates, log_sums, lists
    )
    by_block = (SEQ // KEY_BLOCK, KEY_BLOCK, HEAD_DIM)
    outs = run_scatter(
        lists,
        k_all.reshape(by_block),
        v_all.reshape(by_block),
        h_all.reshape(TOKENS, MODEL),
        *more,
    )
    return run_finish(*outs)


def solution(mesh):
    placed = (
        P(("kv", "tp"), None),
        P("kv", "tp"),
        P("kv", "tp"),
        P("kv", "tp"),
        P(None, "tp", "kv"),
        P(None, "tp", "kv"),
        P("tp", "kv", None),
        P("kv", "tp"),
    )
    return jax.shard_map(
        body,
        mesh=mesh,
        in_specs=placed,
        out_specs=(P("kv", "tp"), P("kv", "tp"), P("kv", "tp"), P("kv", "tp")),
        check_vma=False,
    )
```

```python
import jax
import jax.numpy as jnp
from jax import lax
from jax.experimental import pallas as pl
from jax.experimental.pallas import tpu as pltpu
from jax.sharding import PartitionSpec as P

HEADS = 32
KV_HEADS = 8
HEAD_DIM = 128
QUERY_BLOCK = 128
KEY_BLOCK = 32
POOL_BLOCK = 32
CHOSEN = 16
GROUP = HEADS // KV_HEADS
SIDE = 4
OWNERS = SIDE * SIDE
TOKENS = 1024
BLOCKS = TOKENS // QUERY_BLOCK
POOLED = TOKENS // POOL_BLOCK
SEQ = TOKENS * OWNERS
LISTED = BLOCKS * CHOSEN
SLOTS = OWNERS * CHOSEN
MODEL = 4096
SCALE = HEAD_DIM ** (-0.5)
LOG2E = 1.4426950408889634
MIB = 1 << 20
MESH = pl.DeviceIdType.MESH
F32 = jnp.float32
BF16 = jnp.bfloat16

NT = (((1,), (1,)), ((), ()))
NN = (((1,), (0,)), ((), ()))


def dot(a, b, dims):
    return lax.dot_general(a, b, dims, preferred_element_type=F32)


class Sender:
    def __init__(self, send_sems, recv_sems):
        self.send_sems, self.recv_sems, self.at, self.sent = send_sems, recv_sems, 0, []

    def __call__(self, src, dst, dev):
        copy = pltpu.make_async_remote_copy(
            src_ref=src,
            dst_ref=dst,
            send_sem=self.send_sems.at[self.at],
            recv_sem=self.recv_sems.at[self.at],
            device_id=dev,
            device_id_type=MESH,
        )
        self.at += 1
        copy.start()
        self.sent.append(copy)
        return copy

    def finish(self):
        for copy in self.sent:
            copy.wait_send()


def place():
    kv, tp = lax.axis_index("kv"), lax.axis_index("tp")
    return kv, tp, kv // SIDE, kv % SIDE, tp // 2, tp % 2


def shifted(c, o):
    return (c + (o + SIDE)) % SIDE


def greet(devices):
    for dev in devices:
        pl.semaphore_signal(
            pltpu.get_barrier_semaphore(), inc=1, device_id=dev, device_id_type=MESH
        )


def meet(count):
    pl.semaphore_wait(pltpu.get_barrier_semaphore(), count)


def tile_operands(q_ref, g_ref, gate_ref, ls_ref, t):
    rows = pl.ds(pl.multiple_of(t * QUERY_BLOCK, QUERY_BLOCK), QUERY_BLOCK)
    gates = jnp.concatenate([gate_ref[0, :, rows], gate_ref[1, :, rows]], axis=0).T
    qs, cs, ls = [], ([], []), ([], [])
    for h in range(GROUP):
        cols = slice(h * HEAD_DIM, (h + 1) * HEAD_DIM)
        qs.append(q_ref[rows, cols])
        grad = g_ref[rows, cols].astype(F32)
        for branch in (0, 1):
            at = branch * GROUP + h
            cs[branch].append((gates[:, at : at + 1] * grad).astype(BF16))
            ls[branch].append(ls_ref[branch, h : h + 1, rows])
    return (
        jnp.concatenate(qs, axis=0),
        [jnp.concatenate(c, axis=0) for c in cs],
        [jnp.concatenate(x, axis=1) * LOG2E for x in ls],
    )


def attend_back(qs, cs, log_sum, keys, values, visible):
    scores = dot(keys, qs, NT) * (SCALE * LOG2E)
    p = jnp.where(visible, jnp.exp2(scores - log_sum), 0.0)
    pr = p.astype(BF16)
    dp = dot(values, cs, NT)
    delta = jnp.sum(p * dp, axis=0, keepdims=True)
    ds = (p * (dp - delta)).astype(BF16)
    return dot(keys.T, ds, NN), dot(ds, qs, NN), dot(pr, cs, NN)


def gather_kernel(
    k_ref, v_ref, h_ref, q_hbm, g_hbm, gate_hbm, ls_hbm, chosen_hbm,
    k_all, v_all, h_all, dq_ref, dpk_ref, dpv_ref, qs_all, cs_all, ls_rows, pick_ref, place_ref,
    chosen_ref, q_ref, g_ref, gate_ref, ls_ref, pool_all, pk_ref, pv_ref, pool_here,
    pool_send, pool_recv, send_sems, recv_sems, local_sems,
):
    kv, tp, cz, cy, cx, core = place()
    half = TOKENS // 2

    def device(oz, oy):
        return (shifted(cz, oz) * SIDE + shifted(cy, oy), tp)

    def along(axis, o):
        return device(o, 0) if axis == 0 else device(0, o)

    def owner(axis, o1, o2):
        a, b = (o1, o2) if axis == 0 else (o2, o1)
        return shifted(cz, a) * SIDE + shifted(cy, b)

    def xdev(o, c):
        return (kv, shifted(cx, o) * 2 + c)

    others = [(oz, oy) for oz in range(SIDE) for oy in range(SIDE) if (oz, oy) != (0, 0)]
    peers = [device(oz, oy) for oz, oy in others] + [
        xdev(1, core), xdev(-1, core), xdev(0, 1 - core)
    ]
    greet(peers)
    local = [
        pltpu.make_async_copy(src, dst, local_sems.at[i])
        for i, (src, dst) in enumerate(
            (
                (k_ref, k_all.at[kv]),
                (v_ref, v_all.at[kv]),
                (h_ref, h_all.at[tp]),
                (chosen_hbm, chosen_ref),
                (gate_hbm, gate_ref),
                (ls_hbm, ls_ref),
                (q_hbm, q_ref),
                (g_hbm, g_ref),
            )
        )
    ]
    for copy in local:
        copy.start()

    blk = lax.broadcasted_iota(jnp.int32, (POOLED, TOKENS), 0)
    row = lax.broadcasted_iota(jnp.int32, (POOLED, TOKENS), 1)
    mean = jnp.where(row // POOL_BLOCK == blk, 1.0 / POOL_BLOCK, 0.0).astype(BF16)
    local[0].wait()
    pool_here[:POOLED] = dot(mean, k_all[kv], NN).astype(BF16)
    local[1].wait()
    pool_here[POOLED : POOLED * 2] = dot(mean, v_all[kv], NN).astype(BF16)

    local[3].wait()
    lane = lax.broadcasted_iota(jnp.int32, (1, LISTED), 1)
    listed = jnp.zeros((1, LISTED), jnp.int32)
    for b in range(BLOCKS):
        for c in range(CHOSEN):
            listed = jnp.where(lane == b * CHOSEN + c, chosen_ref[b, c], listed)
    row = lax.broadcasted_iota(jnp.int32, (16, LISTED), 0)
    both = jnp.where(row == 0, listed // POOLED, jnp.where(row == 1, listed % POOLED, 0))
    pool_here[POOLED * 2 :] = both.astype(F32).astype(BF16)
    meet(len(peers))

    pool_sender = Sender(pool_send, pool_recv)
    for oz, oy in others:
        pool_sender(pool_here, pool_all.at[kv], device(oz, oy))
    pool_all[kv] = pool_here[...]

    send = Sender(send_sems, recv_sems)
    first, wide = {}, {}
    arrays = ((0, k_all), (1, v_all))
    for axis, full in arrays:
        here = full.at[kv]
        first[axis] = [send(here, here, along(axis, s)) for s in (1, -1)]
    local[2].wait()
    here = h_all.at[tp]
    x_first = [send(here, here, xdev(s, core)) for s in (1, -1)]
    x_over = [send(here, here, xdev(0, 1 - core))]
    for axis, full in arrays:
        here = full.at[kv]
        wide[axis] = [(0, [send(here, here, along(1 - axis, s)) for s in (1, -1)])]

    for copy in local[4:]:
        copy.wait()
    for copy in pool_sender.sent:
        copy.wait_recv()
    pk_ref[...] = pool_all[:, :POOLED].reshape(OWNERS * POOLED, HEAD_DIM)
    pv_ref[...] = pool_all[:, POOLED : 2 * POOLED].reshape(OWNERS * POOLED, HEAD_DIM)
    dpk_ref[...] = jnp.zeros_like(dpk_ref)
    dpv_ref[...] = jnp.zeros_like(dpv_ref)

    def listing(i):
        both = pool_all[i, 2 * POOLED :].astype(F32)
        owners, numbers, column = both[0:1, :], both[1:2, :], both.T[:, 0:1]
        one = lax.broadcasted_iota(jnp.int32, (LISTED, LISTED), 0)
        two = lax.broadcasted_iota(jnp.int32, (LISTED, LISTED), 1)
        same = jnp.where(column == owners, 1.0, 0.0)
        rank = jnp.sum(jnp.where(one < two, same, 0.0), axis=0, keepdims=True)
        return owners, numbers, rank

    def grid(rows, f):
        return f(lax.broadcasted_iota(jnp.int32, (rows, LISTED), 0)).astype(F32)

    def ones(seen):
        return jnp.where(seen, 1.0, 0.0)

    owners, numbers, rank = listing(kv)
    kv_f = kv.astype(F32)
    at, nth = grid(SLOTS, lambda i: i // CHOSEN), grid(SLOTS, lambda i: i % CHOSEN)
    own = jnp.where(owners == kv_f, -1.0, owners)
    pick_ref[:SLOTS] = (ones(own == at) * ones(rank == nth)).astype(BF16)
    at = grid(POOLED, lambda i: i)
    pick_ref[SLOTS:] = (ones(owners == kv_f) * ones(numbers == at)).astype(BF16)

    for axis in (0, 1):
        def owner_id(i, axis=axis):
            return cz * SIDE + i if axis == 0 else i * SIDE + cy

        for pair in (0, 1):
            total = None
            for n in (0, 1):
                who = owner(axis, (0, -1, 1, 2)[2 * pair + n], 0)
                owners, numbers, rank = listing(who)
                at = grid(LISTED, lambda i: owner_id(i // POOLED))
                nth = grid(LISTED, lambda i: i % POOLED)
                blocks = ones(owners == at) * ones(numbers == nth)
                at = grid(LISTED, lambda i: owner_id((i % 64) // CHOSEN))
                nth = grid(LISTED, lambda i, n=n: jnp.where(i // 64 == n, i % CHOSEN, -1))
                own = jnp.where(owners == who.astype(F32), -1.0, owners)
                slots = ones(own == at) * ones(rank == nth)
                part = dot(blocks.astype(BF16), slots.astype(BF16), NT)
                total = part if total is None else total + part
            place_ref[axis, :, pair * LISTED : (pair + 1) * LISTED] = total.astype(BF16)

    n_pool = OWNERS * POOLED
    wide_q = GROUP * QUERY_BLOCK
    pool_end = lax.broadcasted_iota(jnp.int32, (n_pool, wide_q), 0) * POOL_BLOCK + POOL_BLOCK - 1
    lane = lax.broadcasted_iota(jnp.int32, (n_pool, wide_q), 1) % QUERY_BLOCK
    ahead = pool_end - lane

    def tile(t, carry):
        qs, cs, ls = tile_operands(q_ref, g_ref, gate_ref, ls_ref, t)
        qs_all[t] = qs
        cs_all[t] = cs[1]
        ls_rows[t] = ls[1]
        visible = ahead <= kv * TOKENS + t * QUERY_BLOCK
        dq, dk, dv = attend_back(qs, cs[0], ls[0], pk_ref[...], pv_ref[...], visible)
        dq_ref[t] = dq
        dpk_ref[...] += dk
        dpv_ref[...] += dv
        return carry

    lax.fori_loop(0, 4, tile, 0)

    second = {}
    for axis, full in arrays:
        plus, minus = first[axis]
        plus.wait_recv()
        part = full.at[owner(axis, -1, 0), pl.ds(0, half)]
        fwd = send(part, part, along(axis, 1))
        whole = full.at[owner(axis, -1, 0)]
        wide[axis].append((-1, [send(whole, whole, along(1 - axis, s)) for s in (1, -1)]))
        minus.wait_recv()
        part = full.at[owner(axis, 1, 0), pl.ds(half, half)]
        bwd = send(part, part, along(axis, -1))
        whole = full.at[owner(axis, 1, 0)]
        wide[axis].append((1, [send(whole, whole, along(1 - axis, s)) for s in (1, -1)]))
        second[axis] = (fwd, bwd)

    lax.fori_loop(4, BLOCKS, tile, 0)
    dpk_ref[...] = dpk_ref[...] * (SCALE / POOL_BLOCK)
    dpv_ref[...] = dpv_ref[...] * (1.0 / POOL_BLOCK)

    last = []

    def across(axis, full, o, pair):
        plus, minus = pair
        plus.wait_recv()
        part = full.at[owner(axis, o, -1), pl.ds(0, half)]
        last.append(send(part, part, along(1 - axis, 1)))
        minus.wait_recv()
        part = full.at[owner(axis, o, 1), pl.ds(half, half)]
        last.append(send(part, part, along(1 - axis, -1)))

    for axis, full in arrays:
        across(axis, full, *wide[axis][0])
    for axis, full in arrays:
        for copy in second[axis]:
            copy.wait_recv()
        whole = full.at[owner(axis, 2, 0)]
        wide[axis].append((2, [send(whole, whole, along(1 - axis, s)) for s in (1, -1)]))
    rows = TOKENS // 16
    plus, minus = x_first
    plus.wait_recv()
    whole = h_all.at[shifted(cx, -1) * 2 + core]
    part = whole.at[pl.ds(0, rows)]
    x_second = [send(part, part, xdev(1, core))]
    x_over.append(send(whole, whole, xdev(0, 1 - core)))
    minus.wait_recv()
    whole = h_all.at[shifted(cx, 1) * 2 + core]
    part = whole.at[pl.ds(rows, rows)]
    x_second.append(send(part, part, xdev(-1, core)))
    x_over.append(send(whole, whole, xdev(0, 1 - core)))
    for i in (1, 2):
        for axis, full in arrays:
            across(axis, full, *wide[axis][i])
    for copy in x_second:
        copy.wait_recv()
    whole = h_all.at[shifted(cx, 2) * 2 + core]
    x_over.append(send(whole, whole, xdev(0, 1 - core)))
    for axis, full in arrays:
        across(axis, full, *wide[axis][3])
    for copy in last:
        copy.wait_recv()
    for copy in x_over:
        copy.wait_recv()
    pool_sender.finish()
    send.finish()


GATHER_COPIES = 2 * (2 + 2 + 8 + 8) + 2 + 2 + 4


def run_gather(k, v, h, q, g, gates, sums, chosen):
    hbm = pl.BlockSpec(memory_space=pltpu.HBM)
    vmem = pl.BlockSpec(memory_space=pltpu.VMEM)
    n_pool = OWNERS * POOLED
    wide_q = GROUP * QUERY_BLOCK
    return pl.pallas_call(
        gather_kernel,
        name="gather",
        out_shape=(
            jax.ShapeDtypeStruct((OWNERS, TOKENS, HEAD_DIM), BF16),
            jax.ShapeDtypeStruct((OWNERS, TOKENS, HEAD_DIM), BF16),
            jax.ShapeDtypeStruct((8, TOKENS // 8, MODEL), BF16),
            jax.ShapeDtypeStruct((BLOCKS, HEAD_DIM, wide_q), F32),
            jax.ShapeDtypeStruct((n_pool, HEAD_DIM), F32),
            jax.ShapeDtypeStruct((n_pool, HEAD_DIM), F32),
            jax.ShapeDtypeStruct((BLOCKS, wide_q, HEAD_DIM), BF16),
            jax.ShapeDtypeStruct((BLOCKS, wide_q, HEAD_DIM), BF16),
            jax.ShapeDtypeStruct((BLOCKS, 1, wide_q), F32),
            jax.ShapeDtypeStruct((SLOTS + POOLED, LISTED), BF16),
            jax.ShapeDtypeStruct((2, LISTED, SLOTS), BF16),
        ),
        in_specs=[hbm] * 8,
        out_specs=(vmem,) * 11,
        scratch_shapes=[
            pltpu.SMEM((BLOCKS, CHOSEN), jnp.int32),
            pltpu.VMEM(q.shape, BF16),
            pltpu.VMEM(g.shape, BF16),
            pltpu.VMEM(gates.shape, F32),
            pltpu.VMEM(sums.shape, F32),
            pltpu.VMEM((OWNERS, 2 * POOLED + 16, HEAD_DIM), BF16),
            pltpu.VMEM((n_pool, HEAD_DIM), BF16),
            pltpu.VMEM((n_pool, HEAD_DIM), BF16),
            pltpu.VMEM((2 * POOLED + 16, HEAD_DIM), BF16),
            pltpu.SemaphoreType.DMA((OWNERS - 1,)),
            pltpu.SemaphoreType.DMA((OWNERS - 1,)),
            pltpu.SemaphoreType.DMA((GATHER_COPIES,)),
            pltpu.SemaphoreType.DMA((GATHER_COPIES,)),
            pltpu.SemaphoreType.DMA((8,)),
        ],
        compiler_params=pltpu.CompilerParams(
            collective_id=0, has_side_effects=True, vmem_limit_bytes=12 * MIB
        ),
        cost_estimate=pl.CostEstimate(
            flops=40_000_000_000, bytes_accessed=8 * MIB, transcendentals=0
        ),
    )(*(pltpu.with_memory_space_constraint(a, pltpu.HBM) for a in (k, v, h, q, g, gates, sums, chosen)))


class Reduce:
    def __init__(self, send, axis, src, bufs, coords, along):
        self.relay, self.direct, self.comb, self.relay2, self.direct2, self.comb2 = bufs
        self.send, self.axis, self.src = send, axis, src
        self.c1, self.c2 = (coords[0], coords[1]) if axis == 0 else (coords[1], coords[0])
        self.to1 = lambda o: along(axis, o)
        self.to2 = lambda o: along(1 - axis, o)
        self.half = src.shape[2] // 2
        self.rows = (pl.ds(0, self.half), pl.ds(self.half, self.half))

    def bundle(self, o, n):
        c = shifted(self.c1, o)
        rows = self.rows[n]
        return self.src.at[c, :, rows] if self.axis == 0 else self.src.at[:, c, rows]

    def piece(self, o, i, n):
        c = shifted(self.c1, o)
        if self.axis == 0:
            return self.src[c, i, self.rows[n], :].astype(F32)
        return self.src[i, c, self.rows[n], :].astype(F32)

    def part(self, o, n):
        return self.comb.at[n, shifted(self.c2, o)]

    def begin(self):
        s = self.send
        self.r = [
            s(self.bundle(2, 0), self.relay.at[0], self.to1(1)),
            s(self.bundle(2, 1), self.relay.at[1], self.to1(-1)),
        ]
        self.d = [
            s(self.bundle(1, 1), self.direct.at[0], self.to1(1)),
            s(self.bundle(-1, 0), self.direct.at[1], self.to1(-1)),
        ]

    def combine(self):
        self.c = []
        for n, o in enumerate((1, -1)):
            self.r[n].wait_recv()

            def add(i, carry, n=n, o=o):
                self.relay[n, i] = (self.piece(o, i, n) + self.relay[n, i].astype(F32)).astype(BF16)
                return carry

            lax.fori_loop(0, SIDE, add, 0)
            self.c.append(self.send(self.relay.at[n], self.comb.at[n], self.to1(o)))

    def turn(self):
        for copy in self.d + self.c:
            copy.wait_recv()

        def add(i, carry):
            for n in (0, 1):
                self.comb[n, i] = (
                    self.piece(0, i, n)
                    + self.comb[n, i].astype(F32)
                    + self.direct[1 - n, i].astype(F32)
                ).astype(BF16)
            return carry

        lax.fori_loop(0, SIDE, add, 0)
        self.start_second()

    def start_second(self):
        s = self.send
        self.r = [
            s(self.part(2, 0), self.relay2.at[0], self.to2(1)),
            s(self.part(2, 1), self.relay2.at[1], self.to2(-1)),
        ]
        self.d = [
            s(self.part(1, 1), self.direct2.at[0], self.to2(1)),
            s(self.part(-1, 0), self.direct2.at[1], self.to2(-1)),
        ]

    def combine2(self):
        self.c = []
        for n, o in enumerate((1, -1)):
            self.r[n].wait_recv()
            self.relay2[n] = (
                self.comb[n, shifted(self.c2, o)].astype(F32) + self.relay2[n].astype(F32)
            ).astype(BF16)
            self.c.append(self.send(self.relay2.at[n], self.comb2.at[n], self.to2(o)))

    def end(self):
        for copy in self.d + self.c:
            copy.wait_recv()
        return [
            self.comb[n, self.c2].astype(F32)
            + self.comb2[n].astype(F32)
            + self.direct2[1 - n].astype(F32)
            for n in (0, 1)
        ]


class ListedReduce(Reduce):
    def __init__(self, send, axis, src, bufs, coords, along, place_ref, own):
        self.passed, self.far, self.near, *after = bufs
        super().__init__(send, axis, src, (None, None, *after), coords, along)
        self.place_ref, self.own = place_ref, own
        self.steps = HALF_BLOCK * CHOSEN
        self.pooled = self

    def begin(self):
        s = self.send
        every = pl.ds(0, self.src.shape[2])
        self.rows = self.rows + (every,)
        self.r = [
            s(self.bundle(2, 0), self.passed.at[0], self.to1(1)),
            s(self.bundle(2, 1), self.passed.at[1], self.to1(-1)),
        ]
        self.d = [
            s(self.bundle(1, 2), self.near.at[0], self.to1(1)),
            s(self.bundle(-1, 2), self.near.at[1], self.to1(-1)),
        ]

    def combine(self):
        self.c = []
        for n, o in enumerate((1, -1)):
            self.r[n].wait_recv()
            self.c.append(self.send(self.passed.at[n], self.far.at[:, self.rows[n]], self.to1(o)))

    def sources(self, rows):
        mine = self.src[self.c1, :, rows, :] if self.axis == 0 else self.src[:, self.c1, rows, :]
        return [mine, self.near[0, :, rows, :], self.near[1, :, rows, :], self.far[:, rows, :]]

    def turn(self):
        for copy in self.d + self.c:
            copy.wait_recv()
        pooled = sum(x.astype(F32) for x in self.pooled.sources(pl.ds(self.steps, POOLED)))
        pooled = pooled.reshape(SIDE * POOLED, HEAD_DIM)
        pooled = jnp.concatenate([pooled, pooled], axis=1)
        for n in (0, 1):

            def put(i, carry, n=n):
                pieces = []
                for j in (0, 1):
                    first = pl.multiple_of((n * HALF_BLOCK // 2 + 2 * i + j) * CHOSEN, CHOSEN)
                    got = [x.reshape(SIDE * CHOSEN, HEAD_DIM) for x in self.sources(pl.ds(first, CHOSEN))]
                    pieces.append(jnp.concatenate(got, axis=0))
                total = dot(self.place_ref[self.axis], jnp.concatenate(pieces, axis=1), NN)
                total = total + pooled
                for j in (0, 1):
                    rows = pl.ds(pl.multiple_of((2 * i + j) * POOLED, POOLED), POOLED)
                    part = total[:, j * HEAD_DIM : (j + 1) * HEAD_DIM].astype(BF16)
                    self.comb[n, :, rows, :] = part.reshape(SIDE, POOLED, HEAD_DIM)
                return carry

            lax.fori_loop(0, HALF_BLOCK // 4, put, 0, unroll=2)
        self.start_second()

    def end(self):
        at = self.own[1]
        size = HALF_BLOCK // 2 * POOLED
        return [
            part + self.own[0][at + n * size : at + (n + 1) * size, :]
            for n, part in enumerate(super().end())
        ]


def listed_buffers(rows):
    half, size = rows // 2, HALF_BLOCK // 2 * POOLED
    slim = pltpu.VMEM((2, size, HEAD_DIM), BF16)
    return [
        pltpu.VMEM((2, SIDE, half, HEAD_DIM), BF16),
        pltpu.VMEM((SIDE, rows, HEAD_DIM), BF16),
        pltpu.VMEM((2, SIDE, rows, HEAD_DIM), BF16),
        pltpu.VMEM((2, SIDE, size, HEAD_DIM), BF16),
        slim, slim, slim,
    ]


def reduce_buffers(rows, lanes):
    half = rows // 2
    wide = pltpu.VMEM((2, SIDE, half, lanes), BF16)
    slim = pltpu.VMEM((2, half, lanes), BF16)
    return [wide] * 3 + [slim] * 3


REDUCE_BUFS = 6
LISTED_BUFS = 7
GW_COLS = MODEL // OWNERS
PAIR = GROUP // 2 * HEAD_DIM
PAIR_Q = GROUP // 2 * QUERY_BLOCK
UNROLL = 4
HALF_BLOCK = KEY_BLOCK // 2
SETS = CHOSEN * KEY_BLOCK


def scatter_kernel(
    chosen_ref, k_ref, v_ref, h_ref, dqp_ref, dpk_ref, dpv_ref, qs_all, cs_all, ls_rows, pick_ref, place_ref,
    gq_ref, gk_out, gv_out, gw_out,
    kb, vb, dk_set, dv_set, gqt, dk0, dv0, dk1, dv1, own_k, own_v, gw0, gw1, gw2, gw3, *rest
):
    cut = 4 * LISTED_BUFS
    bufs = [rest[i * LISTED_BUFS : (i + 1) * LISTED_BUFS] for i in range(4)]
    gw_bufs = [rest[cut + i * REDUCE_BUFS : cut + (i + 1) * REDUCE_BUFS] for i in range(4)]
    send_sems, recv_sems = rest[cut + 4 * REDUCE_BUFS :]
    kv, tp, cz, cy, cx, core = place()

    def along(axis, o):
        if axis == 0:
            return (shifted(cz, o) * SIDE + cy, tp)
        return (cz * SIDE + shifted(cy, o), tp)

    peers = [along(axis, o) for axis in (0, 1) for o in (1, -1)]
    greet(peers)
    send = Sender(send_sems, recv_sems)
    gws = (gw0, gw1, gw2, gw3)
    kv_parts = (dk0, dv0, dk1, dv1)
    half_rows = HALF_BLOCK * POOLED
    owns = ((own_k, 0), (own_v, 0), (own_k, half_rows), (own_v, half_rows))
    k0, v0, k1, v1 = [
        ListedReduce(send, axis, src, buf, (cz, cy), along, place_ref, own)
        for axis, src, buf, own in zip((0, 1) * 2, kv_parts, bufs, owns)
    ]
    k1.pooled, v1.pooled = k0, v0
    w0, w1, w2, w3 = [
        Reduce(send, axis, src, buf, (cz, cy), along)
        for axis, src, buf in zip((0, 1) * 2, gws, gw_bufs)
    ]

    ahead = (
        lax.broadcasted_iota(jnp.int32, (KEY_BLOCK, PAIR_Q), 0)
        - lax.broadcasted_iota(jnp.int32, (KEY_BLOCK, PAIR_Q), 1) % QUERY_BLOCK
    )

    def attend(pair):
        across = slice(pair * PAIR_Q, (pair + 1) * PAIR_Q)

        def block(b, carry):
            start_row = kv * TOKENS + b * QUERY_BLOCK
            seen = []
            for c in range(CHOSEN):
                at = chosen_ref[b, c]
                kb[c * KEY_BLOCK : (c + 1) * KEY_BLOCK, :] = k_ref[at]
                vb[c * KEY_BLOCK : (c + 1) * KEY_BLOCK, :] = v_ref[at]
                seen.append(ahead <= start_row - at * KEY_BLOCK)
            dq, dk, dv = attend_back(
                qs_all[b, across, :],
                cs_all[b, across, :],
                ls_rows[b, :, across],
                kb[...],
                vb[...],
                jnp.concatenate(seen, axis=0),
            )
            total = (dqp_ref[b, :, across] + dq) * SCALE
            rows = pl.ds(pl.multiple_of(b * QUERY_BLOCK, QUERY_BLOCK), QUERY_BLOCK)
            for h in range(GROUP // 2):
                part = total[:, h * QUERY_BLOCK : (h + 1) * QUERY_BLOCK]
                at = pair * PAIR + h * HEAD_DIM
                gqt[at : at + HEAD_DIM, rows] = part.astype(BF16)
                gq_ref[rows, at : at + HEAD_DIM] = part.T.astype(BF16)
            here = pl.ds(pl.multiple_of(b * SETS, SETS), SETS)
            if pair == 0:
                dk_set[here, :] = dk * SCALE
                dv_set[here, :] = dv
            else:
                dk_set[here, :] += dk * SCALE
                dv_set[here, :] += dv
            return carry

        return block

    def product(pair):
        def one(j, carry):
            wide = SIDE * GW_COLS
            cols = pl.ds(pl.multiple_of(j * wide, wide), wide)
            part = dot(gqt[pair * PAIR : (pair + 1) * PAIR, :], h_ref[:, cols], NN).astype(BF16)
            for i in range(SIDE):
                piece = part[:, i * GW_COLS : (i + 1) * GW_COLS]
                gws[2 * pair][j, i] = piece[:HEAD_DIM]
                gws[2 * pair + 1][j, i] = piece[HEAD_DIM:]
            return carry

        lax.fori_loop(0, SIDE, one, 0)

    lax.fori_loop(0, BLOCKS, attend(0), 0, unroll=2)
    product(0)
    meet(len(peers))
    w0.begin()
    w1.begin()
    lax.fori_loop(0, BLOCKS // 2, attend(1), 0, unroll=2)
    w0.combine()
    w1.combine()
    lax.fori_loop(BLOCKS // 2, BLOCKS, attend(1), 0, unroll=2)

    product(1)
    w2.begin()
    w3.begin()
    w0.turn()
    w1.turn()

    slots = (SIDE, SIDE, CHOSEN, HEAD_DIM)

    def spread(part):
        dk_out, dv_out = kv_parts[2 * part : 2 * part + 2]

        def one(i, carry):
            every = pl.ds(part * HALF_BLOCK + i, LISTED, stride=KEY_BLOCK)
            got = jnp.concatenate([dk_set[every, :], dv_set[every, :]], axis=1).astype(BF16)
            got = dot(pick_ref[...], got, NN)
            rows = pl.ds(pl.multiple_of(i * CHOSEN, CHOSEN), CHOSEN)
            dk_out[:, :, rows, :] = got[:SLOTS, :HEAD_DIM].astype(BF16).reshape(slots)
            dv_out[:, :, rows, :] = got[:SLOTS, HEAD_DIM:].astype(BF16).reshape(slots)
            rows = pl.ds(pl.multiple_of((part * HALF_BLOCK + i) * POOLED, POOLED), POOLED)
            own_k[rows, :] = got[SLOTS:, :HEAD_DIM]
            own_v[rows, :] = got[SLOTS:, HEAD_DIM:]
            return carry

        lax.fori_loop(0, HALF_BLOCK, one, 0, unroll=UNROLL)

    tail = slice(HALF_BLOCK * CHOSEN, HALF_BLOCK * CHOSEN + POOLED)
    pooled = (SIDE, SIDE, POOLED, HEAD_DIM)
    dk0[:, :, tail, :] = dpk_ref[...].astype(BF16).reshape(pooled)
    dv0[:, :, tail, :] = dpv_ref[...].astype(BF16).reshape(pooled)
    spread(0)
    k0.begin()
    v0.begin()
    w2.combine()
    w3.combine()
    w0.combine2()
    w1.combine2()
    spread(1)
    k1.begin()
    v1.begin()
    w2.turn()
    w3.turn()

    def weight(n, w):
        for i, part in enumerate(w.end()):
            at = n * HEAD_DIM + i * HEAD_DIM // 2
            gw_out[:, at : at + HEAD_DIM // 2] = part.T

    def ordered(into, part, r):
        for n, rows in enumerate(r.end()):
            for i in range(HALF_BLOCK // 2):
                at = part * HALF_BLOCK + n * (HALF_BLOCK // 2) + i
                into[pl.ds(at, POOLED, stride=KEY_BLOCK), :] = rows[i * POOLED : (i + 1) * POOLED]

    k0.combine()
    v0.combine()
    w2.combine2()
    w3.combine2()
    k1.combine()
    v1.combine()
    k0.turn()
    v0.turn()
    k1.turn()
    v1.turn()
    weight(0, w0)
    weight(1, w1)
    k0.combine2()
    v0.combine2()
    k1.combine2()
    v1.combine2()
    weight(2, w2)
    weight(3, w3)
    ordered(dk_set, 0, k0)
    ordered(dv_set, 0, v0)
    ordered(dk_set, 1, k1)
    ordered(dv_set, 1, v1)
    gk_out[...] = dk_set[:TOKENS, :].astype(BF16)
    gv_out[...] = dv_set[:TOKENS, :].astype(BF16)
    send.finish()


SCATTER_COPIES = 8 * 12
SCATTER_MIB = 28


def run_scatter(chosen, k_all, v_all, h_all, dqp, dpk, dpv, qs, cs, ls, pick, places):
    vmem = pl.BlockSpec(memory_space=pltpu.VMEM)
    smem = pl.BlockSpec(memory_space=pltpu.SMEM)
    first = HALF_BLOCK * CHOSEN + POOLED
    second = HALF_BLOCK * CHOSEN
    outgoing = [pltpu.VMEM((SIDE, SIDE, n, HEAD_DIM), BF16) for n in (first, first, second, second)]
    grad = pltpu.VMEM((SIDE, SIDE, HEAD_DIM, GW_COLS), BF16)
    return pl.pallas_call(
        scatter_kernel,
        name="scatter",
        out_shape=(
            jax.ShapeDtypeStruct((TOKENS, GROUP * HEAD_DIM), BF16),
            jax.ShapeDtypeStruct((TOKENS, HEAD_DIM), BF16),
            jax.ShapeDtypeStruct((TOKENS, HEAD_DIM), BF16),
            jax.ShapeDtypeStruct((GW_COLS, GROUP * HEAD_DIM), F32),
        ),
        in_specs=[smem] + [vmem] * 11,
        out_specs=(vmem,) * 4,
        scratch_shapes=[
            pltpu.VMEM((SETS, HEAD_DIM), BF16),
            pltpu.VMEM((SETS, HEAD_DIM), BF16),
            pltpu.VMEM((BLOCKS * SETS, HEAD_DIM), F32),
            pltpu.VMEM((BLOCKS * SETS, HEAD_DIM), F32),
            pltpu.VMEM((GROUP * HEAD_DIM, TOKENS), BF16),
            *outgoing,
            pltpu.VMEM((TOKENS, HEAD_DIM), F32),
            pltpu.VMEM((TOKENS, HEAD_DIM), F32),
            grad,
            grad,
            grad,
            grad,
            *(listed_buffers(first) * 2),
            *(listed_buffers(second) * 2),
            *(reduce_buffers(HEAD_DIM, GW_COLS) * 4),
            pltpu.SemaphoreType.DMA((SCATTER_COPIES,)),
            pltpu.SemaphoreType.DMA((SCATTER_COPIES,)),
        ],
        compiler_params=pltpu.CompilerParams(
            collective_id=1, has_side_effects=True, vmem_limit_bytes=SCATTER_MIB * MIB
        ),
    )(chosen, k_all, v_all, h_all, dqp, dpk, dpv, qs, cs, ls, pick, places)


def finish_kernel(*refs):
    copies = [pltpu.make_async_copy(refs[i], refs[4 + i], refs[8].at[i]) for i in range(4)]
    for copy in copies:
        copy.start()
    for copy in copies:
        copy.wait()


def run_finish(*outs):
    return pl.pallas_call(
        finish_kernel,
        name="finish",
        out_shape=tuple(jax.ShapeDtypeStruct(a.shape, a.dtype) for a in outs),
        in_specs=[pl.BlockSpec(memory_space=pltpu.VMEM)] * 4,
        out_specs=(pl.BlockSpec(memory_space=pltpu.HBM),) * 4,
        scratch_shapes=[pltpu.SemaphoreType.DMA((4,))],
        compiler_params=pltpu.CompilerParams(vmem_limit_bytes=8 * MIB),
    )(*outs)


def body(hidden_rows, queries, key_rows, value_rows, branch_gates, log_sums, chosen, out_grad):
    lists = chosen.reshape(BLOCKS, CHOSEN)
    k_all, v_all, h_all, *more = run_gather(
        key_rows, value_rows, hidden_rows, queries, out_grad, branch_gates, log_sums, lists
    )
    by_block = (SEQ // KEY_BLOCK, KEY_BLOCK, HEAD_DIM)
    outs = run_scatter(
        lists,
        k_all.reshape(by_block),
        v_all.reshape(by_block),
        h_all.reshape(TOKENS, MODEL),
        *more,
    )
    return run_finish(*outs)


def solution(mesh):
    placed = (
        P(("kv", "tp"), None),
        P("kv", "tp"),
        P("kv", "tp"),
        P("kv", "tp"),
        P(None, "tp", "kv"),
        P(None, "tp", "kv"),
        P("tp", "kv", None),
        P("kv", "tp"),
    )
    return jax.shard_map(
        body,
        mesh=mesh,
        in_specs=placed,
        out_specs=(P("kv", "tp"), P("kv", "tp"), P("kv", "tp"), P("kv", "tp")),
        check_vma=False,
    )
```

```python
import jax
import jax.numpy as jnp
from jax import lax
from jax.experimental import pallas as pl
from jax.experimental.pallas import tpu as pltpu
from jax.sharding import PartitionSpec as P

HEADS = 32
KV_HEADS = 8
HEAD_DIM = 128
QUERY_BLOCK = 128
KEY_BLOCK = 32
POOL_BLOCK = 32
CHOSEN = 16
GROUP = HEADS // KV_HEADS
SIDE = 4
OWNERS = SIDE * SIDE
TOKENS = 1024
BLOCKS = TOKENS // QUERY_BLOCK
POOLED = TOKENS // POOL_BLOCK
SEQ = TOKENS * OWNERS
LISTED = BLOCKS * CHOSEN
SLOTS = OWNERS * CHOSEN
MODEL = 4096
SCALE = HEAD_DIM ** (-0.5)
LOG2E = 1.4426950408889634
MIB = 1 << 20
MESH = pl.DeviceIdType.MESH
F32 = jnp.float32
BF16 = jnp.bfloat16

NT = (((1,), (1,)), ((), ()))
NN = (((1,), (0,)), ((), ()))


def dot(a, b, dims):
    return lax.dot_general(a, b, dims, preferred_element_type=F32)


class Sender:
    def __init__(self, send_sems, recv_sems):
        self.send_sems, self.recv_sems, self.at, self.sent = send_sems, recv_sems, 0, []

    def __call__(self, src, dst, dev):
        copy = pltpu.make_async_remote_copy(
            src_ref=src,
            dst_ref=dst,
            send_sem=self.send_sems.at[self.at],
            recv_sem=self.recv_sems.at[self.at],
            device_id=dev,
            device_id_type=MESH,
        )
        self.at += 1
        copy.start()
        self.sent.append(copy)
        return copy

    def finish(self):
        for copy in self.sent:
            copy.wait_send()


def place():
    kv, tp = lax.axis_index("kv"), lax.axis_index("tp")
    return kv, tp, kv // SIDE, kv % SIDE, tp // 2, tp % 2


def shifted(c, o):
    return (c + (o + SIDE)) % SIDE


def greet(devices):
    for dev in devices:
        pl.semaphore_signal(
            pltpu.get_barrier_semaphore(), inc=1, device_id=dev, device_id_type=MESH
        )


def meet(count):
    pl.semaphore_wait(pltpu.get_barrier_semaphore(), count)


def tile_operands(q_ref, g_ref, gate_ref, ls_ref, t):
    rows = pl.ds(pl.multiple_of(t * QUERY_BLOCK, QUERY_BLOCK), QUERY_BLOCK)
    gates = jnp.concatenate([gate_ref[0, :, rows], gate_ref[1, :, rows]], axis=0).T
    qs, cs, ls = [], ([], []), ([], [])
    for h in range(GROUP):
        cols = slice(h * HEAD_DIM, (h + 1) * HEAD_DIM)
        qs.append(q_ref[rows, cols])
        grad = g_ref[rows, cols].astype(F32)
        for branch in (0, 1):
            at = branch * GROUP + h
            cs[branch].append((gates[:, at : at + 1] * grad).astype(BF16))
            ls[branch].append(ls_ref[branch, h : h + 1, rows])
    return (
        jnp.concatenate(qs, axis=0),
        [jnp.concatenate(c, axis=0) for c in cs],
        [jnp.concatenate(x, axis=1) * LOG2E for x in ls],
    )


def attend_back(qs, cs, log_sum, keys, values, visible):
    scores = dot(keys, qs, NT) * (SCALE * LOG2E)
    p = jnp.where(visible, jnp.exp2(scores - log_sum), 0.0)
    pr = p.astype(BF16)
    dp = dot(values, cs, NT)
    delta = jnp.sum(p * dp, axis=0, keepdims=True)
    ds = (p * (dp - delta)).astype(BF16)
    return dot(keys.T, ds, NN), dot(ds, qs, NN), dot(pr, cs, NN)


def gather_kernel(
    k_ref, v_ref, h_ref, q_hbm, g_hbm, gate_hbm, ls_hbm, chosen_hbm,
    k_all, v_all, h_all, dq_ref, dpk_ref, dpv_ref, qs_all, cs_all, ls_rows, pick_ref, place_ref,
    chosen_ref, q_ref, g_ref, gate_ref, ls_ref, pool_k, pool_v, pk_ref, pv_ref,
    send_sems, recv_sems, local_sems,
):
    kv, tp, cz, cy, cx, core = place()
    half = TOKENS // 2

    def device(oz, oy):
        return (shifted(cz, oz) * SIDE + shifted(cy, oy), tp)

    def along(axis, o):
        return device(o, 0) if axis == 0 else device(0, o)

    def owner(axis, o1, o2):
        a, b = (o1, o2) if axis == 0 else (o2, o1)
        return shifted(cz, a) * SIDE + shifted(cy, b)

    def xdev(o, c):
        return (kv, shifted(cx, o) * 2 + c)

    peers = [along(axis, s) for axis in (0, 1) for s in (1, -1)] + [
        xdev(1, core), xdev(-1, core), xdev(0, 1 - core)
    ]
    greet(peers)
    local = [
        pltpu.make_async_copy(src, dst, local_sems.at[i])
        for i, (src, dst) in enumerate(
            (
                (k_ref, k_all.at[kv]),
                (v_ref, v_all.at[kv]),
                (h_ref, h_all.at[tp]),
                (chosen_hbm, chosen_ref),
                (gate_hbm, gate_ref),
                (ls_hbm, ls_ref),
                (q_hbm, q_ref),
                (g_hbm, g_ref),
            )
        )
    ]
    for copy in local:
        copy.start()

    blk = lax.broadcasted_iota(jnp.int32, (POOLED, TOKENS), 0)
    row = lax.broadcasted_iota(jnp.int32, (POOLED, TOKENS), 1)
    mean = jnp.where(row // POOL_BLOCK == blk, 1.0 / POOL_BLOCK, 0.0).astype(BF16)
    local[0].wait()
    pool_k[cz, cy, :POOLED] = dot(mean, k_all[kv], NN).astype(BF16)
    local[1].wait()
    pool_v[cz, cy] = dot(mean, v_all[kv], NN).astype(BF16)

    local[3].wait()
    lane = lax.broadcasted_iota(jnp.int32, (1, LISTED), 1)
    listed = jnp.zeros((1, LISTED), jnp.int32)
    for b in range(BLOCKS):
        for c in range(CHOSEN):
            listed = jnp.where(lane == b * CHOSEN + c, chosen_ref[b, c], listed)
    row = lax.broadcasted_iota(jnp.int32, (16, LISTED), 0)
    both = jnp.where(row == 0, listed // POOLED, jnp.where(row == 1, listed % POOLED, 0))
    pool_k[cz, cy, POOLED:] = both.astype(F32).astype(BF16)
    meet(len(peers))

    send = Sender(send_sems, recv_sems)
    first, wide, small = {}, {}, {}
    pools = ((0, pool_k), (1, pool_v))

    def pool_chunk(axis, ref, o):
        return ref.at[shifted(cz, o), cy] if axis == 0 else ref.at[cz, shifted(cy, o)]

    def pool_row(axis, ref, o, part=pl.ds(0, SIDE)):
        return ref.at[part, shifted(cy, o)] if axis == 0 else ref.at[shifted(cz, o), part]

    for axis, ref in pools:
        here = pool_chunk(axis, ref, 0)
        small[axis] = [send(here, here, along(axis, s)) for s in (1, -1)]
    arrays = ((0, k_all), (1, v_all))
    for axis, full in arrays:
        here = full.at[kv]
        first[axis] = [send(here, here, along(axis, s)) for s in (1, -1)]
    local[2].wait()
    here = h_all.at[tp]
    x_first = [send(here, here, xdev(s, core)) for s in (1, -1)]
    x_over = [send(here, here, xdev(0, 1 - core))]
    for axis, ref in pools:
        for copy in small[axis]:
            copy.wait_recv()
        passed = pool_chunk(axis, ref, -1)
        small[axis] = [send(passed, passed, along(axis, 1))]
    for axis, full in arrays:
        here = full.at[kv]
        wide[axis] = [(0, [send(here, here, along(1 - axis, s)) for s in (1, -1)])]
    for axis, ref in pools:
        small[axis][0].wait_recv()
        row = pool_row(axis, ref, 0)
        small[axis] = [send(row, row, along(1 - axis, s)) for s in (1, -1)]

    second = {}
    for axis, full in arrays:
        plus, minus = first[axis]
        plus.wait_recv()
        part = full.at[owner(axis, -1, 0), pl.ds(0, half)]
        fwd = send(part, part, along(axis, 1))
        whole = full.at[owner(axis, -1, 0)]
        wide[axis].append((-1, [send(whole, whole, along(1 - axis, s)) for s in (1, -1)]))
        minus.wait_recv()
        part = full.at[owner(axis, 1, 0), pl.ds(half, half)]
        bwd = send(part, part, along(axis, -1))
        second[axis] = (fwd, bwd)
    for axis, ref in pools:
        plus, minus = small[axis]
        plus.wait_recv()
        part = pool_row(axis, ref, -1, pl.ds(0, 2))
        minus_part = pool_row(axis, ref, 1, pl.ds(2, 2))
        fwd = send(part, part, along(1 - axis, 1))
        minus.wait_recv()
        small[axis] = [fwd, send(minus_part, minus_part, along(1 - axis, -1))]
    for axis, full in arrays:
        whole = full.at[owner(axis, 1, 0)]
        wide[axis].append((1, [send(whole, whole, along(1 - axis, s)) for s in (1, -1)]))

    last = []

    def across(axis, full, o, pair):
        plus, minus = pair
        plus.wait_recv()
        part = full.at[owner(axis, o, -1), pl.ds(0, half)]
        last.append(send(part, part, along(1 - axis, 1)))
        minus.wait_recv()
        part = full.at[owner(axis, o, 1), pl.ds(half, half)]
        last.append(send(part, part, along(1 - axis, -1)))

    for axis, full in arrays:
        across(axis, full, *wide[axis][0])
    for axis, full in arrays:
        for copy in second[axis]:
            copy.wait_recv()
        whole = full.at[owner(axis, 2, 0)]
        wide[axis].append((2, [send(whole, whole, along(1 - axis, s)) for s in (1, -1)]))

    for copy in local[4:]:
        copy.wait()
    for axis, ref in pools:
        for copy in small[axis]:
            copy.wait_recv()
    pk_ref[...] = pool_k[:, :, :POOLED].reshape(OWNERS * POOLED, HEAD_DIM)
    pv_ref[...] = pool_v[...].reshape(OWNERS * POOLED, HEAD_DIM)
    dpk_ref[...] = jnp.zeros_like(dpk_ref)
    dpv_ref[...] = jnp.zeros_like(dpv_ref)

    def listing(i):
        both = pool_k[i // SIDE, i % SIDE, POOLED:].astype(F32)
        owners, numbers, column = both[0:1, :], both[1:2, :], both.T[:, 0:1]
        one = lax.broadcasted_iota(jnp.int32, (LISTED, LISTED), 0)
        two = lax.broadcasted_iota(jnp.int32, (LISTED, LISTED), 1)
        same = jnp.where(column == owners, 1.0, 0.0)
        rank = jnp.sum(jnp.where(one < two, same, 0.0), axis=0, keepdims=True)
        return owners, numbers, rank

    def grid(rows, f):
        return f(lax.broadcasted_iota(jnp.int32, (rows, LISTED), 0)).astype(F32)

    def ones(seen):
        return jnp.where(seen, 1.0, 0.0)

    owners, numbers, rank = listing(kv)
    kv_f = kv.astype(F32)
    at, nth = grid(SLOTS, lambda i: i // CHOSEN), grid(SLOTS, lambda i: i % CHOSEN)
    own = jnp.where(owners == kv_f, -1.0, owners)
    pick_ref[:SLOTS] = (ones(own == at) * ones(rank == nth)).astype(BF16)
    at = grid(POOLED, lambda i: i)
    pick_ref[SLOTS:] = (ones(owners == kv_f) * ones(numbers == at)).astype(BF16)

    for axis in (0, 1):
        def owner_id(i, axis=axis):
            return cz * SIDE + i if axis == 0 else i * SIDE + cy

        for pair in (0, 1):
            total = None
            for n in (0, 1):
                who = owner(axis, (0, -1, 1, 2)[2 * pair + n], 0)
                owners, numbers, rank = listing(who)
                at = grid(LISTED, lambda i: owner_id(i // POOLED))
                nth = grid(LISTED, lambda i: i % POOLED)
                blocks = ones(owners == at) * ones(numbers == nth)
                at = grid(LISTED, lambda i: owner_id((i % 64) // CHOSEN))
                nth = grid(LISTED, lambda i, n=n: jnp.where(i // 64 == n, i % CHOSEN, -1))
                own = jnp.where(owners == who.astype(F32), -1.0, owners)
                slots = ones(own == at) * ones(rank == nth)
                part = dot(blocks.astype(BF16), slots.astype(BF16), NT)
                total = part if total is None else total + part
            place_ref[axis, :, pair * LISTED : (pair + 1) * LISTED] = total.astype(BF16)

    n_pool = OWNERS * POOLED
    wide_q = GROUP * QUERY_BLOCK
    pool_end = lax.broadcasted_iota(jnp.int32, (n_pool, wide_q), 0) * POOL_BLOCK + POOL_BLOCK - 1
    lane = lax.broadcasted_iota(jnp.int32, (n_pool, wide_q), 1) % QUERY_BLOCK
    ahead = pool_end - lane

    def tile(t, carry):
        qs, cs, ls = tile_operands(q_ref, g_ref, gate_ref, ls_ref, t)
        qs_all[t] = qs
        cs_all[t] = cs[1]
        ls_rows[t] = ls[1]
        visible = ahead <= kv * TOKENS + t * QUERY_BLOCK
        dq, dk, dv = attend_back(qs, cs[0], ls[0], pk_ref[...], pv_ref[...], visible)
        dq_ref[t] = dq
        dpk_ref[...] += dk
        dpv_ref[...] += dv
        return carry

    lax.fori_loop(0, BLOCKS // 2, tile, 0)
    rows = TOKENS // 16
    plus, minus = x_first
    plus.wait_recv()
    whole = h_all.at[shifted(cx, -1) * 2 + core]
    part = whole.at[pl.ds(0, rows)]
    x_second = [send(part, part, xdev(1, core))]
    x_over.append(send(whole, whole, xdev(0, 1 - core)))
    minus.wait_recv()
    whole = h_all.at[shifted(cx, 1) * 2 + core]
    part = whole.at[pl.ds(rows, rows)]
    x_second.append(send(part, part, xdev(-1, core)))
    x_over.append(send(whole, whole, xdev(0, 1 - core)))
    for axis, full in arrays:
        across(axis, full, *wide[axis][1])
    lax.fori_loop(BLOCKS // 2, BLOCKS, tile, 0)
    dpk_ref[...] = dpk_ref[...] * (SCALE / POOL_BLOCK)
    dpv_ref[...] = dpv_ref[...] * (1.0 / POOL_BLOCK)
    for axis, full in arrays:
        across(axis, full, *wide[axis][2])
    for copy in x_second:
        copy.wait_recv()
    whole = h_all.at[shifted(cx, 2) * 2 + core]
    x_over.append(send(whole, whole, xdev(0, 1 - core)))
    for axis, full in arrays:
        across(axis, full, *wide[axis][3])
    for copy in last:
        copy.wait_recv()
    for copy in x_over:
        copy.wait_recv()
    send.finish()


GATHER_COPIES = 2 * (2 + 2 + 8 + 8) + 2 + 2 + 4 + 14


def run_gather(k, v, h, q, g, gates, sums, chosen):
    hbm = pl.BlockSpec(memory_space=pltpu.HBM)
    vmem = pl.BlockSpec(memory_space=pltpu.VMEM)
    n_pool = OWNERS * POOLED
    wide_q = GROUP * QUERY_BLOCK
    return pl.pallas_call(
        gather_kernel,
        name="gather",
        out_shape=(
            jax.ShapeDtypeStruct((OWNERS, TOKENS, HEAD_DIM), BF16),
            jax.ShapeDtypeStruct((OWNERS, TOKENS, HEAD_DIM), BF16),
            jax.ShapeDtypeStruct((8, TOKENS // 8, MODEL), BF16),
            jax.ShapeDtypeStruct((BLOCKS, HEAD_DIM, wide_q), F32),
            jax.ShapeDtypeStruct((n_pool, HEAD_DIM), F32),
            jax.ShapeDtypeStruct((n_pool, HEAD_DIM), F32),
            jax.ShapeDtypeStruct((BLOCKS, wide_q, HEAD_DIM), BF16),
            jax.ShapeDtypeStruct((BLOCKS, wide_q, HEAD_DIM), BF16),
            jax.ShapeDtypeStruct((BLOCKS, 1, wide_q), F32),
            jax.ShapeDtypeStruct((SLOTS + POOLED, LISTED), BF16),
            jax.ShapeDtypeStruct((2, LISTED, SLOTS), BF16),
        ),
        in_specs=[hbm] * 8,
        out_specs=(vmem,) * 11,
        scratch_shapes=[
            pltpu.SMEM((BLOCKS, CHOSEN), jnp.int32),
            pltpu.VMEM(q.shape, BF16),
            pltpu.VMEM(g.shape, BF16),
            pltpu.VMEM(gates.shape, F32),
            pltpu.VMEM(sums.shape, F32),
            pltpu.VMEM((SIDE, SIDE, POOLED + 16, HEAD_DIM), BF16),
            pltpu.VMEM((SIDE, SIDE, POOLED, HEAD_DIM), BF16),
            pltpu.VMEM((n_pool, HEAD_DIM), BF16),
            pltpu.VMEM((n_pool, HEAD_DIM), BF16),
            pltpu.SemaphoreType.DMA((GATHER_COPIES,)),
            pltpu.SemaphoreType.DMA((GATHER_COPIES,)),
            pltpu.SemaphoreType.DMA((8,)),
        ],
        compiler_params=pltpu.CompilerParams(
            collective_id=0, has_side_effects=True, vmem_limit_bytes=12 * MIB
        ),
        cost_estimate=pl.CostEstimate(
            flops=40_000_000_000, bytes_accessed=8 * MIB, transcendentals=0
        ),
    )(*(pltpu.with_memory_space_constraint(a, pltpu.HBM) for a in (k, v, h, q, g, gates, sums, chosen)))


class Reduce:
    def __init__(self, send, axis, src, bufs, coords, along):
        self.relay, self.direct, self.comb, self.relay2, self.direct2, self.comb2 = bufs
        self.send, self.axis, self.src = send, axis, src
        self.c1, self.c2 = (coords[0], coords[1]) if axis == 0 else (coords[1], coords[0])
        self.to1 = lambda o: along(axis, o)
        self.to2 = lambda o: along(1 - axis, o)
        self.half = src.shape[2] // 2
        self.rows = (pl.ds(0, self.half), pl.ds(self.half, self.half))

    def bundle(self, o, n):
        c = shifted(self.c1, o)
        rows = self.rows[n]
        return self.src.at[c, :, rows] if self.axis == 0 else self.src.at[:, c, rows]

    def piece(self, o, i, n):
        c = shifted(self.c1, o)
        if self.axis == 0:
            return self.src[c, i, self.rows[n], :].astype(F32)
        return self.src[i, c, self.rows[n], :].astype(F32)

    def part(self, o, n):
        return self.comb.at[n, shifted(self.c2, o)]

    def begin(self):
        s = self.send
        self.r = [
            s(self.bundle(2, 0), self.relay.at[0], self.to1(1)),
            s(self.bundle(2, 1), self.relay.at[1], self.to1(-1)),
        ]
        self.d = [
            s(self.bundle(1, 1), self.direct.at[0], self.to1(1)),
            s(self.bundle(-1, 0), self.direct.at[1], self.to1(-1)),
        ]

    def combine(self):
        self.c = []
        for n, o in enumerate((1, -1)):
            self.r[n].wait_recv()

            def add(i, carry, n=n, o=o):
                self.relay[n, i] = (self.piece(o, i, n) + self.relay[n, i].astype(F32)).astype(BF16)
                return carry

            lax.fori_loop(0, SIDE, add, 0)
            self.c.append(self.send(self.relay.at[n], self.comb.at[n], self.to1(o)))

    def turn(self):
        for copy in self.d + self.c:
            copy.wait_recv()

        def add(i, carry):
            for n in (0, 1):
                self.comb[n, i] = (
                    self.piece(0, i, n)
                    + self.comb[n, i].astype(F32)
                    + self.direct[1 - n, i].astype(F32)
                ).astype(BF16)
            return carry

        lax.fori_loop(0, SIDE, add, 0)
        self.start_second()

    def start_second(self):
        s = self.send
        self.r = [
            s(self.part(2, 0), self.relay2.at[0], self.to2(1)),
            s(self.part(2, 1), self.relay2.at[1], self.to2(-1)),
        ]
        self.d = [
            s(self.part(1, 1), self.direct2.at[0], self.to2(1)),
            s(self.part(-1, 0), self.direct2.at[1], self.to2(-1)),
        ]

    def combine2(self):
        self.c = []
        for n, o in enumerate((1, -1)):
            self.r[n].wait_recv()
            self.relay2[n] = (
                self.comb[n, shifted(self.c2, o)].astype(F32) + self.relay2[n].astype(F32)
            ).astype(BF16)
            self.c.append(self.send(self.relay2.at[n], self.comb2.at[n], self.to2(o)))

    def end(self):
        for copy in self.d + self.c:
            copy.wait_recv()
        return [
            self.comb[n, self.c2].astype(F32)
            + self.comb2[n].astype(F32)
            + self.direct2[1 - n].astype(F32)
            for n in (0, 1)
        ]


class ListedReduce(Reduce):
    def __init__(self, send, axis, src, bufs, coords, along, place_ref, own):
        self.passed, self.far, self.near, *after = bufs
        super().__init__(send, axis, src, (None, None, *after), coords, along)
        self.place_ref, self.own = place_ref, own
        self.steps = HALF_BLOCK * CHOSEN
        self.pooled = self

    def begin(self):
        s = self.send
        every = pl.ds(0, self.src.shape[2])
        self.rows = self.rows + (every,)
        self.r = [
            s(self.bundle(2, 0), self.passed.at[0], self.to1(1)),
            s(self.bundle(2, 1), self.passed.at[1], self.to1(-1)),
        ]
        self.d = [
            s(self.bundle(1, 2), self.near.at[0], self.to1(1)),
            s(self.bundle(-1, 2), self.near.at[1], self.to1(-1)),
        ]

    def combine(self):
        self.c = []
        for n, o in enumerate((1, -1)):
            self.r[n].wait_recv()
            self.c.append(self.send(self.passed.at[n], self.far.at[:, self.rows[n]], self.to1(o)))

    def sources(self, rows):
        mine = self.src[self.c1, :, rows, :] if self.axis == 0 else self.src[:, self.c1, rows, :]
        return [mine, self.near[0, :, rows, :], self.near[1, :, rows, :], self.far[:, rows, :]]

    def turn(self):
        for copy in self.d + self.c:
            copy.wait_recv()
        pooled = sum(x.astype(F32) for x in self.pooled.sources(pl.ds(self.steps, POOLED)))
        pooled = pooled.reshape(SIDE * POOLED, HEAD_DIM)
        pooled = jnp.concatenate([pooled, pooled], axis=1)
        for n in (0, 1):

            def put(i, carry, n=n):
                pieces = []
                for j in (0, 1):
                    first = pl.multiple_of((n * HALF_BLOCK // 2 + 2 * i + j) * CHOSEN, CHOSEN)
                    got = [x.reshape(SIDE * CHOSEN, HEAD_DIM) for x in self.sources(pl.ds(first, CHOSEN))]
                    pieces.append(jnp.concatenate(got, axis=0))
                total = dot(self.place_ref[self.axis], jnp.concatenate(pieces, axis=1), NN)
                total = total + pooled
                for j in (0, 1):
                    rows = pl.ds(pl.multiple_of((2 * i + j) * POOLED, POOLED), POOLED)
                    part = total[:, j * HEAD_DIM : (j + 1) * HEAD_DIM].astype(BF16)
                    self.comb[n, :, rows, :] = part.reshape(SIDE, POOLED, HEAD_DIM)
                return carry

            lax.fori_loop(0, HALF_BLOCK // 4, put, 0, unroll=2)
        self.start_second()

    def end(self):
        at = self.own[1]
        size = HALF_BLOCK // 2 * POOLED
        return [
            part + self.own[0][at + n * size : at + (n + 1) * size, :]
            for n, part in enumerate(super().end())
        ]


def listed_buffers(rows):
    half, size = rows // 2, HALF_BLOCK // 2 * POOLED
    slim = pltpu.VMEM((2, size, HEAD_DIM), BF16)
    return [
        pltpu.VMEM((2, SIDE, half, HEAD_DIM), BF16),
        pltpu.VMEM((SIDE, rows, HEAD_DIM), BF16),
        pltpu.VMEM((2, SIDE, rows, HEAD_DIM), BF16),
        pltpu.VMEM((2, SIDE, size, HEAD_DIM), BF16),
        slim, slim, slim,
    ]


def reduce_buffers(rows, lanes):
    half = rows // 2
    wide = pltpu.VMEM((2, SIDE, half, lanes), BF16)
    slim = pltpu.VMEM((2, half, lanes), BF16)
    return [wide] * 3 + [slim] * 3


REDUCE_BUFS = 6
LISTED_BUFS = 7
GW_COLS = MODEL // OWNERS
PAIR = GROUP // 2 * HEAD_DIM
PAIR_Q = GROUP // 2 * QUERY_BLOCK
UNROLL = 4
HALF_BLOCK = KEY_BLOCK // 2
SETS = CHOSEN * KEY_BLOCK


def scatter_kernel(
    chosen_ref, k_ref, v_ref, h_ref, dqp_ref, dpk_ref, dpv_ref, qs_all, cs_all, ls_rows, pick_ref, place_ref,
    gq_ref, gk_out, gv_out, gw_out,
    kb, vb, dk_set, dv_set, gqt, dk0, dv0, dk1, dv1, own_k, own_v, gw0, gw1, gw2, gw3, *rest
):
    cut = 4 * LISTED_BUFS
    bufs = [rest[i * LISTED_BUFS : (i + 1) * LISTED_BUFS] for i in range(4)]
    gw_bufs = [rest[cut + i * REDUCE_BUFS : cut + (i + 1) * REDUCE_BUFS] for i in range(4)]
    send_sems, recv_sems = rest[cut + 4 * REDUCE_BUFS :]
    kv, tp, cz, cy, cx, core = place()

    def along(axis, o):
        if axis == 0:
            return (shifted(cz, o) * SIDE + cy, tp)
        return (cz * SIDE + shifted(cy, o), tp)

    peers = [along(axis, o) for axis in (0, 1) for o in (1, -1)]
    greet(peers)
    send = Sender(send_sems, recv_sems)
    gws = (gw0, gw1, gw2, gw3)
    kv_parts = (dk0, dv0, dk1, dv1)
    half_rows = HALF_BLOCK * POOLED
    owns = ((own_k, 0), (own_v, 0), (own_k, half_rows), (own_v, half_rows))
    k0, v0, k1, v1 = [
        ListedReduce(send, axis, src, buf, (cz, cy), along, place_ref, own)
        for axis, src, buf, own in zip((0, 1) * 2, kv_parts, bufs, owns)
    ]
    k1.pooled, v1.pooled = k0, v0
    w0, w1, w2, w3 = [
        Reduce(send, axis, src, buf, (cz, cy), along)
        for axis, src, buf in zip((0, 1) * 2, gws, gw_bufs)
    ]

    ahead = (
        lax.broadcasted_iota(jnp.int32, (KEY_BLOCK, PAIR_Q), 0)
        - lax.broadcasted_iota(jnp.int32, (KEY_BLOCK, PAIR_Q), 1) % QUERY_BLOCK
    )

    def attend(pair):
        across = slice(pair * PAIR_Q, (pair + 1) * PAIR_Q)

        def block(b, carry):
            start_row = kv * TOKENS + b * QUERY_BLOCK
            seen = []
            for c in range(CHOSEN):
                at = chosen_ref[b, c]
                kb[c * KEY_BLOCK : (c + 1) * KEY_BLOCK, :] = k_ref[at]
                vb[c * KEY_BLOCK : (c + 1) * KEY_BLOCK, :] = v_ref[at]
                seen.append(ahead <= start_row - at * KEY_BLOCK)
            dq, dk, dv = attend_back(
                qs_all[b, across, :],
                cs_all[b, across, :],
                ls_rows[b, :, across],
                kb[...],
                vb[...],
                jnp.concatenate(seen, axis=0),
            )
            total = (dqp_ref[b, :, across] + dq) * SCALE
            rows = pl.ds(pl.multiple_of(b * QUERY_BLOCK, QUERY_BLOCK), QUERY_BLOCK)
            for h in range(GROUP // 2):
                part = total[:, h * QUERY_BLOCK : (h + 1) * QUERY_BLOCK]
                at = pair * PAIR + h * HEAD_DIM
                gqt[at : at + HEAD_DIM, rows] = part.astype(BF16)
                gq_ref[rows, at : at + HEAD_DIM] = part.T.astype(BF16)
            here = pl.ds(pl.multiple_of(b * SETS, SETS), SETS)
            if pair == 0:
                dk_set[here, :] = dk * SCALE
                dv_set[here, :] = dv
            else:
                dk_set[here, :] += dk * SCALE
                dv_set[here, :] += dv
            return carry

        return block

    def product(pair):
        def one(j, carry):
            wide = SIDE * GW_COLS
            cols = pl.ds(pl.multiple_of(j * wide, wide), wide)
            part = dot(gqt[pair * PAIR : (pair + 1) * PAIR, :], h_ref[:, cols], NN).astype(BF16)
            for i in range(SIDE):
                piece = part[:, i * GW_COLS : (i + 1) * GW_COLS]
                gws[2 * pair][j, i] = piece[:HEAD_DIM]
                gws[2 * pair + 1][j, i] = piece[HEAD_DIM:]
            return carry

        lax.fori_loop(0, SIDE, one, 0)

    lax.fori_loop(0, BLOCKS, attend(0), 0, unroll=2)
    product(0)
    meet(len(peers))
    w0.begin()
    w1.begin()
    lax.fori_loop(0, BLOCKS // 2, attend(1), 0, unroll=2)
    w0.combine()
    w1.combine()
    lax.fori_loop(BLOCKS // 2, BLOCKS, attend(1), 0, unroll=2)

    product(1)
    w2.begin()
    w3.begin()
    w0.turn()
    w1.turn()

    slots = (SIDE, SIDE, CHOSEN, HEAD_DIM)

    def spread(part):
        dk_out, dv_out = kv_parts[2 * part : 2 * part + 2]

        def one(i, carry):
            every = pl.ds(part * HALF_BLOCK + i, LISTED, stride=KEY_BLOCK)
            got = jnp.concatenate([dk_set[every, :], dv_set[every, :]], axis=1).astype(BF16)
            got = dot(pick_ref[...], got, NN)
            rows = pl.ds(pl.multiple_of(i * CHOSEN, CHOSEN), CHOSEN)
            dk_out[:, :, rows, :] = got[:SLOTS, :HEAD_DIM].astype(BF16).reshape(slots)
            dv_out[:, :, rows, :] = got[:SLOTS, HEAD_DIM:].astype(BF16).reshape(slots)
            rows = pl.ds(pl.multiple_of((part * HALF_BLOCK + i) * POOLED, POOLED), POOLED)
            own_k[rows, :] = got[SLOTS:, :HEAD_DIM]
            own_v[rows, :] = got[SLOTS:, HEAD_DIM:]
            return carry

        lax.fori_loop(0, HALF_BLOCK, one, 0, unroll=UNROLL)

    tail = slice(HALF_BLOCK * CHOSEN, HALF_BLOCK * CHOSEN + POOLED)
    pooled = (SIDE, SIDE, POOLED, HEAD_DIM)
    dk0[:, :, tail, :] = dpk_ref[...].astype(BF16).reshape(pooled)
    dv0[:, :, tail, :] = dpv_ref[...].astype(BF16).reshape(pooled)
    spread(0)
    k0.begin()
    v0.begin()
    w2.combine()
    w3.combine()
    w0.combine2()
    w1.combine2()
    spread(1)
    k1.begin()
    v1.begin()
    w2.turn()
    w3.turn()

    def weight(n, w):
        for i, part in enumerate(w.end()):
            at = n * HEAD_DIM + i * HEAD_DIM // 2
            gw_out[:, at : at + HEAD_DIM // 2] = part.T

    def ordered(into, part, r):
        for n, rows in enumerate(r.end()):
            for i in range(HALF_BLOCK // 2):
                at = part * HALF_BLOCK + n * (HALF_BLOCK // 2) + i
                into[pl.ds(at, POOLED, stride=KEY_BLOCK), :] = rows[i * POOLED : (i + 1) * POOLED]

    k0.combine()
    v0.combine()
    w2.combine2()
    w3.combine2()
    k1.combine()
    v1.combine()
    k0.turn()
    v0.turn()
    k1.turn()
    v1.turn()
    weight(0, w0)
    weight(1, w1)
    k0.combine2()
    v0.combine2()
    k1.combine2()
    v1.combine2()
    weight(2, w2)
    weight(3, w3)
    ordered(dk_set, 0, k0)
    ordered(dv_set, 0, v0)
    ordered(dk_set, 1, k1)
    ordered(dv_set, 1, v1)
    gk_out[...] = dk_set[:TOKENS, :].astype(BF16)
    gv_out[...] = dv_set[:TOKENS, :].astype(BF16)
    send.finish()


SCATTER_COPIES = 8 * 12
SCATTER_MIB = 28


def run_scatter(chosen, k_all, v_all, h_all, dqp, dpk, dpv, qs, cs, ls, pick, places):
    vmem = pl.BlockSpec(memory_space=pltpu.VMEM)
    smem = pl.BlockSpec(memory_space=pltpu.SMEM)
    first = HALF_BLOCK * CHOSEN + POOLED
    second = HALF_BLOCK * CHOSEN
    outgoing = [pltpu.VMEM((SIDE, SIDE, n, HEAD_DIM), BF16) for n in (first, first, second, second)]
    grad = pltpu.VMEM((SIDE, SIDE, HEAD_DIM, GW_COLS), BF16)
    return pl.pallas_call(
        scatter_kernel,
        name="scatter",
        out_shape=(
            jax.ShapeDtypeStruct((TOKENS, GROUP * HEAD_DIM), BF16),
            jax.ShapeDtypeStruct((TOKENS, HEAD_DIM), BF16),
            jax.ShapeDtypeStruct((TOKENS, HEAD_DIM), BF16),
            jax.ShapeDtypeStruct((GW_COLS, GROUP * HEAD_DIM), F32),
        ),
        in_specs=[smem] + [vmem] * 11,
        out_specs=(vmem,) * 4,
        scratch_shapes=[
            pltpu.VMEM((SETS, HEAD_DIM), BF16),
            pltpu.VMEM((SETS, HEAD_DIM), BF16),
            pltpu.VMEM((BLOCKS * SETS, HEAD_DIM), F32),
            pltpu.VMEM((BLOCKS * SETS, HEAD_DIM), F32),
            pltpu.VMEM((GROUP * HEAD_DIM, TOKENS), BF16),
            *outgoing,
            pltpu.VMEM((TOKENS, HEAD_DIM), F32),
            pltpu.VMEM((TOKENS, HEAD_DIM), F32),
            grad,
            grad,
            grad,
            grad,
            *(listed_buffers(first) * 2),
            *(listed_buffers(second) * 2),
            *(reduce_buffers(HEAD_DIM, GW_COLS) * 4),
            pltpu.SemaphoreType.DMA((SCATTER_COPIES,)),
            pltpu.SemaphoreType.DMA((SCATTER_COPIES,)),
        ],
        compiler_params=pltpu.CompilerParams(
            collective_id=1, has_side_effects=True, vmem_limit_bytes=SCATTER_MIB * MIB
        ),
    )(chosen, k_all, v_all, h_all, dqp, dpk, dpv, qs, cs, ls, pick, places)


def finish_kernel(*refs):
    copies = [pltpu.make_async_copy(refs[i], refs[4 + i], refs[8].at[i]) for i in range(4)]
    for copy in copies:
        copy.start()
    for copy in copies:
        copy.wait()


def run_finish(*outs):
    return pl.pallas_call(
        finish_kernel,
        name="finish",
        out_shape=tuple(jax.ShapeDtypeStruct(a.shape, a.dtype) for a in outs),
        in_specs=[pl.BlockSpec(memory_space=pltpu.VMEM)] * 4,
        out_specs=(pl.BlockSpec(memory_space=pltpu.HBM),) * 4,
        scratch_shapes=[pltpu.SemaphoreType.DMA((4,))],
        compiler_params=pltpu.CompilerParams(vmem_limit_bytes=8 * MIB),
    )(*outs)


def body(hidden_rows, queries, key_rows, value_rows, branch_gates, log_sums, chosen, out_grad):
    lists = chosen.reshape(BLOCKS, CHOSEN)
    k_all, v_all, h_all, *more = run_gather(
        key_rows, value_rows, hidden_rows, queries, out_grad, branch_gates, log_sums, lists
    )
    by_block = (SEQ // KEY_BLOCK, KEY_BLOCK, HEAD_DIM)
    outs = run_scatter(
        lists,
        k_all.reshape(by_block),
        v_all.reshape(by_block),
        h_all.reshape(TOKENS, MODEL),
        *more,
    )
    return run_finish(*outs)


def solution(mesh):
    placed = (
        P(("kv", "tp"), None),
        P("kv", "tp"),
        P("kv", "tp"),
        P("kv", "tp"),
        P(None, "tp", "kv"),
        P(None, "tp", "kv"),
        P("tp", "kv", None),
        P("kv", "tp"),
    )
    return jax.shard_map(
        body,
        mesh=mesh,
        in_specs=placed,
        out_specs=(P("kv", "tp"), P("kv", "tp"), P("kv", "tp"), P("kv", "tp")),
        check_vma=False,
    )
```

```python
import jax
import jax.numpy as jnp
from jax import lax
from jax.experimental import pallas as pl
from jax.experimental.pallas import tpu as pltpu
from jax.sharding import PartitionSpec as P

HEADS = 32
KV_HEADS = 8
HEAD_DIM = 128
QUERY_BLOCK = 128
KEY_BLOCK = 32
POOL_BLOCK = 32
CHOSEN = 16
GROUP = HEADS // KV_HEADS
SIDE = 4
OWNERS = SIDE * SIDE
TOKENS = 1024
BLOCKS = TOKENS // QUERY_BLOCK
POOLED = TOKENS // POOL_BLOCK
SEQ = TOKENS * OWNERS
LISTED = BLOCKS * CHOSEN
SLOTS = OWNERS * CHOSEN
MODEL = 4096
SCALE = HEAD_DIM ** (-0.5)
LOG2E = 1.4426950408889634
MIB = 1 << 20
MESH = pl.DeviceIdType.MESH
F32 = jnp.float32
BF16 = jnp.bfloat16

NT = (((1,), (1,)), ((), ()))
NN = (((1,), (0,)), ((), ()))


def dot(a, b, dims):
    return lax.dot_general(a, b, dims, preferred_element_type=F32)


class Sender:
    def __init__(self, send_sems, recv_sems):
        self.send_sems, self.recv_sems, self.at, self.sent = send_sems, recv_sems, 0, []

    def __call__(self, src, dst, dev):
        copy = pltpu.make_async_remote_copy(
            src_ref=src,
            dst_ref=dst,
            send_sem=self.send_sems.at[self.at],
            recv_sem=self.recv_sems.at[self.at],
            device_id=dev,
            device_id_type=MESH,
        )
        self.at += 1
        copy.start()
        self.sent.append(copy)
        return copy

    def finish(self):
        for copy in self.sent:
            copy.wait_send()


def place():
    kv, tp = lax.axis_index("kv"), lax.axis_index("tp")
    return kv, tp, kv // SIDE, kv % SIDE, tp // 2, tp % 2


def shifted(c, o):
    return (c + (o + SIDE)) % SIDE


def greet(devices):
    for dev in devices:
        pl.semaphore_signal(
            pltpu.get_barrier_semaphore(), inc=1, device_id=dev, device_id_type=MESH
        )


def meet(count):
    pl.semaphore_wait(pltpu.get_barrier_semaphore(), count)


def tile_operands(q_ref, g_ref, gate_ref, ls_ref, t):
    rows = pl.ds(pl.multiple_of(t * QUERY_BLOCK, QUERY_BLOCK), QUERY_BLOCK)
    gates = jnp.concatenate([gate_ref[0, :, rows], gate_ref[1, :, rows]], axis=0).T
    qs, cs, ls = [], ([], []), ([], [])
    for h in range(GROUP):
        cols = slice(h * HEAD_DIM, (h + 1) * HEAD_DIM)
        qs.append(q_ref[rows, cols])
        grad = g_ref[rows, cols].astype(F32)
        for branch in (0, 1):
            at = branch * GROUP + h
            cs[branch].append((gates[:, at : at + 1] * grad).astype(BF16))
            ls[branch].append(ls_ref[branch, h : h + 1, rows])
    return (
        jnp.concatenate(qs, axis=0),
        [jnp.concatenate(c, axis=0) for c in cs],
        [jnp.concatenate(x, axis=1) * LOG2E for x in ls],
    )


def attend_back(qs, cs, log_sum, keys, values, visible):
    scores = dot(keys, qs, NT) * (SCALE * LOG2E)
    p = jnp.where(visible, jnp.exp2(scores - log_sum), 0.0)
    pr = p.astype(BF16)
    dp = dot(values, cs, NT)
    delta = jnp.sum(p * dp, axis=0, keepdims=True)
    ds = (p * (dp - delta)).astype(BF16)
    return dot(keys.T, ds, NN), ds, pr


def gather_kernel(
    k_ref, v_ref, h_ref, q_hbm, g_hbm, gate_hbm, ls_hbm, chosen_hbm,
    k_all, v_all, h_all, dq_ref, dpk_ref, dpv_ref, qs_all, cs_all, ls_rows, pick_ref, place_ref,
    chosen_ref, q_ref, g_ref, gate_ref, ls_ref, pool_k, pool_v, pk_ref, pv_ref,
    send_sems, recv_sems, local_sems,
):
    kv, tp, cz, cy, cx, core = place()
    half = TOKENS // 2

    def device(oz, oy):
        return (shifted(cz, oz) * SIDE + shifted(cy, oy), tp)

    def along(axis, o):
        return device(o, 0) if axis == 0 else device(0, o)

    def owner(axis, o1, o2):
        a, b = (o1, o2) if axis == 0 else (o2, o1)
        return shifted(cz, a) * SIDE + shifted(cy, b)

    def xdev(o, c):
        return (kv, shifted(cx, o) * 2 + c)

    peers = [along(axis, s) for axis in (0, 1) for s in (1, -1)] + [
        xdev(1, core), xdev(-1, core), xdev(0, 1 - core)
    ]
    greet(peers)
    local = [
        pltpu.make_async_copy(src, dst, local_sems.at[i])
        for i, (src, dst) in enumerate(
            (
                (k_ref, k_all.at[kv]),
                (v_ref, v_all.at[kv]),
                (h_ref, h_all.at[tp]),
                (chosen_hbm, chosen_ref),
                (gate_hbm, gate_ref),
                (ls_hbm, ls_ref),
                (q_hbm, q_ref),
                (g_hbm, g_ref),
            )
        )
    ]
    for copy in local:
        copy.start()

    blk = lax.broadcasted_iota(jnp.int32, (POOLED, TOKENS), 0)
    row = lax.broadcasted_iota(jnp.int32, (POOLED, TOKENS), 1)
    mean = jnp.where(row // POOL_BLOCK == blk, 1.0 / POOL_BLOCK, 0.0).astype(BF16)
    local[0].wait()
    pool_k[cz, cy, :POOLED] = dot(mean, k_all[kv], NN).astype(BF16)
    local[1].wait()
    pool_v[cz, cy] = dot(mean, v_all[kv], NN).astype(BF16)

    local[3].wait()
    lane = lax.broadcasted_iota(jnp.int32, (1, LISTED), 1)
    listed = jnp.zeros((1, LISTED), jnp.int32)
    for b in range(BLOCKS):
        for c in range(CHOSEN):
            listed = jnp.where(lane == b * CHOSEN + c, chosen_ref[b, c], listed)
    row = lax.broadcasted_iota(jnp.int32, (16, LISTED), 0)
    both = jnp.where(row == 0, listed // POOLED, jnp.where(row == 1, listed % POOLED, 0))
    pool_k[cz, cy, POOLED:] = both.astype(F32).astype(BF16)
    meet(len(peers))

    send = Sender(send_sems, recv_sems)
    first, wide, small = {}, {}, {}
    pools = ((0, pool_k), (1, pool_v))

    def pool_chunk(axis, ref, o):
        return ref.at[shifted(cz, o), cy] if axis == 0 else ref.at[cz, shifted(cy, o)]

    def pool_row(axis, ref, o, part=pl.ds(0, SIDE)):
        return ref.at[part, shifted(cy, o)] if axis == 0 else ref.at[shifted(cz, o), part]

    for axis, ref in pools:
        here = pool_chunk(axis, ref, 0)
        small[axis] = [send(here, here, along(axis, s)) for s in (1, -1)]
    arrays = ((0, k_all), (1, v_all))
    for axis, full in arrays:
        here = full.at[kv]
        first[axis] = [send(here, here, along(axis, s)) for s in (1, -1)]
    local[2].wait()
    here = h_all.at[tp]
    x_first = [send(here, here, xdev(s, core)) for s in (1, -1)]
    x_over = [send(here, here, xdev(0, 1 - core))]
    for axis, ref in pools:
        for copy in small[axis]:
            copy.wait_recv()
        passed = pool_chunk(axis, ref, -1)
        small[axis] = [send(passed, passed, along(axis, 1))]
    for axis, full in arrays:
        here = full.at[kv]
        wide[axis] = [(0, [send(here, here, along(1 - axis, s)) for s in (1, -1)])]
    for axis, ref in pools:
        small[axis][0].wait_recv()
        row = pool_row(axis, ref, 0)
        small[axis] = [send(row, row, along(1 - axis, s)) for s in (1, -1)]

    second = {}
    for axis, full in arrays:
        plus, minus = first[axis]
        plus.wait_recv()
        part = full.at[owner(axis, -1, 0), pl.ds(0, half)]
        fwd = send(part, part, along(axis, 1))
        whole = full.at[owner(axis, -1, 0)]
        wide[axis].append((-1, [send(whole, whole, along(1 - axis, s)) for s in (1, -1)]))
        minus.wait_recv()
        part = full.at[owner(axis, 1, 0), pl.ds(half, half)]
        bwd = send(part, part, along(axis, -1))
        second[axis] = (fwd, bwd)
    for axis, ref in pools:
        plus, minus = small[axis]
        plus.wait_recv()
        part = pool_row(axis, ref, -1, pl.ds(0, 2))
        minus_part = pool_row(axis, ref, 1, pl.ds(2, 2))
        fwd = send(part, part, along(1 - axis, 1))
        minus.wait_recv()
        small[axis] = [fwd, send(minus_part, minus_part, along(1 - axis, -1))]
    for axis, full in arrays:
        whole = full.at[owner(axis, 1, 0)]
        wide[axis].append((1, [send(whole, whole, along(1 - axis, s)) for s in (1, -1)]))

    last = []

    def across(axis, full, o, pair):
        plus, minus = pair
        plus.wait_recv()
        part = full.at[owner(axis, o, -1), pl.ds(0, half)]
        last.append(send(part, part, along(1 - axis, 1)))
        minus.wait_recv()
        part = full.at[owner(axis, o, 1), pl.ds(half, half)]
        last.append(send(part, part, along(1 - axis, -1)))

    for axis, full in arrays:
        across(axis, full, *wide[axis][0])
    for axis, full in arrays:
        for copy in second[axis]:
            copy.wait_recv()
        whole = full.at[owner(axis, 2, 0)]
        wide[axis].append((2, [send(whole, whole, along(1 - axis, s)) for s in (1, -1)]))

    for copy in local[4:]:
        copy.wait()
    for axis, ref in pools:
        for copy in small[axis]:
            copy.wait_recv()
    pk_ref[...] = pool_k[:, :, :POOLED].reshape(OWNERS * POOLED, HEAD_DIM)
    pv_ref[...] = pool_v[...].reshape(OWNERS * POOLED, HEAD_DIM)
    dpk_ref[...] = jnp.zeros_like(dpk_ref)
    dpv_ref[...] = jnp.zeros_like(dpv_ref)

    def listing(i):
        both = pool_k[i // SIDE, i % SIDE, POOLED:].astype(F32)
        owners, numbers, column = both[0:1, :], both[1:2, :], both.T[:, 0:1]
        one = lax.broadcasted_iota(jnp.int32, (LISTED, LISTED), 0)
        two = lax.broadcasted_iota(jnp.int32, (LISTED, LISTED), 1)
        same = jnp.where(column == owners, 1.0, 0.0)
        rank = jnp.sum(jnp.where(one < two, same, 0.0), axis=0, keepdims=True)
        return owners, numbers, rank

    def grid(rows, f):
        return f(lax.broadcasted_iota(jnp.int32, (rows, LISTED), 0)).astype(F32)

    def ones(seen):
        return jnp.where(seen, 1.0, 0.0)

    owners, numbers, rank = listing(kv)
    kv_f = kv.astype(F32)
    at, nth = grid(SLOTS, lambda i: i // CHOSEN), grid(SLOTS, lambda i: i % CHOSEN)
    own = jnp.where(owners == kv_f, -1.0, owners)
    pick_ref[:SLOTS] = (ones(own == at) * ones(rank == nth)).astype(BF16)
    at = grid(POOLED, lambda i: i)
    pick_ref[SLOTS:] = (ones(owners == kv_f) * ones(numbers == at)).astype(BF16)

    for axis in (0, 1):
        def owner_id(i, axis=axis):
            return cz * SIDE + i if axis == 0 else i * SIDE + cy

        for pair in (0, 1):
            total = None
            for n in (0, 1):
                who = owner(axis, (0, -1, 1, 2)[2 * pair + n], 0)
                owners, numbers, rank = listing(who)
                at = grid(LISTED, lambda i: owner_id(i // POOLED))
                nth = grid(LISTED, lambda i: i % POOLED)
                blocks = ones(owners == at) * ones(numbers == nth)
                at = grid(LISTED, lambda i: owner_id((i % 64) // CHOSEN))
                nth = grid(LISTED, lambda i, n=n: jnp.where(i // 64 == n, i % CHOSEN, -1))
                own = jnp.where(owners == who.astype(F32), -1.0, owners)
                slots = ones(own == at) * ones(rank == nth)
                part = dot(blocks.astype(BF16), slots.astype(BF16), NT)
                total = part if total is None else total + part
            place_ref[axis, :, pair * LISTED : (pair + 1) * LISTED] = total.astype(BF16)

    n_pool = OWNERS * POOLED
    wide_q = GROUP * QUERY_BLOCK
    pool_end = lax.broadcasted_iota(jnp.int32, (n_pool, wide_q), 0) * POOL_BLOCK + POOL_BLOCK - 1
    lane = lax.broadcasted_iota(jnp.int32, (n_pool, wide_q), 1) % QUERY_BLOCK
    ahead = pool_end - lane

    def tile(t, carry):
        qs, cs, ls = tile_operands(q_ref, g_ref, gate_ref, ls_ref, t)
        qs_all[t] = qs
        cs_all[t] = cs[1]
        ls_rows[t] = ls[1]
        visible = ahead <= kv * TOKENS + t * QUERY_BLOCK
        dq, ds, pr = attend_back(qs, cs[0], ls[0], pk_ref[...], pv_ref[...], visible)
        dq_ref[t] = dq
        dpk_ref[...] += dot(ds, qs, NN)
        dpv_ref[...] += dot(pr, cs[0], NN)
        return carry

    lax.fori_loop(0, BLOCKS // 2, tile, 0)
    rows = TOKENS // 16
    plus, minus = x_first
    plus.wait_recv()
    whole = h_all.at[shifted(cx, -1) * 2 + core]
    part = whole.at[pl.ds(0, rows)]
    x_second = [send(part, part, xdev(1, core))]
    x_over.append(send(whole, whole, xdev(0, 1 - core)))
    minus.wait_recv()
    whole = h_all.at[shifted(cx, 1) * 2 + core]
    part = whole.at[pl.ds(rows, rows)]
    x_second.append(send(part, part, xdev(-1, core)))
    x_over.append(send(whole, whole, xdev(0, 1 - core)))
    for axis, full in arrays:
        across(axis, full, *wide[axis][1])
    lax.fori_loop(BLOCKS // 2, BLOCKS, tile, 0)
    dpk_ref[...] = dpk_ref[...] * (SCALE / POOL_BLOCK)
    dpv_ref[...] = dpv_ref[...] * (1.0 / POOL_BLOCK)
    for axis, full in arrays:
        across(axis, full, *wide[axis][2])
    for copy in x_second:
        copy.wait_recv()
    whole = h_all.at[shifted(cx, 2) * 2 + core]
    x_over.append(send(whole, whole, xdev(0, 1 - core)))
    for axis, full in arrays:
        across(axis, full, *wide[axis][3])
    for copy in last:
        copy.wait_recv()
    for copy in x_over:
        copy.wait_recv()
    send.finish()


GATHER_COPIES = 2 * (2 + 2 + 8 + 8) + 2 + 2 + 4 + 14


def run_gather(k, v, h, q, g, gates, sums, chosen):
    hbm = pl.BlockSpec(memory_space=pltpu.HBM)
    vmem = pl.BlockSpec(memory_space=pltpu.VMEM)
    n_pool = OWNERS * POOLED
    wide_q = GROUP * QUERY_BLOCK
    return pl.pallas_call(
        gather_kernel,
        name="gather",
        out_shape=(
            jax.ShapeDtypeStruct((OWNERS, TOKENS, HEAD_DIM), BF16),
            jax.ShapeDtypeStruct((OWNERS, TOKENS, HEAD_DIM), BF16),
            jax.ShapeDtypeStruct((8, TOKENS // 8, MODEL), BF16),
            jax.ShapeDtypeStruct((BLOCKS, HEAD_DIM, wide_q), F32),
            jax.ShapeDtypeStruct((n_pool, HEAD_DIM), F32),
            jax.ShapeDtypeStruct((n_pool, HEAD_DIM), F32),
            jax.ShapeDtypeStruct((BLOCKS, wide_q, HEAD_DIM), BF16),
            jax.ShapeDtypeStruct((BLOCKS, wide_q, HEAD_DIM), BF16),
            jax.ShapeDtypeStruct((BLOCKS, 1, wide_q), F32),
            jax.ShapeDtypeStruct((SLOTS + POOLED, LISTED), BF16),
            jax.ShapeDtypeStruct((2, LISTED, SLOTS), BF16),
        ),
        in_specs=[hbm] * 8,
        out_specs=(vmem,) * 11,
        scratch_shapes=[
            pltpu.SMEM((BLOCKS, CHOSEN), jnp.int32),
            pltpu.VMEM(q.shape, BF16),
            pltpu.VMEM(g.shape, BF16),
            pltpu.VMEM(gates.shape, F32),
            pltpu.VMEM(sums.shape, F32),
            pltpu.VMEM((SIDE, SIDE, POOLED + 16, HEAD_DIM), BF16),
            pltpu.VMEM((SIDE, SIDE, POOLED, HEAD_DIM), BF16),
            pltpu.VMEM((n_pool, HEAD_DIM), BF16),
            pltpu.VMEM((n_pool, HEAD_DIM), BF16),
            pltpu.SemaphoreType.DMA((GATHER_COPIES,)),
            pltpu.SemaphoreType.DMA((GATHER_COPIES,)),
            pltpu.SemaphoreType.DMA((8,)),
        ],
        compiler_params=pltpu.CompilerParams(
            collective_id=0, has_side_effects=True, vmem_limit_bytes=12 * MIB
        ),
        cost_estimate=pl.CostEstimate(
            flops=40_000_000_000, bytes_accessed=8 * MIB, transcendentals=0
        ),
    )(*(pltpu.with_memory_space_constraint(a, pltpu.HBM) for a in (k, v, h, q, g, gates, sums, chosen)))


class Reduce:
    def __init__(self, send, axis, src, bufs, coords, along):
        self.relay, self.direct, self.comb, self.relay2, self.direct2, self.comb2 = bufs
        self.send, self.axis, self.src = send, axis, src
        self.c1, self.c2 = (coords[0], coords[1]) if axis == 0 else (coords[1], coords[0])
        self.to1 = lambda o: along(axis, o)
        self.to2 = lambda o: along(1 - axis, o)
        self.half = src.shape[2] // 2
        self.rows = (pl.ds(0, self.half), pl.ds(self.half, self.half))

    def bundle(self, o, n):
        c = shifted(self.c1, o)
        rows = self.rows[n]
        return self.src.at[c, :, rows] if self.axis == 0 else self.src.at[:, c, rows]

    def piece(self, o, i, n):
        c = shifted(self.c1, o)
        if self.axis == 0:
            return self.src[c, i, self.rows[n], :].astype(F32)
        return self.src[i, c, self.rows[n], :].astype(F32)

    def part(self, o, n):
        return self.comb.at[n, shifted(self.c2, o)]

    def begin(self):
        s = self.send
        self.r = [
            s(self.bundle(2, 0), self.relay.at[0], self.to1(1)),
            s(self.bundle(2, 1), self.relay.at[1], self.to1(-1)),
        ]
        self.d = [
            s(self.bundle(1, 1), self.direct.at[0], self.to1(1)),
            s(self.bundle(-1, 0), self.direct.at[1], self.to1(-1)),
        ]

    def combine(self):
        self.c = []
        for n, o in enumerate((1, -1)):
            self.r[n].wait_recv()

            def add(i, carry, n=n, o=o):
                self.relay[n, i] = (self.piece(o, i, n) + self.relay[n, i].astype(F32)).astype(BF16)
                return carry

            lax.fori_loop(0, SIDE, add, 0)
            self.c.append(self.send(self.relay.at[n], self.comb.at[n], self.to1(o)))

    def turn(self):
        for copy in self.d + self.c:
            copy.wait_recv()

        def add(i, carry):
            for n in (0, 1):
                self.comb[n, i] = (
                    self.piece(0, i, n)
                    + self.comb[n, i].astype(F32)
                    + self.direct[1 - n, i].astype(F32)
                ).astype(BF16)
            return carry

        lax.fori_loop(0, SIDE, add, 0)
        self.start_second()

    def start_second(self):
        s = self.send
        self.r = [
            s(self.part(2, 0), self.relay2.at[0], self.to2(1)),
            s(self.part(2, 1), self.relay2.at[1], self.to2(-1)),
        ]
        self.d = [
            s(self.part(1, 1), self.direct2.at[0], self.to2(1)),
            s(self.part(-1, 0), self.direct2.at[1], self.to2(-1)),
        ]

    def combine2(self):
        self.c = []
        for n, o in enumerate((1, -1)):
            self.r[n].wait_recv()
            self.relay2[n] = (
                self.comb[n, shifted(self.c2, o)].astype(F32) + self.relay2[n].astype(F32)
            ).astype(BF16)
            self.c.append(self.send(self.relay2.at[n], self.comb2.at[n], self.to2(o)))

    def end(self):
        for copy in self.d + self.c:
            copy.wait_recv()
        return [
            self.comb[n, self.c2].astype(F32)
            + self.comb2[n].astype(F32)
            + self.direct2[1 - n].astype(F32)
            for n in (0, 1)
        ]


class ListedReduce(Reduce):
    def __init__(self, send, axis, src, bufs, coords, along, place_ref, own):
        self.passed, self.far, self.near, *after = bufs
        super().__init__(send, axis, src, (None, None, *after), coords, along)
        self.place_ref, self.own = place_ref, own
        self.steps = HALF_BLOCK * CHOSEN
        self.pooled = self

    def begin(self):
        s = self.send
        every = pl.ds(0, self.src.shape[2])
        self.rows = self.rows + (every,)
        self.r = [
            s(self.bundle(2, 0), self.passed.at[0], self.to1(1)),
            s(self.bundle(2, 1), self.passed.at[1], self.to1(-1)),
        ]
        self.d = [
            s(self.bundle(1, 2), self.near.at[0], self.to1(1)),
            s(self.bundle(-1, 2), self.near.at[1], self.to1(-1)),
        ]

    def combine(self):
        self.c = []
        for n, o in enumerate((1, -1)):
            self.r[n].wait_recv()
            self.c.append(self.send(self.passed.at[n], self.far.at[:, self.rows[n]], self.to1(o)))

    def sources(self, rows):
        mine = self.src[self.c1, :, rows, :] if self.axis == 0 else self.src[:, self.c1, rows, :]
        return [mine, self.near[0, :, rows, :], self.near[1, :, rows, :], self.far[:, rows, :]]

    def turn(self):
        for copy in self.d + self.c:
            copy.wait_recv()
        pooled = sum(x.astype(F32) for x in self.pooled.sources(pl.ds(self.steps, POOLED)))
        pooled = pooled.reshape(SIDE * POOLED, HEAD_DIM)
        pooled = jnp.concatenate([pooled, pooled], axis=1)
        for n in (0, 1):

            def put(i, carry, n=n):
                pieces = []
                for j in (0, 1):
                    first = pl.multiple_of((n * HALF_BLOCK // 2 + 2 * i + j) * CHOSEN, CHOSEN)
                    got = [x.reshape(SIDE * CHOSEN, HEAD_DIM) for x in self.sources(pl.ds(first, CHOSEN))]
                    pieces.append(jnp.concatenate(got, axis=0))
                total = dot(self.place_ref[self.axis], jnp.concatenate(pieces, axis=1), NN)
                total = total + pooled
                for j in (0, 1):
                    rows = pl.ds(pl.multiple_of((2 * i + j) * POOLED, POOLED), POOLED)
                    part = total[:, j * HEAD_DIM : (j + 1) * HEAD_DIM].astype(BF16)
                    self.comb[n, :, rows, :] = part.reshape(SIDE, POOLED, HEAD_DIM)
                return carry

            lax.fori_loop(0, HALF_BLOCK // 4, put, 0, unroll=2)
        self.start_second()

    def end(self):
        at = self.own[1]
        size = HALF_BLOCK // 2 * POOLED
        return [
            part + self.own[0][at + n * size : at + (n + 1) * size, :]
            for n, part in enumerate(super().end())
        ]


def listed_buffers(rows):
    half, size = rows // 2, HALF_BLOCK // 2 * POOLED
    slim = pltpu.VMEM((2, size, HEAD_DIM), BF16)
    return [
        pltpu.VMEM((2, SIDE, half, HEAD_DIM), BF16),
        pltpu.VMEM((SIDE, rows, HEAD_DIM), BF16),
        pltpu.VMEM((2, SIDE, rows, HEAD_DIM), BF16),
        pltpu.VMEM((2, SIDE, size, HEAD_DIM), BF16),
        slim, slim, slim,
    ]


def reduce_buffers(rows, lanes):
    half = rows // 2
    wide = pltpu.VMEM((2, SIDE, half, lanes), BF16)
    slim = pltpu.VMEM((2, half, lanes), BF16)
    return [wide] * 3 + [slim] * 3


REDUCE_BUFS = 6
LISTED_BUFS = 7
GW_COLS = MODEL // OWNERS
PAIR = GROUP // 2 * HEAD_DIM
PAIR_Q = GROUP // 2 * QUERY_BLOCK
UNROLL = 4
HALF_BLOCK = KEY_BLOCK // 2
SETS = CHOSEN * KEY_BLOCK


def scatter_kernel(
    chosen_ref, k_ref, v_ref, h_ref, dqp_ref, dpk_ref, dpv_ref, qs_all, cs_all, ls_rows, pick_ref, place_ref,
    gq_ref, gk_out, gv_out, gw_out,
    kb, vb, ds_held, pr_held, dk_set, dv_set, gqt, dk0, dv0, dk1, dv1, own_k, own_v, gw0, gw1, gw2, gw3, *rest
):
    cut = 4 * LISTED_BUFS
    bufs = [rest[i * LISTED_BUFS : (i + 1) * LISTED_BUFS] for i in range(4)]
    gw_bufs = [rest[cut + i * REDUCE_BUFS : cut + (i + 1) * REDUCE_BUFS] for i in range(4)]
    send_sems, recv_sems = rest[cut + 4 * REDUCE_BUFS :]
    kv, tp, cz, cy, cx, core = place()

    def along(axis, o):
        if axis == 0:
            return (shifted(cz, o) * SIDE + cy, tp)
        return (cz * SIDE + shifted(cy, o), tp)

    peers = [along(axis, o) for axis in (0, 1) for o in (1, -1)]
    greet(peers)
    send = Sender(send_sems, recv_sems)
    gws = (gw0, gw1, gw2, gw3)
    kv_parts = (dk0, dv0, dk1, dv1)
    half_rows = HALF_BLOCK * POOLED
    owns = ((own_k, 0), (own_v, 0), (own_k, half_rows), (own_v, half_rows))
    k0, v0, k1, v1 = [
        ListedReduce(send, axis, src, buf, (cz, cy), along, place_ref, own)
        for axis, src, buf, own in zip((0, 1) * 2, kv_parts, bufs, owns)
    ]
    k1.pooled, v1.pooled = k0, v0
    w0, w1, w2, w3 = [
        Reduce(send, axis, src, buf, (cz, cy), along)
        for axis, src, buf in zip((0, 1) * 2, gws, gw_bufs)
    ]

    ahead = (
        lax.broadcasted_iota(jnp.int32, (KEY_BLOCK, PAIR_Q), 0)
        - lax.broadcasted_iota(jnp.int32, (KEY_BLOCK, PAIR_Q), 1) % QUERY_BLOCK
    )

    def attend(pair):
        across = slice(pair * PAIR_Q, (pair + 1) * PAIR_Q)

        def block(b, carry):
            start_row = kv * TOKENS + b * QUERY_BLOCK
            seen = []
            for c in range(CHOSEN):
                at = chosen_ref[b, c]
                kb[c * KEY_BLOCK : (c + 1) * KEY_BLOCK, :] = k_ref[at]
                vb[c * KEY_BLOCK : (c + 1) * KEY_BLOCK, :] = v_ref[at]
                seen.append(ahead <= start_row - at * KEY_BLOCK)
            dq, ds, pr = attend_back(
                qs_all[b, across, :],
                cs_all[b, across, :],
                ls_rows[b, :, across],
                kb[...],
                vb[...],
                jnp.concatenate(seen, axis=0),
            )
            total = (dqp_ref[b, :, across] + dq) * SCALE
            rows = pl.ds(pl.multiple_of(b * QUERY_BLOCK, QUERY_BLOCK), QUERY_BLOCK)
            for h in range(GROUP // 2):
                part = total[:, h * QUERY_BLOCK : (h + 1) * QUERY_BLOCK]
                at = pair * PAIR + h * HEAD_DIM
                gqt[at : at + HEAD_DIM, rows] = part.astype(BF16)
                gq_ref[rows, at : at + HEAD_DIM] = part.T.astype(BF16)
            if pair == 0:
                ds_held[b] = ds
                pr_held[b] = pr
            else:
                for i in (0, 1):
                    at, rows = 2 * b + i, slice(i * PAIR_Q, (i + 1) * PAIR_Q)
                    spot = (at // SIDE, at % SIDE, slice(0, PAIR_Q))
                    dk0[spot], dk1[spot] = ds[rows, :HEAD_DIM], ds[rows, HEAD_DIM:]
                    dv0[spot], dv1[spot] = pr[rows, :HEAD_DIM], pr[rows, HEAD_DIM:]
            return carry

        return block

    def sets(b, carry):
        here = pl.ds(pl.multiple_of(b * SETS, SETS), SETS)

        def whole(held, low, high):
            at = [((2 * b + i) // SIDE, (2 * b + i) % SIDE, slice(0, PAIR_Q)) for i in (0, 1)]
            parts = [jnp.concatenate([ref[a] for a in at], axis=0) for ref in (low, high)]
            return jnp.concatenate([held[b], *parts], axis=1)

        dk_set[here, :] = dot(whole(ds_held, dk0, dk1), qs_all[b], NN) * SCALE
        dv_set[here, :] = dot(whole(pr_held, dv0, dv1), cs_all[b], NN)
        return carry

    def product(pair):
        def one(j, carry):
            wide = SIDE * GW_COLS
            cols = pl.ds(pl.multiple_of(j * wide, wide), wide)
            part = dot(gqt[pair * PAIR : (pair + 1) * PAIR, :], h_ref[:, cols], NN).astype(BF16)
            for i in range(SIDE):
                piece = part[:, i * GW_COLS : (i + 1) * GW_COLS]
                gws[2 * pair][j, i] = piece[:HEAD_DIM]
                gws[2 * pair + 1][j, i] = piece[HEAD_DIM:]
            return carry

        lax.fori_loop(0, SIDE, one, 0)

    lax.fori_loop(0, BLOCKS, attend(0), 0, unroll=2)
    product(0)
    meet(len(peers))
    w0.begin()
    w1.begin()
    lax.fori_loop(0, BLOCKS // 2, attend(1), 0, unroll=2)
    w0.combine()
    w1.combine()
    lax.fori_loop(BLOCKS // 2, BLOCKS, attend(1), 0, unroll=2)

    product(1)
    w2.begin()
    w3.begin()
    lax.fori_loop(0, BLOCKS, sets, 0, unroll=2)
    w0.turn()
    w1.turn()

    slots = (SIDE, SIDE, CHOSEN, HEAD_DIM)

    def spread(part):
        dk_out, dv_out = kv_parts[2 * part : 2 * part + 2]

        def one(i, carry):
            every = pl.ds(part * HALF_BLOCK + i, LISTED, stride=KEY_BLOCK)
            got = jnp.concatenate([dk_set[every, :], dv_set[every, :]], axis=1).astype(BF16)
            got = dot(pick_ref[...], got, NN)
            rows = pl.ds(pl.multiple_of(i * CHOSEN, CHOSEN), CHOSEN)
            dk_out[:, :, rows, :] = got[:SLOTS, :HEAD_DIM].astype(BF16).reshape(slots)
            dv_out[:, :, rows, :] = got[:SLOTS, HEAD_DIM:].astype(BF16).reshape(slots)
            rows = pl.ds(pl.multiple_of((part * HALF_BLOCK + i) * POOLED, POOLED), POOLED)
            own_k[rows, :] = got[SLOTS:, :HEAD_DIM]
            own_v[rows, :] = got[SLOTS:, HEAD_DIM:]
            return carry

        lax.fori_loop(0, HALF_BLOCK, one, 0, unroll=UNROLL)

    tail = slice(HALF_BLOCK * CHOSEN, HALF_BLOCK * CHOSEN + POOLED)
    pooled = (SIDE, SIDE, POOLED, HEAD_DIM)
    dk0[:, :, tail, :] = dpk_ref[...].astype(BF16).reshape(pooled)
    dv0[:, :, tail, :] = dpv_ref[...].astype(BF16).reshape(pooled)
    spread(0)
    k0.begin()
    v0.begin()
    w2.combine()
    w3.combine()
    w0.combine2()
    w1.combine2()
    spread(1)
    k1.begin()
    v1.begin()
    w2.turn()
    w3.turn()

    def weight(n, w):
        for i, part in enumerate(w.end()):
            at = n * HEAD_DIM + i * HEAD_DIM // 2
            gw_out[:, at : at + HEAD_DIM // 2] = part.T

    def ordered(into, part, r):
        for n, rows in enumerate(r.end()):
            for i in range(HALF_BLOCK // 2):
                at = part * HALF_BLOCK + n * (HALF_BLOCK // 2) + i
                into[pl.ds(at, POOLED, stride=KEY_BLOCK), :] = rows[i * POOLED : (i + 1) * POOLED]

    k0.combine()
    v0.combine()
    w2.combine2()
    w3.combine2()
    k1.combine()
    v1.combine()
    k0.turn()
    v0.turn()
    k1.turn()
    v1.turn()
    weight(0, w0)
    weight(1, w1)
    k0.combine2()
    v0.combine2()
    k1.combine2()
    v1.combine2()
    weight(2, w2)
    weight(3, w3)
    ordered(dk_set, 0, k0)
    ordered(dv_set, 0, v0)
    ordered(dk_set, 1, k1)
    ordered(dv_set, 1, v1)
    gk_out[...] = dk_set[:TOKENS, :].astype(BF16)
    gv_out[...] = dv_set[:TOKENS, :].astype(BF16)
    send.finish()


SCATTER_COPIES = 8 * 12
SCATTER_MIB = 31.2


def run_scatter(chosen, k_all, v_all, h_all, dqp, dpk, dpv, qs, cs, ls, pick, places):
    vmem = pl.BlockSpec(memory_space=pltpu.VMEM)
    smem = pl.BlockSpec(memory_space=pltpu.SMEM)
    first = HALF_BLOCK * CHOSEN + POOLED
    second = HALF_BLOCK * CHOSEN
    outgoing = [pltpu.VMEM((SIDE, SIDE, n, HEAD_DIM), BF16) for n in (first, first, second, second)]
    grad = pltpu.VMEM((SIDE, SIDE, HEAD_DIM, GW_COLS), BF16)
    return pl.pallas_call(
        scatter_kernel,
        name="scatter",
        out_shape=(
            jax.ShapeDtypeStruct((TOKENS, GROUP * HEAD_DIM), BF16),
            jax.ShapeDtypeStruct((TOKENS, HEAD_DIM), BF16),
            jax.ShapeDtypeStruct((TOKENS, HEAD_DIM), BF16),
            jax.ShapeDtypeStruct((GW_COLS, GROUP * HEAD_DIM), F32),
        ),
        in_specs=[smem] + [vmem] * 11,
        out_specs=(vmem,) * 4,
        scratch_shapes=[
            pltpu.VMEM((SETS, HEAD_DIM), BF16),
            pltpu.VMEM((SETS, HEAD_DIM), BF16),
            pltpu.VMEM((BLOCKS, SETS, PAIR_Q), BF16),
            pltpu.VMEM((BLOCKS, SETS, PAIR_Q), BF16),
            pltpu.VMEM((BLOCKS * SETS, HEAD_DIM), F32),
            pltpu.VMEM((BLOCKS * SETS, HEAD_DIM), F32),
            pltpu.VMEM((GROUP * HEAD_DIM, TOKENS), BF16),
            *outgoing,
            pltpu.VMEM((TOKENS, HEAD_DIM), F32),
            pltpu.VMEM((TOKENS, HEAD_DIM), F32),
            grad,
            grad,
            grad,
            grad,
            *(listed_buffers(first) * 2),
            *(listed_buffers(second) * 2),
            *(reduce_buffers(HEAD_DIM, GW_COLS) * 4),
            pltpu.SemaphoreType.DMA((SCATTER_COPIES,)),
            pltpu.SemaphoreType.DMA((SCATTER_COPIES,)),
        ],
        compiler_params=pltpu.CompilerParams(
            collective_id=1, has_side_effects=True, vmem_limit_bytes=int(SCATTER_MIB * MIB)
        ),
    )(chosen, k_all, v_all, h_all, dqp, dpk, dpv, qs, cs, ls, pick, places)


def finish_kernel(*refs):
    copies = [pltpu.make_async_copy(refs[i], refs[4 + i], refs[8].at[i]) for i in range(4)]
    for copy in copies:
        copy.start()
    for copy in copies:
        copy.wait()


def run_finish(*outs):
    return pl.pallas_call(
        finish_kernel,
        name="finish",
        out_shape=tuple(jax.ShapeDtypeStruct(a.shape, a.dtype) for a in outs),
        in_specs=[pl.BlockSpec(memory_space=pltpu.VMEM)] * 4,
        out_specs=(pl.BlockSpec(memory_space=pltpu.HBM),) * 4,
        scratch_shapes=[pltpu.SemaphoreType.DMA((4,))],
        compiler_params=pltpu.CompilerParams(vmem_limit_bytes=8 * MIB),
    )(*outs)


def body(hidden_rows, queries, key_rows, value_rows, branch_gates, log_sums, chosen, out_grad):
    lists = chosen.reshape(BLOCKS, CHOSEN)
    k_all, v_all, h_all, *more = run_gather(
        key_rows, value_rows, hidden_rows, queries, out_grad, branch_gates, log_sums, lists
    )
    by_block = (SEQ // KEY_BLOCK, KEY_BLOCK, HEAD_DIM)
    outs = run_scatter(
        lists,
        k_all.reshape(by_block),
        v_all.reshape(by_block),
        h_all.reshape(TOKENS, MODEL),
        *more,
    )
    return run_finish(*outs)


def solution(mesh):
    placed = (
        P(("kv", "tp"), None),
        P("kv", "tp"),
        P("kv", "tp"),
        P("kv", "tp"),
        P(None, "tp", "kv"),
        P(None, "tp", "kv"),
        P("tp", "kv", None),
        P("kv", "tp"),
    )
    return jax.shard_map(
        body,
        mesh=mesh,
        in_specs=placed,
        out_specs=(P("kv", "tp"), P("kv", "tp"), P("kv", "tp"), P("kv", "tp")),
        check_vma=False,
    )
```

```python
import jax
import jax.numpy as jnp
from jax import lax
from jax.experimental import pallas as pl
from jax.experimental.pallas import tpu as pltpu
from jax.sharding import PartitionSpec as P

HEADS = 32
KV_HEADS = 8
HEAD_DIM = 128
QUERY_BLOCK = 128
KEY_BLOCK = 32
POOL_BLOCK = 32
CHOSEN = 16
GROUP = HEADS // KV_HEADS
SIDE = 4
OWNERS = SIDE * SIDE
TOKENS = 1024
BLOCKS = TOKENS // QUERY_BLOCK
POOLED = TOKENS // POOL_BLOCK
SEQ = TOKENS * OWNERS
LISTED = BLOCKS * CHOSEN
SLOTS = OWNERS * CHOSEN
MODEL = 4096
SCALE = HEAD_DIM ** (-0.5)
LOG2E = 1.4426950408889634
MIB = 1 << 20
MESH = pl.DeviceIdType.MESH
F32 = jnp.float32
BF16 = jnp.bfloat16

NT = (((1,), (1,)), ((), ()))
NN = (((1,), (0,)), ((), ()))


def dot(a, b, dims):
    return lax.dot_general(a, b, dims, preferred_element_type=F32)


class Sender:
    def __init__(self, send_sems, recv_sems):
        self.send_sems, self.recv_sems, self.at, self.sent = send_sems, recv_sems, 0, []

    def __call__(self, src, dst, dev):
        copy = pltpu.make_async_remote_copy(
            src_ref=src,
            dst_ref=dst,
            send_sem=self.send_sems.at[self.at],
            recv_sem=self.recv_sems.at[self.at],
            device_id=dev,
            device_id_type=MESH,
        )
        self.at += 1
        copy.start()
        self.sent.append(copy)
        return copy

    def finish(self):
        for copy in self.sent:
            copy.wait_send()


def place():
    kv, tp = lax.axis_index("kv"), lax.axis_index("tp")
    return kv, tp, kv // SIDE, kv % SIDE, tp // 2, tp % 2


def shifted(c, o):
    return (c + (o + SIDE)) % SIDE


def greet(devices):
    for dev in devices:
        pl.semaphore_signal(
            pltpu.get_barrier_semaphore(), inc=1, device_id=dev, device_id_type=MESH
        )


def meet(count):
    pl.semaphore_wait(pltpu.get_barrier_semaphore(), count)


def tile_operands(q_ref, g_ref, gate_ref, ls_ref, t):
    rows = pl.ds(pl.multiple_of(t * QUERY_BLOCK, QUERY_BLOCK), QUERY_BLOCK)
    gates = jnp.concatenate([gate_ref[0, :, rows], gate_ref[1, :, rows]], axis=0).T
    qs, cs, ls = [], ([], []), ([], [])
    for h in range(GROUP):
        cols = slice(h * HEAD_DIM, (h + 1) * HEAD_DIM)
        qs.append(q_ref[rows, cols])
        grad = g_ref[rows, cols].astype(F32)
        for branch in (0, 1):
            at = branch * GROUP + h
            cs[branch].append((gates[:, at : at + 1] * grad).astype(BF16))
            ls[branch].append(ls_ref[branch, h : h + 1, rows])
    return (
        jnp.concatenate(qs, axis=0),
        [jnp.concatenate(c, axis=0) for c in cs],
        [jnp.concatenate(x, axis=1) * LOG2E for x in ls],
    )


def attend_back(qs, cs, log_sum, keys, values, visible):
    scores = dot(keys, qs, NT) * (SCALE * LOG2E)
    p = jnp.where(visible, jnp.exp2(scores - log_sum), 0.0)
    pr = p.astype(BF16)
    dp = dot(values, cs, NT)
    delta = jnp.sum(p * dp, axis=0, keepdims=True)
    ds = (p * (dp - delta)).astype(BF16)
    return dot(keys.T, ds, NN), ds, pr


def gather_kernel(
    k_ref, v_ref, h_ref, q_hbm, g_hbm, gate_hbm, ls_hbm, chosen_hbm,
    k_all, v_all, h_all, dq_ref, dpk_ref, dpv_ref, qs_all, cs_all, ls_rows, pick_ref, place_ref,
    chosen_ref, q_ref, g_ref, gate_ref, ls_ref, pool_k, pool_v, pk_ref, pv_ref,
    send_sems, recv_sems, local_sems,
):
    kv, tp, cz, cy, cx, core = place()
    half = TOKENS // 2

    def device(oz, oy):
        return (shifted(cz, oz) * SIDE + shifted(cy, oy), tp)

    def along(axis, o):
        return device(o, 0) if axis == 0 else device(0, o)

    def owner(axis, o1, o2):
        a, b = (o1, o2) if axis == 0 else (o2, o1)
        return shifted(cz, a) * SIDE + shifted(cy, b)

    def xdev(o, c):
        return (kv, shifted(cx, o) * 2 + c)

    peers = [along(axis, s) for axis in (0, 1) for s in (1, -1)] + [
        xdev(1, core), xdev(-1, core), xdev(0, 1 - core)
    ]
    greet(peers)
    local = [
        pltpu.make_async_copy(src, dst, local_sems.at[i])
        for i, (src, dst) in enumerate(
            (
                (k_ref, k_all.at[kv]),
                (v_ref, v_all.at[kv]),
                (h_ref, h_all.at[tp]),
                (chosen_hbm, chosen_ref),
                (gate_hbm, gate_ref),
                (ls_hbm, ls_ref),
                (q_hbm, q_ref),
                (g_hbm, g_ref),
            )
        )
    ]
    for copy in local:
        copy.start()

    blk = lax.broadcasted_iota(jnp.int32, (POOLED, TOKENS), 0)
    row = lax.broadcasted_iota(jnp.int32, (POOLED, TOKENS), 1)
    mean = jnp.where(row // POOL_BLOCK == blk, 1.0 / POOL_BLOCK, 0.0).astype(BF16)
    local[0].wait()
    pool_k[cz, cy, :POOLED] = dot(mean, k_all[kv], NN).astype(BF16)
    local[1].wait()
    pool_v[cz, cy] = dot(mean, v_all[kv], NN).astype(BF16)

    local[3].wait()
    lane = lax.broadcasted_iota(jnp.int32, (1, LISTED), 1)
    listed = jnp.zeros((1, LISTED), jnp.int32)
    for b in range(BLOCKS):
        for c in range(CHOSEN):
            listed = jnp.where(lane == b * CHOSEN + c, chosen_ref[b, c], listed)
    row = lax.broadcasted_iota(jnp.int32, (16, LISTED), 0)
    both = jnp.where(row == 0, listed // POOLED, jnp.where(row == 1, listed % POOLED, 0))
    pool_k[cz, cy, POOLED:] = both.astype(F32).astype(BF16)
    meet(len(peers))

    send = Sender(send_sems, recv_sems)
    first, wide, small = {}, {}, {}
    pools = ((0, pool_k), (1, pool_v))

    def pool_chunk(axis, ref, o):
        return ref.at[shifted(cz, o), cy] if axis == 0 else ref.at[cz, shifted(cy, o)]

    def pool_row(axis, ref, o, part=pl.ds(0, SIDE)):
        return ref.at[part, shifted(cy, o)] if axis == 0 else ref.at[shifted(cz, o), part]

    for axis, ref in pools:
        here = pool_chunk(axis, ref, 0)
        small[axis] = [send(here, here, along(axis, s)) for s in (1, -1)]
    arrays = ((0, k_all), (1, v_all))
    for axis, full in arrays:
        here = full.at[kv]
        first[axis] = [send(here, here, along(axis, s)) for s in (1, -1)]
    local[2].wait()
    here = h_all.at[tp]
    x_first = [send(here, here, xdev(s, core)) for s in (1, -1)]
    x_over = [send(here, here, xdev(0, 1 - core))]
    for axis, ref in pools:
        for copy in small[axis]:
            copy.wait_recv()
        passed = pool_chunk(axis, ref, -1)
        small[axis] = [send(passed, passed, along(axis, 1))]
    for axis, full in arrays:
        here = full.at[kv]
        wide[axis] = [(0, [send(here, here, along(1 - axis, s)) for s in (1, -1)])]
    for axis, ref in pools:
        small[axis][0].wait_recv()
        row = pool_row(axis, ref, 0)
        small[axis] = [send(row, row, along(1 - axis, s)) for s in (1, -1)]

    second = {}
    for axis, full in arrays:
        plus, minus = first[axis]
        plus.wait_recv()
        part = full.at[owner(axis, -1, 0), pl.ds(0, half)]
        fwd = send(part, part, along(axis, 1))
        whole = full.at[owner(axis, -1, 0)]
        wide[axis].append((-1, [send(whole, whole, along(1 - axis, s)) for s in (1, -1)]))
        minus.wait_recv()
        part = full.at[owner(axis, 1, 0), pl.ds(half, half)]
        bwd = send(part, part, along(axis, -1))
        second[axis] = (fwd, bwd)
    for axis, ref in pools:
        plus, minus = small[axis]
        plus.wait_recv()
        part = pool_row(axis, ref, -1, pl.ds(0, 2))
        minus_part = pool_row(axis, ref, 1, pl.ds(2, 2))
        fwd = send(part, part, along(1 - axis, 1))
        minus.wait_recv()
        small[axis] = [fwd, send(minus_part, minus_part, along(1 - axis, -1))]
    for axis, full in arrays:
        whole = full.at[owner(axis, 1, 0)]
        wide[axis].append((1, [send(whole, whole, along(1 - axis, s)) for s in (1, -1)]))

    last = []

    def across(axis, full, o, pair):
        plus, minus = pair
        plus.wait_recv()
        part = full.at[owner(axis, o, -1), pl.ds(0, half)]
        last.append(send(part, part, along(1 - axis, 1)))
        minus.wait_recv()
        part = full.at[owner(axis, o, 1), pl.ds(half, half)]
        last.append(send(part, part, along(1 - axis, -1)))

    for axis, full in arrays:
        across(axis, full, *wide[axis][0])
    for axis, full in arrays:
        for copy in second[axis]:
            copy.wait_recv()
        whole = full.at[owner(axis, 2, 0)]
        wide[axis].append((2, [send(whole, whole, along(1 - axis, s)) for s in (1, -1)]))

    for copy in local[4:]:
        copy.wait()
    for axis, ref in pools:
        for copy in small[axis]:
            copy.wait_recv()
    pk_ref[...] = pool_k[:, :, :POOLED].reshape(OWNERS * POOLED, HEAD_DIM)
    pv_ref[...] = pool_v[...].reshape(OWNERS * POOLED, HEAD_DIM)
    dpk_ref[...] = jnp.zeros_like(dpk_ref)
    dpv_ref[...] = jnp.zeros_like(dpv_ref)

    def listing(i):
        both = pool_k[i // SIDE, i % SIDE, POOLED:].astype(F32)
        owners, numbers, column = both[0:1, :], both[1:2, :], both.T[:, 0:1]
        one = lax.broadcasted_iota(jnp.int32, (LISTED, LISTED), 0)
        two = lax.broadcasted_iota(jnp.int32, (LISTED, LISTED), 1)
        same = jnp.where(column == owners, 1.0, 0.0)
        rank = jnp.sum(jnp.where(one < two, same, 0.0), axis=0, keepdims=True)
        return owners, numbers, rank

    def grid(rows, f):
        return f(lax.broadcasted_iota(jnp.int32, (rows, LISTED), 0)).astype(F32)

    def ones(seen):
        return jnp.where(seen, 1.0, 0.0)

    owners, numbers, rank = listing(kv)
    kv_f = kv.astype(F32)
    at, nth = grid(SLOTS, lambda i: i // CHOSEN), grid(SLOTS, lambda i: i % CHOSEN)
    own = jnp.where(owners == kv_f, -1.0, owners)
    pick_ref[:SLOTS] = (ones(own == at) * ones(rank == nth)).astype(BF16)
    at = grid(POOLED, lambda i: i)
    pick_ref[SLOTS:] = (ones(owners == kv_f) * ones(numbers == at)).astype(BF16)

    for axis in (0, 1):
        def owner_id(i, axis=axis):
            return cz * SIDE + i if axis == 0 else i * SIDE + cy

        for pair in (0, 1):
            total = None
            for n in (0, 1):
                who = owner(axis, (0, -1, 1, 2)[2 * pair + n], 0)
                owners, numbers, rank = listing(who)
                at = grid(LISTED, lambda i: owner_id(i // POOLED))
                nth = grid(LISTED, lambda i: i % POOLED)
                blocks = ones(owners == at) * ones(numbers == nth)
                at = grid(LISTED, lambda i: owner_id((i % 64) // CHOSEN))
                nth = grid(LISTED, lambda i, n=n: jnp.where(i // 64 == n, i % CHOSEN, -1))
                own = jnp.where(owners == who.astype(F32), -1.0, owners)
                slots = ones(own == at) * ones(rank == nth)
                part = dot(blocks.astype(BF16), slots.astype(BF16), NT)
                total = part if total is None else total + part
            place_ref[axis, :, pair * LISTED : (pair + 1) * LISTED] = total.astype(BF16)

    n_pool = OWNERS * POOLED
    wide_q = GROUP * QUERY_BLOCK
    pool_end = lax.broadcasted_iota(jnp.int32, (n_pool, wide_q), 0) * POOL_BLOCK + POOL_BLOCK - 1
    lane = lax.broadcasted_iota(jnp.int32, (n_pool, wide_q), 1) % QUERY_BLOCK
    ahead = pool_end - lane

    def tile(t, carry):
        qs, cs, ls = tile_operands(q_ref, g_ref, gate_ref, ls_ref, t)
        qs_all[t] = qs
        cs_all[t] = cs[1]
        ls_rows[t] = ls[1]
        visible = ahead <= kv * TOKENS + t * QUERY_BLOCK
        dq, ds, pr = attend_back(qs, cs[0], ls[0], pk_ref[...], pv_ref[...], visible)
        dq_ref[t] = dq
        dpk_ref[...] += dot(ds, qs, NN)
        dpv_ref[...] += dot(pr, cs[0], NN)
        return carry

    lax.fori_loop(0, BLOCKS // 2, tile, 0)
    rows = TOKENS // 16
    plus, minus = x_first
    plus.wait_recv()
    whole = h_all.at[shifted(cx, -1) * 2 + core]
    part = whole.at[pl.ds(0, rows)]
    x_second = [send(part, part, xdev(1, core))]
    x_over.append(send(whole, whole, xdev(0, 1 - core)))
    minus.wait_recv()
    whole = h_all.at[shifted(cx, 1) * 2 + core]
    part = whole.at[pl.ds(rows, rows)]
    x_second.append(send(part, part, xdev(-1, core)))
    x_over.append(send(whole, whole, xdev(0, 1 - core)))
    for axis, full in arrays:
        across(axis, full, *wide[axis][1])
    lax.fori_loop(BLOCKS // 2, BLOCKS, tile, 0)
    dpk_ref[...] = dpk_ref[...] * (SCALE / POOL_BLOCK)
    dpv_ref[...] = dpv_ref[...] * (1.0 / POOL_BLOCK)
    for axis, full in arrays:
        across(axis, full, *wide[axis][2])
    for copy in x_second:
        copy.wait_recv()
    whole = h_all.at[shifted(cx, 2) * 2 + core]
    x_over.append(send(whole, whole, xdev(0, 1 - core)))
    for axis, full in arrays:
        across(axis, full, *wide[axis][3])
    for copy in last:
        copy.wait_recv()
    for copy in x_over:
        copy.wait_recv()
    send.finish()


GATHER_COPIES = 2 * (2 + 2 + 8 + 8) + 2 + 2 + 4 + 14


def run_gather(k, v, h, q, g, gates, sums, chosen):
    hbm = pl.BlockSpec(memory_space=pltpu.HBM)
    vmem = pl.BlockSpec(memory_space=pltpu.VMEM)
    n_pool = OWNERS * POOLED
    wide_q = GROUP * QUERY_BLOCK
    return pl.pallas_call(
        gather_kernel,
        name="gather",
        out_shape=(
            jax.ShapeDtypeStruct((OWNERS, TOKENS, HEAD_DIM), BF16),
            jax.ShapeDtypeStruct((OWNERS, TOKENS, HEAD_DIM), BF16),
            jax.ShapeDtypeStruct((8, TOKENS // 8, MODEL), BF16),
            jax.ShapeDtypeStruct((BLOCKS, HEAD_DIM, wide_q), F32),
            jax.ShapeDtypeStruct((n_pool, HEAD_DIM), F32),
            jax.ShapeDtypeStruct((n_pool, HEAD_DIM), F32),
            jax.ShapeDtypeStruct((BLOCKS, wide_q, HEAD_DIM), BF16),
            jax.ShapeDtypeStruct((BLOCKS, wide_q, HEAD_DIM), BF16),
            jax.ShapeDtypeStruct((BLOCKS, 1, wide_q), F32),
            jax.ShapeDtypeStruct((SLOTS + POOLED, LISTED), BF16),
            jax.ShapeDtypeStruct((2, LISTED, SLOTS), BF16),
        ),
        in_specs=[hbm] * 8,
        out_specs=(vmem,) * 11,
        scratch_shapes=[
            pltpu.SMEM((BLOCKS, CHOSEN), jnp.int32),
            pltpu.VMEM(q.shape, BF16),
            pltpu.VMEM(g.shape, BF16),
            pltpu.VMEM(gates.shape, F32),
            pltpu.VMEM(sums.shape, F32),
            pltpu.VMEM((SIDE, SIDE, POOLED + 16, HEAD_DIM), BF16),
            pltpu.VMEM((SIDE, SIDE, POOLED, HEAD_DIM), BF16),
            pltpu.VMEM((n_pool, HEAD_DIM), BF16),
            pltpu.VMEM((n_pool, HEAD_DIM), BF16),
            pltpu.SemaphoreType.DMA((GATHER_COPIES,)),
            pltpu.SemaphoreType.DMA((GATHER_COPIES,)),
            pltpu.SemaphoreType.DMA((8,)),
        ],
        compiler_params=pltpu.CompilerParams(
            collective_id=0, has_side_effects=True, vmem_limit_bytes=12 * MIB
        ),
        cost_estimate=pl.CostEstimate(
            flops=40_000_000_000, bytes_accessed=8 * MIB, transcendentals=0
        ),
    )(*(pltpu.with_memory_space_constraint(a, pltpu.HBM) for a in (k, v, h, q, g, gates, sums, chosen)))


class Reduce:
    def __init__(self, send, axis, src, bufs, coords, along):
        self.relay, self.direct, self.comb, self.relay2, self.direct2, self.comb2 = bufs
        self.send, self.axis, self.src = send, axis, src
        self.c1, self.c2 = (coords[0], coords[1]) if axis == 0 else (coords[1], coords[0])
        self.to1 = lambda o: along(axis, o)
        self.to2 = lambda o: along(1 - axis, o)
        self.half = src.shape[2] // 2
        self.rows = (pl.ds(0, self.half), pl.ds(self.half, self.half))

    def bundle(self, o, n):
        c = shifted(self.c1, o)
        rows = self.rows[n]
        return self.src.at[c, :, rows] if self.axis == 0 else self.src.at[:, c, rows]

    def piece(self, o, i, n):
        c = shifted(self.c1, o)
        if self.axis == 0:
            return self.src[c, i, self.rows[n], :].astype(F32)
        return self.src[i, c, self.rows[n], :].astype(F32)

    def part(self, o, n):
        return self.comb.at[n, shifted(self.c2, o)]

    def begin(self):
        s = self.send
        self.r = [
            s(self.bundle(2, 0), self.relay.at[0], self.to1(1)),
            s(self.bundle(2, 1), self.relay.at[1], self.to1(-1)),
        ]
        self.d = [
            s(self.bundle(1, 1), self.direct.at[0], self.to1(1)),
            s(self.bundle(-1, 0), self.direct.at[1], self.to1(-1)),
        ]

    def combine(self):
        self.c = []
        for n, o in enumerate((1, -1)):
            self.r[n].wait_recv()

            def add(i, carry, n=n, o=o):
                self.relay[n, i] = (self.piece(o, i, n) + self.relay[n, i].astype(F32)).astype(BF16)
                return carry

            lax.fori_loop(0, SIDE, add, 0)
            self.c.append(self.send(self.relay.at[n], self.comb.at[n], self.to1(o)))

    def turn(self):
        for copy in self.d + self.c:
            copy.wait_recv()

        def add(i, carry):
            for n in (0, 1):
                self.comb[n, i] = (
                    self.piece(0, i, n)
                    + self.comb[n, i].astype(F32)
                    + self.direct[1 - n, i].astype(F32)
                ).astype(BF16)
            return carry

        lax.fori_loop(0, SIDE, add, 0)
        self.start_second()

    def start_second(self):
        s = self.send
        self.r = [
            s(self.part(2, 0), self.relay2.at[0], self.to2(1)),
            s(self.part(2, 1), self.relay2.at[1], self.to2(-1)),
        ]
        self.d = [
            s(self.part(1, 1), self.direct2.at[0], self.to2(1)),
            s(self.part(-1, 0), self.direct2.at[1], self.to2(-1)),
        ]

    def combine2(self):
        self.c = []
        for n, o in enumerate((1, -1)):
            self.r[n].wait_recv()
            self.relay2[n] = (
                self.comb[n, shifted(self.c2, o)].astype(F32) + self.relay2[n].astype(F32)
            ).astype(BF16)
            self.c.append(self.send(self.relay2.at[n], self.comb2.at[n], self.to2(o)))

    def end(self):
        for copy in self.d + self.c:
            copy.wait_recv()
        return [
            self.comb[n, self.c2].astype(F32)
            + self.comb2[n].astype(F32)
            + self.direct2[1 - n].astype(F32)
            for n in (0, 1)
        ]


class ListedReduce(Reduce):
    def __init__(self, send, axis, src, bufs, coords, along, place_ref, own):
        self.passed, self.far, self.near, *after = bufs
        super().__init__(send, axis, src, (None, None, *after), coords, along)
        self.place_ref, self.own = place_ref, own
        self.steps = HALF_BLOCK * CHOSEN
        self.pooled = self

    def begin(self):
        s = self.send
        every = pl.ds(0, self.src.shape[2])
        self.rows = self.rows + (every,)
        self.r = [
            s(self.bundle(2, 0), self.passed.at[0], self.to1(1)),
            s(self.bundle(2, 1), self.passed.at[1], self.to1(-1)),
        ]
        self.d = [
            s(self.bundle(1, 2), self.near.at[0], self.to1(1)),
            s(self.bundle(-1, 2), self.near.at[1], self.to1(-1)),
        ]

    def combine(self):
        self.c = []
        for n, o in enumerate((1, -1)):
            self.r[n].wait_recv()
            self.c.append(self.send(self.passed.at[n], self.far.at[:, self.rows[n]], self.to1(o)))

    def sources(self, rows):
        mine = self.src[self.c1, :, rows, :] if self.axis == 0 else self.src[:, self.c1, rows, :]
        return [mine, self.near[0, :, rows, :], self.near[1, :, rows, :], self.far[:, rows, :]]

    def turn(self):
        for copy in self.d + self.c:
            copy.wait_recv()
        pooled = sum(x.astype(F32) for x in self.pooled.sources(pl.ds(self.steps, POOLED)))
        pooled = pooled.reshape(SIDE * POOLED, HEAD_DIM)
        pooled = jnp.concatenate([pooled, pooled], axis=1)
        for n in (0, 1):

            def put(i, carry, n=n):
                pieces = []
                for j in (0, 1):
                    first = pl.multiple_of((n * HALF_BLOCK // 2 + 2 * i + j) * CHOSEN, CHOSEN)
                    got = [x.reshape(SIDE * CHOSEN, HEAD_DIM) for x in self.sources(pl.ds(first, CHOSEN))]
                    pieces.append(jnp.concatenate(got, axis=0))
                total = dot(self.place_ref[self.axis], jnp.concatenate(pieces, axis=1), NN)
                total = total + pooled
                for j in (0, 1):
                    rows = pl.ds(pl.multiple_of((2 * i + j) * POOLED, POOLED), POOLED)
                    part = total[:, j * HEAD_DIM : (j + 1) * HEAD_DIM].astype(BF16)
                    self.comb[n, :, rows, :] = part.reshape(SIDE, POOLED, HEAD_DIM)
                return carry

            lax.fori_loop(0, HALF_BLOCK // 4, put, 0, unroll=2)
        self.start_second()

    def end(self):
        at = self.own[1]
        size = HALF_BLOCK // 2 * POOLED
        return [
            part + self.own[0][at + n * size : at + (n + 1) * size, :]
            for n, part in enumerate(super().end())
        ]


def listed_buffers(rows):
    half, size = rows // 2, HALF_BLOCK // 2 * POOLED
    slim = pltpu.VMEM((2, size, HEAD_DIM), BF16)
    return [
        pltpu.VMEM((2, SIDE, half, HEAD_DIM), BF16),
        pltpu.VMEM((SIDE, rows, HEAD_DIM), BF16),
        pltpu.VMEM((2, SIDE, rows, HEAD_DIM), BF16),
        pltpu.VMEM((2, SIDE, size, HEAD_DIM), BF16),
        slim, slim, slim,
    ]


def reduce_buffers(rows, lanes):
    half = rows // 2
    wide = pltpu.VMEM((2, SIDE, half, lanes), BF16)
    slim = pltpu.VMEM((2, half, lanes), BF16)
    return [wide] * 3 + [slim] * 3


REDUCE_BUFS = 6
LISTED_BUFS = 7
GW_COLS = MODEL // OWNERS
PAIR = GROUP // 2 * HEAD_DIM
PAIR_Q = GROUP // 2 * QUERY_BLOCK
UNROLL = 4
HALF_BLOCK = KEY_BLOCK // 2
SETS = CHOSEN * KEY_BLOCK


def scatter_kernel(
    chosen_ref, k_ref, v_ref, h_ref, dqp_ref, dpk_ref, dpv_ref, qs_all, cs_all, ls_rows, pick_ref, place_ref,
    gq_ref, gk_out, gv_out, gw_out,
    kb, vb, ds_held, pr_held, dk_set, dv_set, gqt, dk0, dv0, dk1, dv1, own_k, own_v, gw0, gw1, gw2, gw3, *rest
):
    cut = 4 * LISTED_BUFS
    bufs = [rest[i * LISTED_BUFS : (i + 1) * LISTED_BUFS] for i in range(4)]
    gw_bufs = [rest[cut + i * REDUCE_BUFS : cut + (i + 1) * REDUCE_BUFS] for i in range(4)]
    send_sems, recv_sems = rest[cut + 4 * REDUCE_BUFS :]
    kv, tp, cz, cy, cx, core = place()

    def along(axis, o):
        if axis == 0:
            return (shifted(cz, o) * SIDE + cy, tp)
        return (cz * SIDE + shifted(cy, o), tp)

    peers = [along(axis, o) for axis in (0, 1) for o in (1, -1)]
    greet(peers)
    send = Sender(send_sems, recv_sems)
    gws = (gw0, gw1, gw2, gw3)
    kv_parts = (dk0, dv0, dk1, dv1)
    half_rows = HALF_BLOCK * POOLED
    owns = ((own_k, 0), (own_v, 0), (own_k, half_rows), (own_v, half_rows))
    k0, v0, k1, v1 = [
        ListedReduce(send, axis, src, buf, (cz, cy), along, place_ref, own)
        for axis, src, buf, own in zip((0, 1) * 2, kv_parts, bufs, owns)
    ]
    k1.pooled, v1.pooled = k0, v0
    w0, w1, w2, w3 = [
        Reduce(send, axis, src, buf, (cz, cy), along)
        for axis, src, buf in zip((0, 1) * 2, gws, gw_bufs)
    ]

    ahead = (
        lax.broadcasted_iota(jnp.int32, (KEY_BLOCK, PAIR_Q), 0)
        - lax.broadcasted_iota(jnp.int32, (KEY_BLOCK, PAIR_Q), 1) % QUERY_BLOCK
    )

    def attend(pair):
        across = slice(pair * PAIR_Q, (pair + 1) * PAIR_Q)

        def block(b, carry):
            start_row = kv * TOKENS + b * QUERY_BLOCK
            seen = []
            for c in range(CHOSEN):
                at = chosen_ref[b, c]
                kb[c * KEY_BLOCK : (c + 1) * KEY_BLOCK, :] = k_ref[at]
                vb[c * KEY_BLOCK : (c + 1) * KEY_BLOCK, :] = v_ref[at]
                seen.append(ahead <= start_row - at * KEY_BLOCK)
            dq, ds, pr = attend_back(
                qs_all[b, across, :],
                cs_all[b, across, :],
                ls_rows[b, :, across],
                kb[...],
                vb[...],
                jnp.concatenate(seen, axis=0),
            )
            total = (dqp_ref[b, :, across] + dq) * SCALE
            rows = pl.ds(pl.multiple_of(b * QUERY_BLOCK, QUERY_BLOCK), QUERY_BLOCK)
            for h in range(GROUP // 2):
                part = total[:, h * QUERY_BLOCK : (h + 1) * QUERY_BLOCK]
                at = pair * PAIR + h * HEAD_DIM
                gqt[at : at + HEAD_DIM, rows] = part.astype(BF16)
                gq_ref[rows, at : at + HEAD_DIM] = part.T.astype(BF16)
            if pair == 0:
                ds_held[b] = ds
                pr_held[b] = pr
            else:
                for i in (0, 1):
                    at, rows = 2 * b + i, slice(i * PAIR_Q, (i + 1) * PAIR_Q)
                    spot = (at // SIDE, at % SIDE, slice(0, PAIR_Q))
                    dk0[spot], dk1[spot] = ds[rows, :HEAD_DIM], ds[rows, HEAD_DIM:]
                    dv0[spot], dv1[spot] = pr[rows, :HEAD_DIM], pr[rows, HEAD_DIM:]
            return carry

        return block

    def sets(b, carry):
        here = pl.ds(pl.multiple_of(b * SETS, SETS), SETS)

        def whole(held, low, high):
            at = [((2 * b + i) // SIDE, (2 * b + i) % SIDE, slice(0, PAIR_Q)) for i in (0, 1)]
            parts = [jnp.concatenate([ref[a] for a in at], axis=0) for ref in (low, high)]
            return jnp.concatenate([held[b], *parts], axis=1)

        dk_set[here, :] = dot(whole(ds_held, dk0, dk1), qs_all[b], NN) * SCALE
        dv_set[here, :] = dot(whole(pr_held, dv0, dv1), cs_all[b], NN)
        return carry

    def product(pair):
        def one(j, carry):
            wide = SIDE * GW_COLS
            cols = pl.ds(pl.multiple_of(j * wide, wide), wide)
            part = dot(gqt[pair * PAIR : (pair + 1) * PAIR, :], h_ref[:, cols], NN).astype(BF16)
            for i in range(SIDE):
                piece = part[:, i * GW_COLS : (i + 1) * GW_COLS]
                gws[2 * pair][j, i] = piece[:HEAD_DIM]
                gws[2 * pair + 1][j, i] = piece[HEAD_DIM:]
            return carry

        lax.fori_loop(0, SIDE, one, 0)

    lax.fori_loop(0, BLOCKS, attend(0), 0, unroll=2)
    product(0)
    meet(len(peers))
    w0.begin()
    w1.begin()
    lax.fori_loop(0, BLOCKS // 2, attend(1), 0, unroll=2)
    w0.combine()
    w1.combine()
    lax.fori_loop(BLOCKS // 2, BLOCKS, attend(1), 0, unroll=2)

    product(1)
    w2.begin()
    w3.begin()
    lax.fori_loop(0, BLOCKS, sets, 0, unroll=2)
    w0.turn()
    w1.turn()

    slots = (SIDE, SIDE, CHOSEN, HEAD_DIM)

    def spread(part):
        dk_out, dv_out = kv_parts[2 * part : 2 * part + 2]

        def one(i, carry):
            every = pl.ds(part * HALF_BLOCK + i, LISTED, stride=KEY_BLOCK)
            got = jnp.concatenate([dk_set[every, :], dv_set[every, :]], axis=1).astype(BF16)
            got = dot(pick_ref[...], got, NN)
            rows = pl.ds(pl.multiple_of(i * CHOSEN, CHOSEN), CHOSEN)
            dk_out[:, :, rows, :] = got[:SLOTS, :HEAD_DIM].astype(BF16).reshape(slots)
            dv_out[:, :, rows, :] = got[:SLOTS, HEAD_DIM:].astype(BF16).reshape(slots)
            rows = pl.ds(pl.multiple_of((part * HALF_BLOCK + i) * POOLED, POOLED), POOLED)
            own_k[rows, :] = got[SLOTS:, :HEAD_DIM]
            own_v[rows, :] = got[SLOTS:, HEAD_DIM:]
            return carry

        lax.fori_loop(0, HALF_BLOCK, one, 0, unroll=UNROLL)

    tail = slice(HALF_BLOCK * CHOSEN, HALF_BLOCK * CHOSEN + POOLED)
    pooled = (SIDE, SIDE, POOLED, HEAD_DIM)
    dk0[:, :, tail, :] = dpk_ref[...].astype(BF16).reshape(pooled)
    dv0[:, :, tail, :] = dpv_ref[...].astype(BF16).reshape(pooled)
    spread(0)
    k0.begin()
    v0.begin()
    w2.combine()
    w3.combine()
    w0.combine2()
    w1.combine2()
    spread(1)
    k1.begin()
    v1.begin()
    w2.turn()
    w3.turn()

    def weight(n, w):
        for i, part in enumerate(w.end()):
            at = n * HEAD_DIM + i * HEAD_DIM // 2
            gw_out[:, at : at + HEAD_DIM // 2] = part.T

    def ordered(into, part, r):
        for n, rows in enumerate(r.end()):
            for i in range(HALF_BLOCK // 2):
                at = part * HALF_BLOCK + n * (HALF_BLOCK // 2) + i
                into[pl.ds(at, POOLED, stride=KEY_BLOCK), :] = rows[i * POOLED : (i + 1) * POOLED]

    k0.combine()
    v0.combine()
    w2.combine2()
    w3.combine2()
    k1.combine()
    v1.combine()
    k0.turn()
    v0.turn()
    k1.turn()
    v1.turn()
    k0.combine2()
    v0.combine2()
    k1.combine2()
    v1.combine2()
    weight(0, w0)
    weight(1, w1)
    weight(2, w2)
    weight(3, w3)
    ordered(dk_set, 0, k0)
    ordered(dv_set, 0, v0)
    ordered(dk_set, 1, k1)
    ordered(dv_set, 1, v1)
    gk_out[...] = dk_set[:TOKENS, :].astype(BF16)
    gv_out[...] = dv_set[:TOKENS, :].astype(BF16)
    send.finish()


SCATTER_COPIES = 8 * 12
SCATTER_MIB = 31.2


def run_scatter(chosen, k_all, v_all, h_all, dqp, dpk, dpv, qs, cs, ls, pick, places):
    vmem = pl.BlockSpec(memory_space=pltpu.VMEM)
    smem = pl.BlockSpec(memory_space=pltpu.SMEM)
    first = HALF_BLOCK * CHOSEN + POOLED
    second = HALF_BLOCK * CHOSEN
    outgoing = [pltpu.VMEM((SIDE, SIDE, n, HEAD_DIM), BF16) for n in (first, first, second, second)]
    grad = pltpu.VMEM((SIDE, SIDE, HEAD_DIM, GW_COLS), BF16)
    return pl.pallas_call(
        scatter_kernel,
        name="scatter",
        out_shape=(
            jax.ShapeDtypeStruct((TOKENS, GROUP * HEAD_DIM), BF16),
            jax.ShapeDtypeStruct((TOKENS, HEAD_DIM), BF16),
            jax.ShapeDtypeStruct((TOKENS, HEAD_DIM), BF16),
            jax.ShapeDtypeStruct((GW_COLS, GROUP * HEAD_DIM), F32),
        ),
        in_specs=[smem] + [vmem] * 11,
        out_specs=(vmem,) * 4,
        scratch_shapes=[
            pltpu.VMEM((SETS, HEAD_DIM), BF16),
            pltpu.VMEM((SETS, HEAD_DIM), BF16),
            pltpu.VMEM((BLOCKS, SETS, PAIR_Q), BF16),
            pltpu.VMEM((BLOCKS, SETS, PAIR_Q), BF16),
            pltpu.VMEM((BLOCKS * SETS, HEAD_DIM), F32),
            pltpu.VMEM((BLOCKS * SETS, HEAD_DIM), F32),
            pltpu.VMEM((GROUP * HEAD_DIM, TOKENS), BF16),
            *outgoing,
            pltpu.VMEM((TOKENS, HEAD_DIM), F32),
            pltpu.VMEM((TOKENS, HEAD_DIM), F32),
            grad,
            grad,
            grad,
            grad,
            *(listed_buffers(first) * 2),
            *(listed_buffers(second) * 2),
            *(reduce_buffers(HEAD_DIM, GW_COLS) * 4),
            pltpu.SemaphoreType.DMA((SCATTER_COPIES,)),
            pltpu.SemaphoreType.DMA((SCATTER_COPIES,)),
        ],
        compiler_params=pltpu.CompilerParams(
            collective_id=1, has_side_effects=True, vmem_limit_bytes=int(SCATTER_MIB * MIB)
        ),
    )(chosen, k_all, v_all, h_all, dqp, dpk, dpv, qs, cs, ls, pick, places)


def finish_kernel(*refs):
    copies = [pltpu.make_async_copy(refs[i], refs[4 + i], refs[8].at[i]) for i in range(4)]
    for copy in copies:
        copy.start()
    for copy in copies:
        copy.wait()


def run_finish(*outs):
    return pl.pallas_call(
        finish_kernel,
        name="finish",
        out_shape=tuple(jax.ShapeDtypeStruct(a.shape, a.dtype) for a in outs),
        in_specs=[pl.BlockSpec(memory_space=pltpu.VMEM)] * 4,
        out_specs=(pl.BlockSpec(memory_space=pltpu.HBM),) * 4,
        scratch_shapes=[pltpu.SemaphoreType.DMA((4,))],
        compiler_params=pltpu.CompilerParams(vmem_limit_bytes=8 * MIB),
    )(*outs)


def body(hidden_rows, queries, key_rows, value_rows, branch_gates, log_sums, chosen, out_grad):
    lists = chosen.reshape(BLOCKS, CHOSEN)
    k_all, v_all, h_all, *more = run_gather(
        key_rows, value_rows, hidden_rows, queries, out_grad, branch_gates, log_sums, lists
    )
    by_block = (SEQ // KEY_BLOCK, KEY_BLOCK, HEAD_DIM)
    outs = run_scatter(
        lists,
        k_all.reshape(by_block),
        v_all.reshape(by_block),
        h_all.reshape(TOKENS, MODEL),
        *more,
    )
    return run_finish(*outs)


def solution(mesh):
    placed = (
        P(("kv", "tp"), None),
        P("kv", "tp"),
        P("kv", "tp"),
        P("kv", "tp"),
        P(None, "tp", "kv"),
        P(None, "tp", "kv"),
        P("tp", "kv", None),
        P("kv", "tp"),
    )
    return jax.shard_map(
        body,
        mesh=mesh,
        in_specs=placed,
        out_specs=(P("kv", "tp"), P("kv", "tp"), P("kv", "tp"), P("kv", "tp")),
        check_vma=False,
    )
```
